32 devices in a mesh: sp: 16 (over z, y, x), tp: 2 (over core).
Axes of the slice: x: 2, y: 2, z: 4, core: 2. Of those that a mesh axis runs over, the one named last changes fastest.
Arguments:
- skip_stream_entering: bfloat16 [2048, 2048], P(('sp', 'tp')), may hold values from -6 to 6
- content_signal_matrix: bfloat16 [2048, 4096], P('sp', 'tp'), may hold values from -6 to 6
- writer_signal_matrix: bfloat16 [2048, 1024], P('sp', 'tp'), may hold values from -6 to 6
- reader_signal_matrix: bfloat16 [2048, 1024], P('sp', 'tp'), may hold values from -6 to 6
- multiplier_signal: bfloat16 [2048, 4096], P('sp', 'tp'), may hold values from -6 to 6
- interval_before_softplus: float32 [64, 2048], P('tp', 'sp'), may hold values from -7.5 to 0.5
- extra_log_shrink: float32 [64, 2048], P('tp', 'sp'), may hold values from -2.8 to 0
- log_forget_speed: float32 [64], P('tp'), may hold values from -12 to 0
- content_filter_coefs: bfloat16 [4, 4096], P(None, 'tp'), may hold values from -3 to 3
- writer_filter_coefs: bfloat16 [4, 1024], P(None, 'tp'), may hold values from -3 to 3
- reader_filter_coefs: bfloat16 [4, 1024], P(None, 'tp'), may hold values from -3 to 3
- skip_path_factor: float32 [64], P('tp'), may hold values from 0.25 to 2
- cluster_scaling_vector: float32 [4096], P('tp'), may hold values from 0.1 to 1.9
- blend_result_matrix: bfloat16 [4096, 2048], P('tp'), may hold values from -0.09375 to 0.09375
- feature_blend_scaling: float32 [2048], replicated, may hold values from 0.1 to 1.9
- widening_matrix: bfloat16 [2048, 8192], P('sp', 'tp'), may hold values from -0.125 to 0.125
- narrowing_matrix: bfloat16 [8192, 2048], P('tp', 'sp'), may hold values from -0.0625 to 0.0625
Outputs:
- layer_out: bfloat16 [2048, 2048], P(('sp', 'tp'))
The draws below stay inside these ranges and needn't reach their ends.
All inputs are finite; a program needn't handle non-finite values.
Results may differ from the reference program's by a relative error of at most 0.02.
Values may be sent and summed in bfloat16 or wider, within the bound.
A program may use at most 128 MiB of HBM per device.

```python
import math
import jax
import jax.numpy as jnp
from jax import lax

D = 2048
HEADS = 64
HEAD_DIM = 64
GROUPS = 8
STATE = 128
FF = 8192
CONV = 4
BLOCK = 128
TOK_DEV = 128
D_INNER = 4096
TOKENS = 2048
N_TP = 2


def draw_interval_before_softplus(key, part):
    noise_key, shift_key = jax.random.split(jax.random.fold_in(key, 11))
    noise = jnp.clip(jax.random.normal(noise_key, (HEADS, TOKENS), jnp.float32), -3.0, 3.0)
    offsets = jax.random.uniform(shift_key, (TOKENS // TOK_DEV,), jnp.float32, -1.0, 1.0)
    return -3.5 + noise + jnp.repeat(offsets, TOK_DEV)[None, :]


def draw_log_forget_speed(key, part):
    order_key, slow_key, fast_key = jax.random.split(jax.random.fold_in(key, 23), 3)
    order = jax.random.permutation(order_key, HEADS)
    slow = order < HEADS // 2
    slow_rate = jnp.exp(jax.random.uniform(slow_key, (HEADS,), jnp.float32, math.log(0.3), 0.0)) / (0.06 * TOKENS)
    fast_rate = jnp.exp(jax.random.uniform(fast_key, (HEADS,), jnp.float32, math.log(0.17), math.log(0.55)))
    return jnp.log(jnp.where(slow, slow_rate, fast_rate))


def draw_extra_log_shrink(key, part):
    where_key, depth_key = jax.random.split(jax.random.fold_in(key, 37))
    places = jax.random.randint(where_key, (4,), 0, TOKENS)
    depths = jax.random.uniform(depth_key, (HEADS, 4), jnp.float32, math.log(0.5), math.log(0.8))
    indicator = (jnp.arange(TOKENS)[None, :] == places[:, None]).astype(jnp.float32)
    return jnp.dot(depths, indicator, precision=lax.Precision.HIGHEST)


def level_of(key, dims, pieces, least, top_value):
    def one(axis_at, parts):
        steps = jax.random.uniform(jax.random.fold_in(jax.random.fold_in(key, 6), axis_at), (parts,), jnp.float32, least / len(pieces), top_value / len(pieces))
        return jnp.repeat(jnp.exp(steps), dims[axis_at] // parts).reshape((-1,) + (1,) * (len(dims) - axis_at - 1))

    factor_of = one(*pieces[0])
    for cut in pieces[1:]:
        factor_of = factor_of * one(*cut)
    return factor_of


def centred(key, extent, spread, limit, pieces=(), kind=jnp.bfloat16):
    values = spread * jax.random.normal(key, extent, jnp.float32)
    if pieces:
        values = values * level_of(key, extent, pieces, -0.22, 0.18)
    return jnp.clip(values, -limit, limit).astype(kind)


def setup_inputs(seed: int = 0) -> dict:
    arg_keys = jax.random.split(jax.random.key(seed), 18)
    return {
        "skip_stream_entering": centred(arg_keys[0], (TOKENS, D), 1.0, 6.0, ((0, 32),)),
        "content_signal_matrix": centred(arg_keys[1], (TOKENS, D_INNER), 1.0, 6.0, ((0, 16), (1, 2))),
        "writer_signal_matrix": centred(arg_keys[2], (TOKENS, GROUPS * STATE), 1.0, 6.0, ((0, 16), (1, 2))),
        "reader_signal_matrix": centred(arg_keys[3], (TOKENS, GROUPS * STATE), 1.0, 6.0, ((0, 16), (1, 2))),
        "multiplier_signal": centred(arg_keys[4], (TOKENS, D_INNER), 1.0, 6.0, ((0, 16), (1, 2))),
        "interval_before_softplus": draw_interval_before_softplus(jax.random.fold_in(arg_keys[17], 71), 0),
        "extra_log_shrink": draw_extra_log_shrink(jax.random.fold_in(arg_keys[17], 71), 0),
        "log_forget_speed": draw_log_forget_speed(jax.random.fold_in(arg_keys[17], 71), 0),
        "content_filter_coefs": centred(arg_keys[8], (CONV, D_INNER), 0.5, 3.0, ((1, 2),)),
        "writer_filter_coefs": centred(arg_keys[9], (CONV, GROUPS * STATE), 0.5, 3.0, ((1, 2),)),
        "reader_filter_coefs": centred(arg_keys[10], (CONV, GROUPS * STATE), 0.5, 3.0, ((1, 2),)),
        "skip_path_factor": jnp.clip(0.25 + 1.75 * jax.random.uniform(arg_keys[11], (HEADS,), jnp.float32) ** level_of(arg_keys[11], (HEADS,), ((0, 2),), -0.2, 0.2), 0.25, 2.0),
        "cluster_scaling_vector": jnp.clip(1.0 + 0.18 * jax.random.normal(arg_keys[12], (D_INNER,), jnp.float32), 0.1, 1.9),
        "blend_result_matrix": centred(arg_keys[13], (D_INNER, D), D_INNER ** -0.5, 0.09375, ((0, 2),)),
        "feature_blend_scaling": jnp.clip(1.0 + 0.18 * jax.random.normal(arg_keys[14], (D,), jnp.float32), 0.1, 1.9),
        "widening_matrix": centred(arg_keys[15], (D, FF), D ** -0.5, 0.125, ((0, 16), (1, 2))),
        "narrowing_matrix": centred(arg_keys[16], (FF, D), FF ** -0.5, 0.0625, ((0, 2), (1, 16))),
    }


epsilon = 1e-05
precise = lax.Precision.HIGHEST

def convolve(inputs, conv_taps):
    width = conv_taps.shape[0]
    length = inputs.shape[0]
    extended = jnp.pad(inputs, ((width - 1, 0), (0, 0)))
    summed = extended[0:length].astype(jnp.float32) * conv_taps[0].astype(jnp.float32)
    for offset in range(1, width):
        summed = summed + extended[offset:offset + length].astype(jnp.float32) * conv_taps[offset].astype(jnp.float32)
    return jax.nn.silu(summed)

def advance(carried, pair):
    block_state, block_factor = pair
    return (carried * block_factor[..., None, None] + block_state, carried)

def blockwise(values, interval_lengths, log_forgetting, key_rows, query_rows):
    length, groups, per_group, width = values.shape
    blocks = length // BLOCK
    value_blocks = values.reshape(blocks, BLOCK, groups, per_group, width)
    step_blocks = jnp.transpose(interval_lengths.reshape(groups, per_group, blocks, BLOCK), (2, 3, 0, 1))
    weighted = value_blocks * step_blocks[..., None]
    cumulative = jnp.cumsum(jnp.transpose(log_forgetting.reshape(groups, per_group, blocks, BLOCK), (2, 0, 1, 3)), axis=-1)
    key_blocks = key_rows.reshape(blocks, BLOCK, groups, -1)
    query_blocks = query_rows.reshape(blocks, BLOCK, groups, -1)
    causal = jnp.tril(jnp.ones((BLOCK, BLOCK), dtype=bool))
    decay_mask = jnp.exp(jnp.where(causal, cumulative[..., :, None] - cumulative[..., None, :], -jnp.inf))
    scores = jnp.einsum('clgn,csgn->cgls', query_blocks, key_blocks, precision=precise)
    within = jnp.einsum('cgls,cgrls,csgrp->clgrp', scores, decay_mask, weighted, precision=precise)
    to_end = jnp.exp(cumulative[..., -1:] - cumulative)
    states = jnp.einsum('clgn,cgrl,clgrp->cgrpn', key_blocks, to_end, weighted, precision=precise)
    block_totals = cumulative[..., -1]
    initial = jnp.zeros(states.shape[1:], jnp.float32)
    final, entering = lax.scan(advance, initial, (states, jnp.exp(block_totals)))
    carried = jnp.einsum('clgn,cgrpn,cgrl->clgrp', query_blocks, entering, jnp.exp(cumulative), precision=precise)
    return ((within + carried).reshape(length, groups, per_group, width), final)

def one_group(members):
    value_part, step_part, log_part, key_part, query_part = members
    result = blockwise(value_part[:, None], step_part[None], log_part[None], key_part, query_part)[0]
    return result[:, 0]

def normalize(rows, gain):
    widened = rows.astype(jnp.float32)
    scaled = widened * lax.rsqrt(lax.optimization_barrier(jnp.mean(widened * widened, axis=-1, keepdims=True)) + epsilon)
    return (scaled * gain).astype(jnp.bfloat16)

def reference(skip_stream_entering, content_signal_matrix, writer_signal_matrix, reader_signal_matrix, multiplier_signal, interval_before_softplus, extra_log_shrink, log_forget_speed, content_filter_coefs, writer_filter_coefs, reader_filter_coefs, skip_path_factor, cluster_scaling_vector, blend_result_matrix, feature_blend_scaling, widening_matrix, narrowing_matrix):
    per_group = HEADS // GROUPS
    values = convolve(content_signal_matrix, content_filter_coefs)
    key_rows = convolve(writer_signal_matrix, writer_filter_coefs)
    query_rows = convolve(reader_signal_matrix, reader_filter_coefs)
    interval_lengths = jax.nn.softplus(interval_before_softplus)
    log_forgetting = extra_log_shrink - jnp.exp(log_forget_speed)[:, None] * interval_lengths
    members = (jnp.transpose(values.reshape(TOKENS, GROUPS, per_group, HEAD_DIM), (1, 0, 2, 3)), interval_lengths.reshape(GROUPS, per_group, TOKENS), log_forgetting.reshape(GROUPS, per_group, TOKENS), jnp.transpose(key_rows.reshape(TOKENS, GROUPS, STATE), (1, 0, 2)), jnp.transpose(query_rows.reshape(TOKENS, GROUPS, STATE), (1, 0, 2)))
    scan_out = jnp.transpose(lax.map(one_group, members), (1, 0, 2, 3)).reshape(TOKENS, D_INNER)
    gated = (scan_out + jnp.repeat(skip_path_factor, HEAD_DIM) * values) * jax.nn.silu(multiplier_signal.astype(jnp.float32))
    grouped = gated.reshape(TOKENS, GROUPS, D_INNER // GROUPS)
    grouped = grouped * lax.rsqrt(lax.optimization_barrier(jnp.mean(grouped * grouped, axis=-1, keepdims=True)) + epsilon)
    heads_out = (grouped.reshape(TOKENS, D_INNER) * cluster_scaling_vector).astype(jnp.bfloat16)
    part_width = D_INNER // N_TP
    mixer_sum = jnp.zeros((TOKENS, D), jnp.float32)
    for index in range(N_TP):
        partial_term = jnp.dot(heads_out[:, index * part_width:(index + 1) * part_width], blend_result_matrix[index * part_width:(index + 1) * part_width], preferred_element_type=jnp.float32)
        mixer_sum = mixer_sum + lax.optimization_barrier(partial_term.astype(jnp.bfloat16)).astype(jnp.float32)
    mixer_out = mixer_sum.astype(jnp.bfloat16)
    layer_state = (skip_stream_entering.astype(jnp.float32) + mixer_out.astype(jnp.float32)).astype(jnp.bfloat16)
    normed = normalize(layer_state, feature_blend_scaling)
    hidden_width = FF // N_TP
    mlp_sum = jnp.zeros((TOKENS, D), jnp.float32)
    for index in range(N_TP):
        lifted = jax.nn.relu(jnp.dot(normed, widening_matrix[:, index * hidden_width:(index + 1) * hidden_width], preferred_element_type=jnp.float32))
        hidden = (lifted * lifted).astype(jnp.bfloat16)
        partial_term = jnp.dot(hidden, narrowing_matrix[index * hidden_width:(index + 1) * hidden_width], preferred_element_type=jnp.float32)
        mlp_sum = mlp_sum + lax.optimization_barrier(partial_term.astype(jnp.bfloat16)).astype(jnp.float32)
    mlp_out = mlp_sum.astype(jnp.bfloat16)
    return (layer_state.astype(jnp.float32) + mlp_out.astype(jnp.float32)).astype(jnp.bfloat16)
```

```python
import functools
import math
import jax
import jax.numpy as jnp
from jax import lax
from jax.experimental import pallas as pl
from jax.experimental.pallas import tpu as pltpu
from jax.sharding import PartitionSpec as P

HEAD_DIM = 64
STATE = 128
BLOCK = 128


epsilon = 1e-05
precise = lax.Precision.HIGHEST
SP = ("sa", "sb")
TEAM = 8


def shifted(value, axis, steps):
    count = lax.axis_size(axis)
    initial, last = (max(0, -steps), min(count, count - steps))
    return lax.ppermute(value, axis, [(source, source + steps) for source in range(initial, last)])


def scan_rows(parts, factors, entering):
    def one(place, carried):
        entering[place] = carried.astype(jnp.bfloat16)
        return carried * factors[place] + parts[place].astype(jnp.float32)

    lax.fori_loop(0, parts.shape[0], one, jnp.zeros(parts.shape[1:], jnp.float32))


def prefix(log_total, end_state, rider):
    shards = lax.axis_size(SP)
    heads = end_state.shape[0] * end_state.shape[1]
    state_width = end_state.shape[-1]
    rows = end_state.reshape(-1, state_width).astype(jnp.bfloat16)
    count = rows.shape[0] // shards
    decays = jnp.repeat(jnp.exp(log_total).reshape(heads), rows.shape[0] // heads)
    extra = -(-count // state_width) * 16
    decays = decays.astype(jnp.bfloat16).reshape(shards, count)
    decays = jnp.pad(decays, ((0, 0), (0, extra * state_width - count)))
    packed = jnp.concatenate(
        [rows.reshape(shards, count, state_width), decays.reshape(shards, extra, state_width)],
        axis=1,
    )
    packed = lax.all_to_all(packed, SP, split_axis=0, concat_axis=0)
    parts = packed[:, :count]
    factors = packed[:, count:].reshape(shards, -1)[:, :count].astype(jnp.float32)
    entering = pl.pallas_call(
        scan_rows,
        out_shape=jax.ShapeDtypeStruct(parts.shape, jnp.bfloat16),
    )(parts, jnp.broadcast_to(factors[..., None], parts.shape))
    entering, rider = lax.optimization_barrier((entering, rider))
    back = lax.all_to_all(
        entering.reshape(rows.shape), SP, split_axis=0, concat_axis=0, tiled=True
    )
    return back.reshape(end_state.shape).astype(jnp.float32), rider


def summed_share(partial, axis):
    count = lax.axis_size(axis)
    if count != 2:
        return lax.psum_scatter(partial, axis, scatter_dimension=0, tiled=True)
    me = lax.axis_index(axis)
    length = partial.shape[0] // 2
    away = lax.dynamic_slice_in_dim(partial, (1 - me) * length, length, 0)
    kept = lax.dynamic_slice_in_dim(partial, me * length, length, 0)
    arrived = lax.ppermute(away, axis, [(0, 1), (1, 0)])
    return (kept.astype(jnp.float32) + arrived.astype(jnp.float32)).astype(jnp.bfloat16)


def convolve(inputs, rim_rows, conv_taps):
    width = conv_taps.shape[0]
    length = inputs.shape[0]
    extended = jnp.concatenate([rim_rows, inputs], axis=0)
    summed = extended[0:length].astype(jnp.float32) * conv_taps[0].astype(jnp.float32)
    for offset in range(1, width):
        summed = summed + extended[offset : offset + length].astype(jnp.float32) * conv_taps[
            offset
        ].astype(jnp.float32)
    return jax.nn.silu(summed)


def advance(carried, pair):
    block_state, block_factor = pair
    return (carried * block_factor[..., None, None] + block_state, carried)


def blockwise(values, interval_lengths, log_forgetting, key_rows, query_rows):
    length, groups, per_group, width = values.shape
    blocks = length // BLOCK
    value_blocks = values.reshape(blocks, BLOCK, groups, per_group, width)
    step_blocks = jnp.transpose(
        interval_lengths.reshape(groups, per_group, blocks, BLOCK), (2, 3, 0, 1)
    )
    weighted = value_blocks * step_blocks[..., None]
    cumulative = jnp.cumsum(
        jnp.transpose(log_forgetting.reshape(groups, per_group, blocks, BLOCK), (2, 0, 1, 3)),
        axis=-1,
    )
    key_blocks = key_rows.reshape(blocks, BLOCK, groups, -1)
    query_blocks = query_rows.reshape(blocks, BLOCK, groups, -1)
    causal = jnp.tril(jnp.ones((BLOCK, BLOCK), dtype=bool))
    decay_mask = jnp.exp(
        jnp.where(causal, cumulative[..., :, None] - cumulative[..., None, :], -jnp.inf)
    )
    scores = jnp.einsum("clgn,csgn->cgls", query_blocks, key_blocks, precision=precise)
    within = jnp.einsum("cgls,cgrls,csgrp->clgrp", scores, decay_mask, weighted, precision=precise)
    to_end = jnp.exp(cumulative[..., -1:] - cumulative)
    states = jnp.einsum("clgn,cgrl,clgrp->cgrpn", key_blocks, to_end, weighted, precision=precise)
    block_totals = cumulative[..., -1]
    initial = jnp.zeros(states.shape[1:], jnp.float32)
    final, entering = lax.scan(advance, initial, (states, jnp.exp(block_totals)))
    carried = jnp.einsum(
        "clgn,cgrpn,cgrl->clgrp", query_blocks, entering, jnp.exp(cumulative), precision=precise
    )
    from_start = (jnp.cumsum(block_totals, axis=0) - block_totals)[..., None] + cumulative
    return (within + carried, final, from_start, jnp.sum(block_totals, axis=0))


def normalize(rows, gain):
    widened = rows.astype(jnp.float32)
    scaled = widened * lax.rsqrt(jnp.mean(widened * widened, axis=-1, keepdims=True) + epsilon)
    return (scaled * gain).astype(jnp.bfloat16)


def per_device(
    skip_stream_entering,
    content_signal_matrix,
    writer_signal_matrix,
    reader_signal_matrix,
    multiplier_signal,
    interval_before_softplus,
    extra_log_shrink,
    log_forget_speed,
    content_filter_coefs,
    writer_filter_coefs,
    reader_filter_coefs,
    skip_path_factor,
    cluster_scaling_vector,
    blend_result_matrix,
    feature_blend_scaling,
    widening_matrix,
    narrowing_matrix,
):
    up_part = lax.all_to_all(widening_matrix, "sb", split_axis=1, concat_axis=0, tiled=True)
    narrowing_matrix, up_part = lax.optimization_barrier((narrowing_matrix, up_part))
    up_use = lax.all_gather(up_part, "sa", axis=0, tiled=True)
    down_part = lax.all_to_all(narrowing_matrix, "sb", split_axis=0, concat_axis=1, tiled=True)
    (
        content_signal_matrix,
        writer_signal_matrix,
        reader_signal_matrix,
        interval_before_softplus,
        down_part,
    ) = lax.optimization_barrier(
        (
            content_signal_matrix,
            writer_signal_matrix,
            reader_signal_matrix,
            interval_before_softplus,
            down_part,
        )
    )
    down_use = lax.all_gather(down_part, "sa")
    rim_width = content_filter_coefs.shape[0] - 1
    length = content_signal_matrix.shape[0]
    signals = (content_signal_matrix, writer_signal_matrix, reader_signal_matrix)
    tails = jnp.concatenate([signal[length - rim_width :] for signal in signals], axis=1)
    rims = shifted(tails, SP, 1)
    first, second = signals[0].shape[1], signals[0].shape[1] + signals[1].shape[1]
    values = convolve(signals[0], rims[:, :first], content_filter_coefs)
    key_rows = convolve(signals[1], rims[:, first:second], writer_filter_coefs)
    query_rows = convolve(signals[2], rims[:, second:], reader_filter_coefs)
    local_heads = interval_before_softplus.shape[0]
    local_groups = writer_signal_matrix.shape[1] // STATE
    per_group = local_heads // local_groups
    interval_lengths = jax.nn.softplus(interval_before_softplus)
    log_forgetting = extra_log_shrink - jnp.exp(log_forget_speed)[:, None] * interval_lengths
    shaped = values.reshape(length, local_groups, per_group, HEAD_DIM)
    local_out, end_state, from_start, device_total = blockwise(
        shaped,
        interval_lengths.reshape(local_groups, per_group, length),
        log_forgetting.reshape(local_groups, per_group, length),
        key_rows,
        query_rows,
    )
    incoming, up_use = prefix(device_total, end_state, up_use)
    query_blocks = query_rows.reshape(length // BLOCK, BLOCK, local_groups, STATE)
    arriving = jnp.einsum(
        "clgn,grpn,cgrl->clgrp", query_blocks, incoming, jnp.exp(from_start), precision=precise
    )
    scan_out = (local_out + arriving).reshape(length, local_heads * HEAD_DIM)
    gated = (scan_out + jnp.repeat(skip_path_factor, HEAD_DIM) * values) * jax.nn.silu(
        multiplier_signal.astype(jnp.float32)
    )
    grouped = gated.reshape(length, local_groups, -1)
    grouped = grouped * lax.rsqrt(jnp.mean(grouped * grouped, axis=-1, keepdims=True) + epsilon)
    heads_out = (grouped.reshape(length, -1) * cluster_scaling_vector).astype(jnp.bfloat16)
    mixer_rows = summed_share(
        jnp.dot(heads_out, blend_result_matrix, preferred_element_type=jnp.float32).astype(
            jnp.bfloat16
        ),
        "tp",
    )
    own_rows = (skip_stream_entering.astype(jnp.float32) + mixer_rows.astype(jnp.float32)).astype(
        jnp.bfloat16
    )
    normed = normalize(own_rows, feature_blend_scaling)
    down_whole = jnp.concatenate([down_use[k] for k in range(down_use.shape[0])], axis=1)

    def mixed(rows):
        lifted = jax.nn.relu(jnp.dot(rows, up_use, preferred_element_type=jnp.float32))
        hidden = (lifted * lifted).astype(jnp.bfloat16)
        partial = jnp.dot(hidden, down_whole, preferred_element_type=jnp.float32)
        return partial.astype(jnp.bfloat16)

    if lax.axis_size("tp") == 2:
        members, width = lax.axis_size("sb"), normed.shape[1]
        swap = [(0, 1), (1, 0)]
        copies = jnp.broadcast_to(normed[None], (members,) + normed.shape)
        own_half = lax.all_to_all(copies, "sb", split_axis=0, concat_axis=0)
        own_half = own_half.reshape(-1, width)
        other_half = lax.ppermute(own_half, "tp", swap)
        arrived = lax.ppermute(mixed(other_half), "tp", swap)
        joined = mixed(own_half).astype(jnp.float32) + arrived.astype(jnp.float32)
        joined = joined.astype(jnp.bfloat16).reshape(members, -1, width)
        shares = lax.all_to_all(joined, "sb", split_axis=0, concat_axis=0)
        mlp_rows = jnp.sum(shares.astype(jnp.float32), axis=0)
    else:
        team_rows = lax.all_gather(normed, ("sb", "tp"), axis=0, tiled=True)
        mlp_rows = lax.psum_scatter(
            mixed(team_rows), ("sb", "tp"), scatter_dimension=0, tiled=True
        )
    mlp_rows = mlp_rows.astype(jnp.bfloat16)
    return (own_rows.astype(jnp.float32) + mlp_rows.astype(jnp.float32)).astype(jnp.bfloat16)


TEAM_LINKS = pl.DeviceIdType.MESH


def split3(wide):
    one = wide.astype(jnp.bfloat16)
    rest = wide - one.astype(jnp.float32)
    two = rest.astype(jnp.bfloat16)
    return one, two, (rest - two.astype(jnp.float32)).astype(jnp.bfloat16)


def contract(left, right, dims):
    return lax.dot_general(left, right, (dims, ((), ())), preferred_element_type=jnp.float32)


def exact(left, right, dims, left_split):
    if left_split:
        terms = [contract(part, right, dims) for part in split3(left)]
    else:
        terms = [contract(left, part, dims) for part in split3(right)]
    return terms[0] + terms[1] + terms[2]


def selector(rows, columns, per_row):
    row = lax.broadcasted_iota(jnp.int32, (rows, columns), 0)
    column = lax.broadcasted_iota(jnp.int32, (rows, columns), 1)
    return jnp.where(column // per_row == row, 1.0, 0.0).astype(jnp.bfloat16)


def layer_kernel(
    team,
    skip_ref,
    content_ref,
    writer_ref,
    reader_ref,
    multiplier_ref,
    interval_ref,
    shrink_ref,
    speed_ref,
    content_taps,
    writer_taps,
    reader_taps,
    skip_factor,
    cluster_gain,
    blend_hbm,
    feature_gain,
    up_hbm,
    down_hbm,
    out_ref,
    halo,
    wide,
    values,
    value_low,
    keyquery,
    blend,
    up,
    down,
    column_decay,
    row_decay,
    scan,
    scale_in,
    state_out,
    state_in,
    entering,
    kept_decay,
    cross_out,
    cross_in,
    back_out,
    back_in,
    heads,
    part_out,
    part_in,
    state_rows,
    acts,
    hidden,
    pair_out,
    pair_in,
    plane_out,
    plane_in,
    depth_out,
    depth_in,
    local_sem,
    halo_ss,
    halo_rs,
    up_ss,
    up_rs,
    down_ss,
    down_rs,
    st_ss,
    st_rs,
    cr_ss,
    cr_rs,
    bk_ss,
    bk_rs,
    pt_ss,
    pt_rs,
    az_ss,
    az_rs,
    ap_ss,
    ap_rs,
    ad_ss,
    ad_rs,
    pr_ss,
    pr_rs,
    pl_ss,
    pl_rs,
    dp_ss,
    dp_rs,
):
    f32, bf16 = jnp.float32, jnp.bfloat16
    batches = plan(team)
    shards = lax.axis_size("sp")
    sp, tp = lax.axis_index("sp"), lax.axis_index("tp")
    own_team, me = sp // team, lax.rem(sp, team)
    length, inner = content_ref.shape
    state_width = writer_ref.shape[1]
    local_heads = interval_ref.shape[0]
    groups = state_width // STATE
    group_width = inner // groups
    model = skip_ref.shape[1]
    unit = up.shape[2]
    slice_width = inner // team
    half = team // 2
    rows_own = skip_ref.shape[0]

    def copy(src, dst, ss, rs, sp_to, tp_to):
        return pltpu.make_async_remote_copy(
            src_ref=src,
            dst_ref=dst,
            send_sem=ss,
            recv_sem=rs,
            device_id=(sp_to, tp_to),
            device_id_type=TEAM_LINKS,
        )

    def mate(step):
        return own_team * team + lax.rem(me + step, team)

    def far(step):
        return (1 - own_team) * team + lax.rem(me + step, team)

    def flip(index, bit):
        return index + bit - 2 * bit * lax.rem(index // bit, 2)

    def weight(kind, place, target):
        index = lax.rem(target, team)
        offset = pl.ds(pl.multiple_of(index * unit, unit), unit)
        if kind == 0:
            return copy(up_hbm.at[:, offset], up.at[sp], up_ss.at[place], up_rs.at[sp], target, tp)
        return copy(
            down_hbm.at[offset, :], down.at[sp], down_ss.at[place], down_rs.at[sp], target, tp
        )

    def weight_near(kind, step):
        return weight(kind, step - 1, mate(step))

    def weight_far(kind, step):
        return weight(kind, team - 1 + step, far(step))

    mine = pl.ds(pl.multiple_of(me * unit, unit), unit)
    local_up = pltpu.make_async_copy(up_hbm.at[:, mine], up.at[sp], local_sem.at[0])
    local_down = pltpu.make_async_copy(down_hbm.at[mine, :], down.at[sp], local_sem.at[1])
    local_blend = pltpu.make_async_copy(blend_hbm, blend, local_sem.at[2])
    local_up.start()
    local_down.start()
    local_blend.start()

    barrier = pltpu.get_barrier_semaphore()
    for step in range(1, shards):
        pl.semaphore_signal(
            barrier,
            inc=1,
            device_id=(lax.rem(sp + step, shards), tp),
            device_id_type=TEAM_LINKS,
        )
    pl.semaphore_signal(barrier, inc=1, device_id=(sp, 1 - tp), device_id_type=TEAM_LINKS)
    pl.semaphore_wait(barrier, shards)

    following = lax.rem(sp + 1, shards)
    spans = ((content_ref, 0, inner), (writer_ref, inner, state_width))
    spans = spans + ((reader_ref, inner + state_width, state_width),)
    halo_copies = []
    for place, (ref, first, size) in enumerate(spans):
        halo_copies.append(
            copy(
                ref.at[pl.ds(length - 16, 16), :],
                halo.at[:, pl.ds(first, size)],
                halo_ss.at[place],
                halo_rs.at[place],
                following,
                tp,
            )
        )
    for one in halo_copies:
        one.start()
    for kind, step, where in batches[0]:
        (weight_near if where == 0 else weight_far)(kind, step).start()

    steps = interval_ref[...]
    steps = jnp.maximum(steps, 0.0) + jnp.log1p(jnp.exp(-jnp.abs(steps)))
    forget = shrink_ref[...] - jnp.exp(speed_ref[...]) * steps
    row_index = lax.broadcasted_iota(jnp.int32, (length, length), 0)
    column_index = lax.broadcasted_iota(jnp.int32, (length, length), 1)
    lower = jnp.where(row_index >= column_index, 1.0, 0.0).astype(bf16)
    upper = jnp.where(row_index <= column_index, 1.0, 0.0).astype(bf16)
    unity = jnp.where(row_index == column_index, 1.0, 0.0).astype(bf16)
    log_steps = jnp.log(steps)
    total_rows = exact(forget, upper, ((1,), (0,)), True)
    total_columns = exact(lower, forget, ((1,), (1,)), False)
    log_columns = exact(unity, log_steps, ((1,), (1,)), False)
    row_decay[...] = total_rows - log_steps
    by_head = selector(local_heads, local_heads * length, length)
    column_decay[...] = exact(total_columns, by_head, ((1,), (0,)), True)
    by_channel = selector(local_heads, inner, HEAD_DIM)
    scale_in[...] = exact(jnp.exp(total_columns), by_channel, ((1,), (0,)), True)
    last = total_columns[length - 1 : length, :]
    to_end = jnp.exp(last - total_columns + log_columns)
    end_scale = exact(to_end, by_channel, ((1,), (0,)), True)
    whole_decay = exact(
        jnp.broadcast_to(jnp.exp(last), (16, local_heads)), by_channel, ((1,), (0,)), True
    )
    skip_scale = exact(
        jnp.broadcast_to(skip_factor[...], (16, local_heads)), by_channel, ((1,), (0,)), True
    )

    for one in halo_copies:
        one.wait_recv()
    chunk = state_width
    for ref, taps, first, size in (
        (content_ref, content_taps, 0, inner),
        (writer_ref, writer_taps, inner, state_width),
        (reader_ref, reader_taps, inner + state_width, state_width),
    ):
        for start in range(0, size, chunk):
            at = slice(start, start + chunk)
            placed = slice(first + start, first + start + chunk)
            wide[8:, placed] = ref[:, at].astype(f32)
            rim = halo[:, placed].astype(f32)[8:, :]
            wide[0:8, placed] = jnp.where(sp > 0, rim, 0.0)
            weights = taps[:, at].astype(f32)
            count = taps.shape[0]
            base = 8 - (count - 1)
            total = wide[base : base + length, placed] * weights[0:1, :]
            for k in range(1, count):
                total = total + wide[base + k : base + k + length, placed] * weights[k : k + 1, :]
            total = total * (1.0 / (1.0 + jnp.exp(-total)))
            if first == 0:
                values[:, at] = total
                value_low[:, at] = total.astype(bf16)
            else:
                keyquery[:, first - inner + start : first - inner + start + chunk] = total.astype(bf16)

    weighted = (values[...] * end_scale).astype(bf16)
    for g in range(groups):
        keys = keyquery[:, g * STATE : (g + 1) * STATE]
        made = contract(keys, weighted[:, g * group_width : (g + 1) * group_width], ((0,), (0,)))
        for part in range(group_width // slice_width):
            place = g * (group_width // slice_width) + part
            state_out[place, 0:STATE, :] = made[
                :, part * slice_width : (part + 1) * slice_width
            ].astype(bf16)
    high = whole_decay.astype(bf16)
    low = (whole_decay - high.astype(f32)).astype(bf16)
    first_row = lax.broadcasted_iota(jnp.int32, whole_decay.shape, 0) == 0
    packed = jnp.where(first_row, high.astype(f32), low.astype(f32)).astype(bf16)
    for place in range(team):
        state_out[place, STATE : STATE + 16, :] = packed[
            :, place * slice_width : (place + 1) * slice_width
        ]
    state_in[me] = state_out[me]
    state_copies = []
    for step in range(1, team):
        target = mate(step)
        state_copies.append(
            copy(
                state_out.at[lax.rem(target, team)],
                state_in.at[me],
                st_ss.at[step],
                st_rs.at[me],
                target,
                tp,
            )
        )
        state_copies[-1].start()
    for kind, step, where in batches[1]:
        (weight_near if where == 0 else weight_far)(kind, step).start()

    causal = row_index >= column_index
    causal_pair = jnp.concatenate([causal, causal], axis=1)
    lane = lax.broadcasted_iota(jnp.int32, (length, 2 * HEAD_DIM), 1)
    pairs_per_group = group_width // (2 * HEAD_DIM)
    for g in range(groups):
        keys = keyquery[:, g * STATE : (g + 1) * STATE]
        queries = keyquery[:, state_width + g * STATE : state_width + (g + 1) * STATE]
        scores = contract(queries, keys, ((1,), (1,)))
        scores = jnp.concatenate([scores, scores], axis=1)
        for j in range(pairs_per_group):
            i = g * pairs_per_group + j
            rows = jnp.concatenate(
                [row_decay[2 * i : 2 * i + 1, :], row_decay[2 * i + 1 : 2 * i + 2, :]], axis=1
            )
            gap = column_decay[:, 2 * i * length : (2 * i + 2) * length] - rows
            decay = jnp.exp(jnp.where(causal_pair, gap, -jnp.inf))
            mixing = (scores * decay).astype(bf16)
            both = values[:, i * 2 * HEAD_DIM : (i + 1) * 2 * HEAD_DIM]
            blocks = jnp.concatenate(
                [jnp.where(lane < HEAD_DIM, both, 0.0), jnp.where(lane < HEAD_DIM, 0.0, both)],
                axis=0,
            ).astype(bf16)
            scan[:, i * 2 * HEAD_DIM : (i + 1) * 2 * HEAD_DIM] = contract(
                mixing, blocks, ((1,), (0,))
            )
    scan[...] = scan[...] + skip_scale[0:1, :] * values[...]

    carried = jnp.zeros((STATE, slice_width), f32)
    kept = jnp.ones((1, slice_width), f32)
    for step in range(1, team):
        source = lax.rem(me + step, team)
        copy(
            state_in.at[source], state_in.at[source], st_ss.at[step], st_rs.at[source], sp, tp
        ).wait_recv()
    for place in range(team):
        entering[place] = carried
        kept_decay[place] = jnp.broadcast_to(kept, (8, slice_width))
        tail = state_in[place, STATE : STATE + 16, :].astype(f32)
        factor = tail[0:1, :] + tail[1:2, :]
        carried = carried * factor + state_in[place, 0:STATE, :].astype(f32)
        kept = kept * factor
    cross_out[...] = carried.astype(bf16)
    cross = copy(
        cross_out, cross_in, cr_ss, cr_rs, (1 - own_team) * team + me, tp
    )
    cross.start()
    for kind, step, where in batches[2]:
        (weight_near if where == 0 else weight_far)(kind, step).start()
    cross.wait_recv()
    earlier = jnp.where(own_team > 0, cross_in[...].astype(f32), 0.0)
    for place in range(team):
        back_out[place] = (entering[place] + kept_decay[place, 0:1, :] * earlier).astype(bf16)
    back_in[me] = back_out[me]
    back_copies = []
    for step in range(1, team):
        target = mate(step)
        back_copies.append(
            copy(
                back_out.at[lax.rem(target, team)],
                back_in.at[me],
                bk_ss.at[step],
                bk_rs.at[me],
                target,
                tp,
            )
        )
        back_copies[-1].start()
    for kind, step, where in batches[3]:
        (weight_near if where == 0 else weight_far)(kind, step).start()
    for step in range(1, team):
        source = lax.rem(me + step, team)
        copy(
            back_in.at[source], back_in.at[source], bk_ss.at[step], bk_rs.at[source], sp, tp
        ).wait_recv()

    for g in range(groups):
        queries = keyquery[:, state_width + g * STATE : state_width + (g + 1) * STATE]
        at = slice(g * group_width, (g + 1) * group_width)
        per = group_width // slice_width
        incoming = jnp.concatenate([back_in[g * per + part] for part in range(per)], axis=1)
        arriving = contract(queries, incoming, ((1,), (0,))) * scale_in[:, at]
        gate = multiplier_ref[:, at].astype(f32)
        gated = (scan[:, at] + arriving) * (gate * (1.0 / (1.0 + jnp.exp(-gate))))
        gated = gated * lax.rsqrt(jnp.mean(gated * gated, axis=1, keepdims=True) + epsilon)
        heads[:, at] = (gated * cluster_gain[:, at]).astype(bf16)

    local_blend.wait()
    column_chunk = 512

    def project(index, carry):
        at = pl.ds(pl.multiple_of(index * column_chunk, column_chunk), column_chunk)
        product = contract(heads[...], blend[:, at], ((1,), (0,))).astype(bf16)
        part_out[0, :, at] = product[0:rows_own, :]
        part_out[1, :, at] = product[rows_own:, :]
        return carry

    lax.fori_loop(0, model // column_chunk, project, 0)
    swap = copy(part_out.at[1 - tp], part_in, pt_ss, pt_rs, sp, 1 - tp)
    swap.start()
    swap.wait_recv()
    mixed = (part_out[tp].astype(f32) + part_in[...].astype(f32)).astype(bf16)
    state = (skip_ref[...].astype(f32) + mixed.astype(f32)).astype(bf16)
    state_rows[...] = state
    state = state.astype(f32)
    state = state * lax.rsqrt(jnp.mean(state * state, axis=1, keepdims=True) + epsilon)
    acts[tp, me] = (state * feature_gain[...]).astype(bf16)

    opposite = flip(me, half)
    base = own_team * team
    plane_first = me - lax.rem(me, half)
    in_plane = [plane_first + lax.rem(me + k, half) for k in range(half)]
    far_plane = [flip(index, half) for index in in_plane]
    deep = copy(acts.at[tp, me], acts.at[tp, me], az_ss, az_rs, base + opposite, tp)
    deep.start()
    near_copies = []
    for k in range(1, half):
        near_copies.append(
            copy(acts.at[tp, me], acts.at[tp, me], ap_ss.at[k], ap_rs.at[me], base + in_plane[k], tp)
        )
        near_copies[-1].start()
    side_copies = [copy(acts.at[tp, me], acts.at[tp, me], ad_ss.at[me], ad_rs.at[me], sp, 1 - tp)]
    side_copies[-1].start()
    for kind, step, where in batches[4]:
        (weight_near if where == 0 else weight_far)(kind, step).start()

    def arrived(place, sems):
        return copy(acts.at[tp, place], acts.at[tp, place], az_ss, sems, sp, tp)

    arrived(opposite, az_rs).wait_recv()
    for k in range(1, half):
        near_copies.append(
            copy(
                acts.at[tp, opposite],
                acts.at[tp, opposite],
                ap_ss.at[half + k],
                ap_rs.at[opposite],
                base + in_plane[k],
                tp,
            )
        )
        near_copies[-1].start()
    side_copies.append(
        copy(acts.at[tp, opposite], acts.at[tp, opposite], ad_ss.at[opposite], ad_rs.at[opposite], sp, 1 - tp)
    )
    side_copies[-1].start()
    for kind, step, where in batches[5]:
        (weight_near if where == 0 else weight_far)(kind, step).start()
    for k in range(1, half):
        for place in (in_plane[k], far_plane[k]):
            arrived(place, ap_rs.at[place]).wait_recv()
            side_copies.append(
                copy(acts.at[tp, place], acts.at[tp, place], ad_ss.at[place], ad_rs.at[place], sp, 1 - tp)
            )
            side_copies[-1].start()
    for place in range(team):
        copy(
            acts.at[1 - tp, place], acts.at[1 - tp, place], ad_ss.at[place], ad_rs.at[place], sp, 1 - tp
        ).wait_recv()

    local_up.wait()
    for step in range(1, shards):
        source = lax.rem(sp + step, shards)
        copy(up.at[source], up.at[source], up_ss.at[step - 1], up_rs.at[source], sp, tp).wait_recv()
    up_whole = (shards * up.shape[1], unit)

    def lift(index, carry):
        core, block = index // 4, lax.rem(index, 4)
        count = team // 4
        rows = acts[core, pl.ds(block * count, count)].reshape(count * rows_own, model)
        lifted = jnp.maximum(contract(rows, up[...].reshape(up_whole), ((1,), (0,))), 0.0)
        at = pl.ds(pl.multiple_of(block * count * rows_own, count * rows_own), count * rows_own)
        hidden[core, at, :] = (lifted * lifted).astype(bf16)
        return carry

    lax.fori_loop(0, 8, lift, 0)

    local_down.wait()
    lanes = down.shape[2]

    def pair_sources(t):
        first = lax.rem(2 * t + own_team * team, shards)
        return first, first + 1

    def pair_copy(t):
        return copy(pair_out.at[t], pair_in.at[t], pr_ss.at[t], pr_rs.at[t], sp, 1 - tp)

    def plane_copy(t, k):
        return copy(
            plane_out.at[t, pl.ds(0, 2), in_plane_slot(k)],
            plane_in.at[t, k],
            pl_ss.at[t, k],
            pl_rs.at[t, k],
            base + in_plane[k],
            tp,
        )

    def in_plane_slot(k):
        return lax.rem(me + k, half)

    def depth_copy(t):
        return copy(depth_out.at[t], depth_in.at[t], dp_ss.at[t], dp_rs.at[t], base + opposite, tp)

    def lower_step(t):
        sources = pair_sources(t)
        for source in sources:

            @pl.when(source != sp)
            def _():
                copy(
                    down.at[source], down.at[source], down_ss.at[0], down_rs.at[source], sp, tp
                ).wait_recv()

        both = jnp.concatenate([down[sources[0]], down[sources[1]]], axis=1)
        pair_out[t] = contract(hidden[1 - tp], both, ((1,), (0,))).astype(bf16)
        pair_copy(t).start()
        plane_sum = contract(hidden[tp], both, ((1,), (0,)))
        plane_out[t] = plane_sum.astype(bf16).reshape(2, half, rows_own, 2 * lanes)

    def pair_step(t):
        pair_copy(t).wait_recv()
        summed = plane_out[t].astype(f32) + pair_in[t].reshape(
            2, half, rows_own, 2 * lanes
        ).astype(f32)
        plane_out[t] = summed.astype(bf16)
        for k in range(1, half):
            plane_copy(t, k).start()

    def plane_step(t):
        summed = plane_out[t, :, lax.rem(me, half)].astype(f32)
        for k in range(1, half):
            plane_copy(t, k).wait_recv()
            summed = summed + plane_in[t, k].astype(f32)
        side = me // half
        plane_out[t, :, lax.rem(me, half)] = summed.astype(bf16)
        depth_out[t] = plane_out[t, 1 - side, lax.rem(me, half)]
        depth_copy(t).start()

    def depth_step(t):
        depth_copy(t).wait_recv()
        side = me // half
        summed = plane_out[t, side, lax.rem(me, half)].astype(f32) + depth_in[t].astype(f32)
        summed = summed.astype(bf16).astype(f32)
        for place, source in enumerate(pair_sources(t)):
            at = pl.ds(pl.multiple_of(source * lanes, lanes), lanes)
            total = state_rows[:, at].astype(f32) + summed[:, place * lanes : (place + 1) * lanes]
            out_ref[:, at] = total.astype(bf16)

    count = shards // 2

    def stage(t, carry):
        @pl.when(t < count)
        def _():
            lower_step(t)

        @pl.when((t >= 1) & (t < count + 1))
        def _():
            pair_step(t - 1)

        @pl.when((t >= 2) & (t < count + 2))
        def _():
            plane_step(t - 2)

        @pl.when(t >= 3)
        def _():
            depth_step(t - 3)

        return carry

    lax.fori_loop(0, count + 3, stage, 0)

    for one in halo_copies + state_copies + back_copies + near_copies + side_copies:
        one.wait_send()
    for one in (cross, swap, deep):
        one.wait_send()
    for kind in range(2):
        for step in range(1, team):
            weight_near(kind, step).wait_send()
        for step in range(team):
            weight_far(kind, step).wait_send()

    def drain(t, carry):
        pair_copy(t).wait_send()
        depth_copy(t).wait_send()
        for k in range(1, half):
            plane_copy(t, k).wait_send()
        return carry

    lax.fori_loop(0, count, drain, 0)


def plan(team):
    ups_far = [(0, step, 1) for step in range(team)]
    downs_far = [(1, step, 1) for step in range(team)]
    ups_near = [(0, step, 0) for step in range(1, team)]
    downs_near = [(1, step, 0) for step in range(1, team)]
    a, b = team // 4, team // 2
    return (
        ups_far[:a] + ups_near[:a],
        ups_far[a : 2 * a] + ups_near[a : 2 * a],
        ups_far[2 * a : 2 * a + 1] + ups_near[2 * a : 2 * a + 1],
        ups_far[2 * a + 1 : 3 * a] + ups_near[2 * a + 1 : 3 * a],
        ups_far[3 * a :] + ups_near[3 * a :],
        downs_near + downs_far,
    )


def per_device_fused(team, *operands):
    (
        skip_stream_entering,
        content_signal_matrix,
        writer_signal_matrix,
        reader_signal_matrix,
        multiplier_signal,
        interval_before_softplus,
        extra_log_shrink,
        log_forget_speed,
        content_filter_coefs,
        writer_filter_coefs,
        reader_filter_coefs,
        skip_path_factor,
        cluster_scaling_vector,
        blend_result_matrix,
        feature_blend_scaling,
        widening_matrix,
        narrowing_matrix,
    ) = operands
    f32, bf16 = jnp.float32, jnp.bfloat16
    shards = lax.axis_size("sp")
    length, inner = content_signal_matrix.shape
    state_width = writer_signal_matrix.shape[1]
    local_heads = interval_before_softplus.shape[0]
    rows_own, model = skip_stream_entering.shape
    unit = widening_matrix.shape[1] // team
    depth = widening_matrix.shape[0]
    lanes = narrowing_matrix.shape[1]
    slice_width = inner // team
    half, pairs = team // 2, shards // 2
    dma = pltpu.SemaphoreType.DMA
    vmem, anywhere = pl.BlockSpec(memory_space=pltpu.VMEM), pl.BlockSpec(memory_space=pl.ANY)
    specs = [vmem] * 13 + [anywhere, vmem, anywhere, anywhere]
    scratch = [
        pltpu.VMEM((16, inner + 2 * state_width), bf16),
        pltpu.VMEM((8 + length, inner + 2 * state_width), f32),
        pltpu.VMEM((length, inner), f32),
        pltpu.VMEM((length, inner), bf16),
        pltpu.VMEM((length, 2 * state_width), bf16),
        pltpu.VMEM(blend_result_matrix.shape, bf16),
        pltpu.VMEM((shards, depth, unit), bf16),
        pltpu.VMEM((shards, unit, lanes), bf16),
        pltpu.VMEM((length, local_heads * length), f32),
        pltpu.VMEM((local_heads, length), f32),
        pltpu.VMEM((length, inner), f32),
        pltpu.VMEM((length, inner), f32),
        pltpu.VMEM((team, STATE + 16, slice_width), bf16),
        pltpu.VMEM((team, STATE + 16, slice_width), bf16),
        pltpu.VMEM((team, STATE, slice_width), f32),
        pltpu.VMEM((team, 8, slice_width), f32),
        pltpu.VMEM((STATE, slice_width), bf16),
        pltpu.VMEM((STATE, slice_width), bf16),
        pltpu.VMEM((team, STATE, slice_width), bf16),
        pltpu.VMEM((team, STATE, slice_width), bf16),
        pltpu.VMEM((length, inner), bf16),
        pltpu.VMEM((2, rows_own, model), bf16),
        pltpu.VMEM((rows_own, model), bf16),
        pltpu.VMEM((rows_own, model), bf16),
        pltpu.VMEM((2, team, rows_own, model), bf16),
        pltpu.VMEM((2, team * rows_own, unit), bf16),
        pltpu.VMEM((pairs, team * rows_own, 2 * lanes), bf16),
        pltpu.VMEM((pairs, team * rows_own, 2 * lanes), bf16),
        pltpu.VMEM((pairs, 2, half, rows_own, 2 * lanes), bf16),
        pltpu.VMEM((pairs, half, 2, rows_own, 2 * lanes), bf16),
        pltpu.VMEM((pairs, rows_own, 2 * lanes), bf16),
        pltpu.VMEM((pairs, rows_own, 2 * lanes), bf16),
        dma((3,)),
        dma((3,)),
        dma((3,)),
        dma((shards,)),
        dma((shards,)),
        dma((shards,)),
        dma((shards,)),
        dma((team,)),
        dma((team,)),
        dma,
        dma,
        dma((team,)),
        dma((team,)),
        dma,
        dma,
        dma,
        dma,
        dma((team,)),
        dma((team,)),
        dma((team,)),
        dma((team,)),
        dma((pairs,)),
        dma((pairs,)),
        dma((pairs, half)),
        dma((pairs, half)),
        dma((pairs,)),
        dma((pairs,)),
    ]
    return pl.pallas_call(
        functools.partial(layer_kernel, team),
        out_shape=jax.ShapeDtypeStruct((rows_own, model), bf16),
        in_specs=specs,
        out_specs=vmem,
        scratch_shapes=scratch,
        compiler_params=pltpu.CompilerParams(
            collective_id=0, has_side_effects=True, vmem_limit_bytes=63 * 1024 * 1024
        ),
    )(
        skip_stream_entering,
        content_signal_matrix,
        writer_signal_matrix,
        reader_signal_matrix,
        multiplier_signal,
        interval_before_softplus,
        extra_log_shrink,
        log_forget_speed.reshape(-1, 1),
        content_filter_coefs,
        writer_filter_coefs,
        reader_filter_coefs,
        skip_path_factor.reshape(1, -1),
        cluster_scaling_vector.reshape(1, -1),
        blend_result_matrix,
        feature_blend_scaling.reshape(1, -1),
        widening_matrix,
        narrowing_matrix,
    )


def general_solution(mesh):
    shards, halves = mesh.shape["sp"], mesh.shape["tp"]
    team = math.gcd(shards, TEAM)
    teams = jax.sharding.Mesh(
        mesh.devices.reshape(shards // team, team, halves), ("sa", "sb", "tp")
    )
    placed = (
        P(("sa", "sb", "tp"), None),
        P(SP, "tp"),
        P(SP, "tp"),
        P(SP, "tp"),
        P(SP, "tp"),
        P("tp", SP),
        P("tp", SP),
        P("tp"),
        P(None, "tp"),
        P(None, "tp"),
        P(None, "tp"),
        P("tp"),
        P("tp"),
        P("tp", None),
        P(),
        P(SP, "tp"),
        P("tp", SP),
    )
    return jax.shard_map(
        per_device, mesh=teams, in_specs=placed, out_specs=P(("sa", "sb", "tp"), None), check_vma=False
    )


def fits(shards, halves, team, rows, tokens, inner, hidden, model, state_width):
    length = tokens // shards
    local = inner // halves
    return (
        halves == 2
        and shards == 2 * team
        and team % 4 == 0
        and length == BLOCK
        and length % 32 == 0
        and local % (team * 128) == 0
        and (hidden // halves) % (team * 128) == 0
        and model % (shards * 128) == 0
        and (state_width // halves) % STATE == 0
        and (local // (state_width // halves // STATE)) % (local // team) == 0
    )


def solution(mesh):
    shards, halves = mesh.shape["sp"], mesh.shape["tp"]
    team = math.gcd(shards, TEAM)
    general = general_solution(mesh)
    row, both = P("sp", "tp"), P(("sp", "tp"), None)
    tp_first, tp_last, tp_only = P("tp", "sp"), P(None, "tp"), P("tp")
    placed = (
        (both, row, row, row, row, tp_first, tp_first, tp_only, tp_last, tp_last, tp_last)
        + (tp_only, tp_only, P("tp", None), P(), row, tp_first)
    )
    fused = jax.shard_map(
        functools.partial(per_device_fused, team),
        mesh=mesh,
        in_specs=placed,
        out_specs=both,
        check_vma=False,
    )

    def layer(*operands):
        tokens, inner = operands[1].shape
        model, hidden = operands[15].shape
        state_width = operands[2].shape[1]
        if fits(shards, halves, team, tokens, tokens, inner, hidden, model, state_width):
            return fused(*operands)
        return general(*operands)

    return layer
```

```python
import functools
import math
import jax
import jax.numpy as jnp
from jax import lax
from jax.experimental import pallas as pl
from jax.experimental.pallas import tpu as pltpu
from jax.sharding import PartitionSpec as P

HEAD_DIM = 64
STATE = 128
BLOCK = 128


epsilon = 1e-05
precise = lax.Precision.HIGHEST
SP = ("sa", "sb")
TEAM = 8


def shifted(value, axis, steps):
    count = lax.axis_size(axis)
    initial, last = (max(0, -steps), min(count, count - steps))
    return lax.ppermute(value, axis, [(source, source + steps) for source in range(initial, last)])


def scan_rows(parts, factors, entering):
    def one(place, carried):
        entering[place] = carried.astype(jnp.bfloat16)
        return carried * factors[place] + parts[place].astype(jnp.float32)

    lax.fori_loop(0, parts.shape[0], one, jnp.zeros(parts.shape[1:], jnp.float32))


def prefix(log_total, end_state, rider):
    shards = lax.axis_size(SP)
    heads = end_state.shape[0] * end_state.shape[1]
    state_width = end_state.shape[-1]
    rows = end_state.reshape(-1, state_width).astype(jnp.bfloat16)
    count = rows.shape[0] // shards
    decays = jnp.repeat(jnp.exp(log_total).reshape(heads), rows.shape[0] // heads)
    extra = -(-count // state_width) * 16
    decays = decays.astype(jnp.bfloat16).reshape(shards, count)
    decays = jnp.pad(decays, ((0, 0), (0, extra * state_width - count)))
    packed = jnp.concatenate(
        [rows.reshape(shards, count, state_width), decays.reshape(shards, extra, state_width)],
        axis=1,
    )
    packed = lax.all_to_all(packed, SP, split_axis=0, concat_axis=0)
    parts = packed[:, :count]
    factors = packed[:, count:].reshape(shards, -1)[:, :count].astype(jnp.float32)
    entering = pl.pallas_call(
        scan_rows,
        out_shape=jax.ShapeDtypeStruct(parts.shape, jnp.bfloat16),
    )(parts, jnp.broadcast_to(factors[..., None], parts.shape))
    entering, rider = lax.optimization_barrier((entering, rider))
    back = lax.all_to_all(
        entering.reshape(rows.shape), SP, split_axis=0, concat_axis=0, tiled=True
    )
    return back.reshape(end_state.shape).astype(jnp.float32), rider


def summed_share(partial, axis):
    count = lax.axis_size(axis)
    if count != 2:
        return lax.psum_scatter(partial, axis, scatter_dimension=0, tiled=True)
    me = lax.axis_index(axis)
    length = partial.shape[0] // 2
    away = lax.dynamic_slice_in_dim(partial, (1 - me) * length, length, 0)
    kept = lax.dynamic_slice_in_dim(partial, me * length, length, 0)
    arrived = lax.ppermute(away, axis, [(0, 1), (1, 0)])
    return (kept.astype(jnp.float32) + arrived.astype(jnp.float32)).astype(jnp.bfloat16)


def convolve(inputs, rim_rows, conv_taps):
    width = conv_taps.shape[0]
    length = inputs.shape[0]
    extended = jnp.concatenate([rim_rows, inputs], axis=0)
    summed = extended[0:length].astype(jnp.float32) * conv_taps[0].astype(jnp.float32)
    for offset in range(1, width):
        summed = summed + extended[offset : offset + length].astype(jnp.float32) * conv_taps[
            offset
        ].astype(jnp.float32)
    return jax.nn.silu(summed)


def advance(carried, pair):
    block_state, block_factor = pair
    return (carried * block_factor[..., None, None] + block_state, carried)


def blockwise(values, interval_lengths, log_forgetting, key_rows, query_rows):
    length, groups, per_group, width = values.shape
    blocks = length // BLOCK
    value_blocks = values.reshape(blocks, BLOCK, groups, per_group, width)
    step_blocks = jnp.transpose(
        interval_lengths.reshape(groups, per_group, blocks, BLOCK), (2, 3, 0, 1)
    )
    weighted = value_blocks * step_blocks[..., None]
    cumulative = jnp.cumsum(
        jnp.transpose(log_forgetting.reshape(groups, per_group, blocks, BLOCK), (2, 0, 1, 3)),
        axis=-1,
    )
    key_blocks = key_rows.reshape(blocks, BLOCK, groups, -1)
    query_blocks = query_rows.reshape(blocks, BLOCK, groups, -1)
    causal = jnp.tril(jnp.ones((BLOCK, BLOCK), dtype=bool))
    decay_mask = jnp.exp(
        jnp.where(causal, cumulative[..., :, None] - cumulative[..., None, :], -jnp.inf)
    )
    scores = jnp.einsum("clgn,csgn->cgls", query_blocks, key_blocks, precision=precise)
    within = jnp.einsum("cgls,cgrls,csgrp->clgrp", scores, decay_mask, weighted, precision=precise)
    to_end = jnp.exp(cumulative[..., -1:] - cumulative)
    states = jnp.einsum("clgn,cgrl,clgrp->cgrpn", key_blocks, to_end, weighted, precision=precise)
    block_totals = cumulative[..., -1]
    initial = jnp.zeros(states.shape[1:], jnp.float32)
    final, entering = lax.scan(advance, initial, (states, jnp.exp(block_totals)))
    carried = jnp.einsum(
        "clgn,cgrpn,cgrl->clgrp", query_blocks, entering, jnp.exp(cumulative), precision=precise
    )
    from_start = (jnp.cumsum(block_totals, axis=0) - block_totals)[..., None] + cumulative
    return (within + carried, final, from_start, jnp.sum(block_totals, axis=0))


def normalize(rows, gain):
    widened = rows.astype(jnp.float32)
    scaled = widened * lax.rsqrt(jnp.mean(widened * widened, axis=-1, keepdims=True) + epsilon)
    return (scaled * gain).astype(jnp.bfloat16)


def per_device(
    skip_stream_entering,
    content_signal_matrix,
    writer_signal_matrix,
    reader_signal_matrix,
    multiplier_signal,
    interval_before_softplus,
    extra_log_shrink,
    log_forget_speed,
    content_filter_coefs,
    writer_filter_coefs,
    reader_filter_coefs,
    skip_path_factor,
    cluster_scaling_vector,
    blend_result_matrix,
    feature_blend_scaling,
    widening_matrix,
    narrowing_matrix,
):
    up_part = lax.all_to_all(widening_matrix, "sb", split_axis=1, concat_axis=0, tiled=True)
    narrowing_matrix, up_part = lax.optimization_barrier((narrowing_matrix, up_part))
    up_use = lax.all_gather(up_part, "sa", axis=0, tiled=True)
    down_part = lax.all_to_all(narrowing_matrix, "sb", split_axis=0, concat_axis=1, tiled=True)
    (
        content_signal_matrix,
        writer_signal_matrix,
        reader_signal_matrix,
        interval_before_softplus,
        down_part,
    ) = lax.optimization_barrier(
        (
            content_signal_matrix,
            writer_signal_matrix,
            reader_signal_matrix,
            interval_before_softplus,
            down_part,
        )
    )
    down_use = lax.all_gather(down_part, "sa")
    rim_width = content_filter_coefs.shape[0] - 1
    length = content_signal_matrix.shape[0]
    signals = (content_signal_matrix, writer_signal_matrix, reader_signal_matrix)
    tails = jnp.concatenate([signal[length - rim_width :] for signal in signals], axis=1)
    rims = shifted(tails, SP, 1)
    first, second = signals[0].shape[1], signals[0].shape[1] + signals[1].shape[1]
    values = convolve(signals[0], rims[:, :first], content_filter_coefs)
    key_rows = convolve(signals[1], rims[:, first:second], writer_filter_coefs)
    query_rows = convolve(signals[2], rims[:, second:], reader_filter_coefs)
    local_heads = interval_before_softplus.shape[0]
    local_groups = writer_signal_matrix.shape[1] // STATE
    per_group = local_heads // local_groups
    interval_lengths = jax.nn.softplus(interval_before_softplus)
    log_forgetting = extra_log_shrink - jnp.exp(log_forget_speed)[:, None] * interval_lengths
    shaped = values.reshape(length, local_groups, per_group, HEAD_DIM)
    local_out, end_state, from_start, device_total = blockwise(
        shaped,
        interval_lengths.reshape(local_groups, per_group, length),
        log_forgetting.reshape(local_groups, per_group, length),
        key_rows,
        query_rows,
    )
    incoming, up_use = prefix(device_total, end_state, up_use)
    query_blocks = query_rows.reshape(length // BLOCK, BLOCK, local_groups, STATE)
    arriving = jnp.einsum(
        "clgn,grpn,cgrl->clgrp", query_blocks, incoming, jnp.exp(from_start), precision=precise
    )
    scan_out = (local_out + arriving).reshape(length, local_heads * HEAD_DIM)
    gated = (scan_out + jnp.repeat(skip_path_factor, HEAD_DIM) * values) * jax.nn.silu(
        multiplier_signal.astype(jnp.float32)
    )
    grouped = gated.reshape(length, local_groups, -1)
    grouped = grouped * lax.rsqrt(jnp.mean(grouped * grouped, axis=-1, keepdims=True) + epsilon)
    heads_out = (grouped.reshape(length, -1) * cluster_scaling_vector).astype(jnp.bfloat16)
    mixer_rows = summed_share(
        jnp.dot(heads_out, blend_result_matrix, preferred_element_type=jnp.float32).astype(
            jnp.bfloat16
        ),
        "tp",
    )
    own_rows = (skip_stream_entering.astype(jnp.float32) + mixer_rows.astype(jnp.float32)).astype(
        jnp.bfloat16
    )
    normed = normalize(own_rows, feature_blend_scaling)
    down_whole = jnp.concatenate([down_use[k] for k in range(down_use.shape[0])], axis=1)

    def mixed(rows):
        lifted = jax.nn.relu(jnp.dot(rows, up_use, preferred_element_type=jnp.float32))
        hidden = (lifted * lifted).astype(jnp.bfloat16)
        partial = jnp.dot(hidden, down_whole, preferred_element_type=jnp.float32)
        return partial.astype(jnp.bfloat16)

    if lax.axis_size("tp") == 2:
        members, width = lax.axis_size("sb"), normed.shape[1]
        swap = [(0, 1), (1, 0)]
        copies = jnp.broadcast_to(normed[None], (members,) + normed.shape)
        own_half = lax.all_to_all(copies, "sb", split_axis=0, concat_axis=0)
        own_half = own_half.reshape(-1, width)
        other_half = lax.ppermute(own_half, "tp", swap)
        arrived = lax.ppermute(mixed(other_half), "tp", swap)
        joined = mixed(own_half).astype(jnp.float32) + arrived.astype(jnp.float32)
        joined = joined.astype(jnp.bfloat16).reshape(members, -1, width)
        shares = lax.all_to_all(joined, "sb", split_axis=0, concat_axis=0)
        mlp_rows = jnp.sum(shares.astype(jnp.float32), axis=0)
    else:
        team_rows = lax.all_gather(normed, ("sb", "tp"), axis=0, tiled=True)
        mlp_rows = lax.psum_scatter(
            mixed(team_rows), ("sb", "tp"), scatter_dimension=0, tiled=True
        )
    mlp_rows = mlp_rows.astype(jnp.bfloat16)
    return (own_rows.astype(jnp.float32) + mlp_rows.astype(jnp.float32)).astype(jnp.bfloat16)


TEAM_LINKS = pl.DeviceIdType.MESH


def split3(wide):
    one = wide.astype(jnp.bfloat16)
    rest = wide - one.astype(jnp.float32)
    two = rest.astype(jnp.bfloat16)
    return one, two, (rest - two.astype(jnp.float32)).astype(jnp.bfloat16)


def contract(left, right, dims):
    return lax.dot_general(left, right, (dims, ((), ())), preferred_element_type=jnp.float32)


def exact(left, right, dims, left_split):
    if left_split:
        terms = [contract(part, right, dims) for part in split3(left)]
    else:
        terms = [contract(left, part, dims) for part in split3(right)]
    return terms[0] + terms[1] + terms[2]


def selector(rows, columns, per_row):
    row = lax.broadcasted_iota(jnp.int32, (rows, columns), 0)
    column = lax.broadcasted_iota(jnp.int32, (rows, columns), 1)
    return jnp.where(column // per_row == row, 1.0, 0.0).astype(jnp.bfloat16)


def layer_kernel(
    team,
    skip_ref,
    content_ref,
    writer_ref,
    reader_ref,
    multiplier_ref,
    interval_ref,
    shrink_ref,
    speed_ref,
    content_taps,
    writer_taps,
    reader_taps,
    skip_factor,
    cluster_gain,
    blend_hbm,
    feature_gain,
    up_hbm,
    down_hbm,
    out_ref,
    halo,
    wide,
    values,
    keyquery,
    blend,
    up,
    down,
    column_decay,
    row_decay,
    scan,
    scale_in,
    state_out,
    state_in,
    entering,
    kept_decay,
    cross_out,
    cross_in,
    back_out,
    back_in,
    heads,
    part_out,
    part_in,
    state_rows,
    acts,
    hidden,
    pair_out,
    pair_in,
    plane_out,
    depth_in,
    local_sem,
    halo_ss,
    halo_rs,
    up_ss,
    up_rs,
    down_ss,
    down_rs,
    st_ss,
    st_rs,
    cr_ss,
    cr_rs,
    bk_ss,
    bk_rs,
    pt_ss,
    pt_rs,
    ap_ss,
    ap_rs,
    ad_ss,
    ad_rs,
    pr_ss,
    pr_rs,
    dp_ss,
    dp_rs,
):
    f32, bf16 = jnp.float32, jnp.bfloat16
    batches = plan(lax.axis_size("sp") // 4)
    shards = lax.axis_size("sp")
    sp, tp = lax.axis_index("sp"), lax.axis_index("tp")
    own_team, me = sp // team, lax.rem(sp, team)
    length, inner = content_ref.shape
    state_width = writer_ref.shape[1]
    local_heads = interval_ref.shape[0]
    groups = state_width // STATE
    group_width = inner // groups
    model = skip_ref.shape[1]
    unit = up.shape[2]
    slice_width = inner // team
    half = team // 2
    rows_own = skip_ref.shape[0]

    open_scope = []

    def phase(name):
        if open_scope:
            open_scope.pop().__exit__(None, None, None)
        if name:
            open_scope.append(jax.named_scope(name))
            open_scope[-1].__enter__()

    def copy(src, dst, ss, rs, sp_to, tp_to):
        return pltpu.make_async_remote_copy(
            src_ref=src,
            dst_ref=dst,
            send_sem=ss,
            recv_sem=rs,
            device_id=(sp_to, tp_to),
            device_id_type=TEAM_LINKS,
        )

    def mate(step):
        return own_team * team + lax.rem(me + step, team)

    level, spot = sp // 4, lax.rem(sp, 4)
    beside = (spot + 1 - 2 * lax.rem(spot, 2), lax.rem(spot + 2, 4))
    levels = shards // 4

    def level_at(step):
        return lax.rem(level + levels + step, levels)

    def weight_piece(kind, index):
        offset = pl.ds(pl.multiple_of(index * unit, unit), unit)
        return up_hbm.at[:, offset] if kind == 0 else down_hbm.at[offset, :]

    def weight_copy(kind, src, source, place, target):
        into, ss, rs = ((up, up_ss, up_rs), (down, down_ss, down_rs))[kind]
        if src is None:
            src = into.at[source]
        return copy(src, into.at[source], ss.at[place], rs.at[source], target, tp)

    def source_level(step):
        if step == 0:
            return level
        return step - 1 + jnp.where(level <= step - 1, 1, 0)

    def rise(kind, step):
        to = level_at(step)
        return weight_copy(kind, weight_piece(kind, to), sp, step, to * 4 + spot)

    def first_pass(kind, step):
        source = source_level(step) * 4 + spot
        piece = weight_piece(kind, level) if step == 0 else None
        return weight_copy(kind, piece, source, 4 + step, level * 4 + beside[kind])

    def second_pass(kind, step, other):
        source = source_level(step) * 4 + (beside[kind] if other else spot)
        piece = weight_piece(kind, level) if step == 0 and not other else None
        place = 8 + step + (4 if other else 0)
        return weight_copy(kind, piece, source, place, level * 4 + beside[1 - kind])

    def issue(batch):
        for what, kind, step in batches.get(batch, ()):
            if what == "rise":
                rise(kind, step).start()
            if what == "first":
                if step:
                    first_pass(kind, step).wait_recv()
                first_pass(kind, step).start()
            if what == "own":
                second_pass(kind, step, False).start()
            if what == "other":
                second_pass(kind, step, True).wait_recv()
                second_pass(kind, step, True).start()

    local_up = pltpu.make_async_copy(weight_piece(0, level), up.at[sp], local_sem.at[0])
    local_down = pltpu.make_async_copy(weight_piece(1, level), down.at[sp], local_sem.at[1])
    local_blend = pltpu.make_async_copy(blend_hbm, blend, local_sem.at[2])
    local_up.start()
    local_down.start()
    local_blend.start()

    barrier = pltpu.get_barrier_semaphore()
    for step in range(1, shards):
        pl.semaphore_signal(
            barrier,
            inc=1,
            device_id=(lax.rem(sp + step, shards), tp),
            device_id_type=TEAM_LINKS,
        )
    pl.semaphore_signal(barrier, inc=1, device_id=(sp, 1 - tp), device_id_type=TEAM_LINKS)

    phase("decays")
    steps = interval_ref[...]
    steps = jnp.maximum(steps, 0.0) + jnp.log1p(jnp.exp(-jnp.abs(steps)))
    head_row = lax.broadcasted_iota(jnp.int32, (local_heads, local_heads), 0)
    head_column = lax.broadcasted_iota(jnp.int32, (local_heads, local_heads), 1)
    speed = jnp.where(head_row == head_column, speed_ref[...], 0.0)
    forget = shrink_ref[...] - jnp.exp(jnp.sum(speed, axis=1, keepdims=True)) * steps
    row_index = lax.broadcasted_iota(jnp.int32, (length, length), 0)
    column_index = lax.broadcasted_iota(jnp.int32, (length, length), 1)
    lower = jnp.where(row_index >= column_index, 1.0, 0.0).astype(bf16)
    upper = jnp.where(row_index <= column_index, 1.0, 0.0).astype(bf16)
    unity = jnp.where(row_index == column_index, 1.0, 0.0).astype(bf16)
    log_steps = jnp.log(steps)
    total_rows = exact(forget, upper, ((1,), (0,)), True)
    total_columns = exact(lower, forget, ((1,), (1,)), False)
    log_columns = exact(unity, log_steps, ((1,), (1,)), False)
    row_decay[...] = total_rows - log_steps
    by_head = selector(local_heads, local_heads * length, length)
    column_decay[...] = exact(total_columns, by_head, ((1,), (0,)), True)
    by_channel = selector(local_heads, inner, HEAD_DIM)
    scale_in[...] = exact(jnp.exp(total_columns), by_channel, ((1,), (0,)), True)
    last = total_columns[length - 1 : length, :]
    to_end = jnp.exp(last - total_columns + log_columns)
    end_scale = exact(to_end, by_channel, ((1,), (0,)), True)
    whole_decay = exact(
        jnp.broadcast_to(jnp.exp(last), (16, local_heads)), by_channel, ((1,), (0,)), True
    )
    skip_scale = exact(
        jnp.broadcast_to(skip_factor[...], (16, local_heads)), by_channel, ((1,), (0,)), True
    )

    phase("barrier_wait")
    pl.semaphore_wait(barrier, shards)
    phase("first_sends")
    following = lax.rem(sp + 1, shards)
    spans = ((content_ref, 0, inner), (writer_ref, inner, state_width))
    spans = spans + ((reader_ref, inner + state_width, state_width),)
    halo_copies = []
    for place, (ref, first, size) in enumerate(spans):
        halo_copies.append(
            copy(
                ref.at[pl.ds(length - 16, 16), :],
                halo.at[:, pl.ds(first, size)],
                halo_ss.at[place],
                halo_rs.at[place],
                following,
                tp,
            )
        )

    @pl.when(sp < shards - 1)
    def _():
        for one in halo_copies:
            one.start()

    issue(0)

    phase("rim_wait")
    @pl.when(sp > 0)
    def _():
        for one in halo_copies:
            one.wait_recv()

    @pl.when(sp == 0)
    def _():
        halo[...] = jnp.zeros_like(halo)

    phase("convolve")
    chunk = state_width
    for ref, taps, first, size in (
        (content_ref, content_taps, 0, inner),
        (writer_ref, writer_taps, inner, state_width),
        (reader_ref, reader_taps, inner + state_width, state_width),
    ):
        for start in range(0, size, chunk):
            at = slice(start, start + chunk)
            placed = slice(first + start, first + start + chunk)
            wide[8:, placed] = ref[:, at].astype(f32)
            wide[0:8, placed] = halo[:, placed].astype(f32)[8:, :]
            weights = taps[:, at].astype(f32)
            count = taps.shape[0]
            base = 8 - (count - 1)
            total = wide[base : base + length, placed] * weights[0:1, :]
            for k in range(1, count):
                total = total + wide[base + k : base + k + length, placed] * weights[k : k + 1, :]
            total = total * (1.0 / (1.0 + jnp.exp(-total)))
            if first == 0:
                values[:, at] = total
            else:
                keyquery[:, first - inner + start : first - inner + start + chunk] = total.astype(bf16)

    phase("states")
    weighted = (values[...] * end_scale).astype(bf16)
    for g in range(groups):
        keys = keyquery[:, g * STATE : (g + 1) * STATE]
        made = contract(keys, weighted[:, g * group_width : (g + 1) * group_width], ((0,), (0,)))
        for part in range(group_width // slice_width):
            place = g * (group_width // slice_width) + part
            state_out[place, 0:STATE, :] = made[
                :, part * slice_width : (part + 1) * slice_width
            ].astype(bf16)
    high = whole_decay.astype(bf16)
    low = (whole_decay - high.astype(f32)).astype(bf16)
    first_row = lax.broadcasted_iota(jnp.int32, whole_decay.shape, 0) == 0
    packed = jnp.where(first_row, high.astype(f32), low.astype(f32)).astype(bf16)
    for place in range(team):
        state_out[place, STATE : STATE + 16, :] = packed[
            :, place * slice_width : (place + 1) * slice_width
        ]
    state_in[me] = state_out[me]
    state_copies = []
    for step in range(1, team):
        target = mate(step)
        state_copies.append(
            copy(
                state_out.at[lax.rem(target, team)],
                state_in.at[me],
                st_ss.at[step],
                st_rs.at[me],
                target,
                tp,
            )
        )
        state_copies[-1].start()
    issue(1)

    phase("within")
    causal = row_index >= column_index
    causal_pair = jnp.concatenate([causal, causal], axis=1)
    lane = lax.broadcasted_iota(jnp.int32, (length, 2 * HEAD_DIM), 1)
    pairs_per_group = group_width // (2 * HEAD_DIM)
    for g in range(groups):
        keys = keyquery[:, g * STATE : (g + 1) * STATE]
        queries = keyquery[:, state_width + g * STATE : state_width + (g + 1) * STATE]
        scores = contract(queries, keys, ((1,), (1,)))
        scores = jnp.concatenate([scores, scores], axis=1)
        for j in range(pairs_per_group):
            i = g * pairs_per_group + j
            rows = jnp.concatenate(
                [row_decay[2 * i : 2 * i + 1, :], row_decay[2 * i + 1 : 2 * i + 2, :]], axis=1
            )
            gap = column_decay[:, 2 * i * length : (2 * i + 2) * length] - rows
            decay = jnp.exp(jnp.where(causal_pair, gap, -jnp.inf))
            mixing = (scores * decay).astype(bf16)
            both = values[:, i * 2 * HEAD_DIM : (i + 1) * 2 * HEAD_DIM]
            blocks = jnp.concatenate(
                [jnp.where(lane < HEAD_DIM, both, 0.0), jnp.where(lane < HEAD_DIM, 0.0, both)],
                axis=0,
            ).astype(bf16)
            scan[:, i * 2 * HEAD_DIM : (i + 1) * 2 * HEAD_DIM] = contract(
                mixing, blocks, ((1,), (0,))
            )
    scan[...] = scan[...] + skip_scale[0:1, :] * values[...]

    phase("state_wait")
    carried = jnp.zeros((STATE, slice_width), f32)
    kept = jnp.ones((1, slice_width), f32)
    for step in range(1, team):
        source = lax.rem(me + step, team)
        copy(
            state_in.at[source], state_in.at[source], st_ss.at[step], st_rs.at[source], sp, tp
        ).wait_recv()
    phase("prefix")
    for place in range(team):
        entering[place] = carried
        kept_decay[place] = jnp.broadcast_to(kept, (8, slice_width))
        tail = state_in[place, STATE : STATE + 16, :].astype(f32)
        factor = tail[0:1, :] + tail[1:2, :]
        carried = carried * factor + state_in[place, 0:STATE, :].astype(f32)
        kept = kept * factor
    cross_out[...] = carried.astype(bf16)
    cross = copy(cross_out, cross_in, cr_ss, cr_rs, team + me, tp)

    @pl.when(own_team == 0)
    def _():
        cross.start()

    issue(2)
    phase("cross_wait")
    @pl.when(own_team > 0)
    def _():
        cross.wait_recv()

    phase("back")

    @pl.when(own_team == 0)
    def _():
        back_out[...] = entering[...].astype(bf16)

    @pl.when(own_team > 0)
    def _():
        earlier = cross_in[...].astype(f32)
        for place in range(team):
            back_out[place] = (entering[place] + kept_decay[place, 0:1, :] * earlier).astype(bf16)

    back_in[me] = back_out[me]
    back_copies = []
    for step in range(1, team):
        target = mate(step)
        back_copies.append(
            copy(
                back_out.at[lax.rem(target, team)],
                back_in.at[me],
                bk_ss.at[step],
                bk_rs.at[me],
                target,
                tp,
            )
        )
        back_copies[-1].start()
    issue(3)
    phase("back_wait")
    for step in range(1, team):
        source = lax.rem(me + step, team)
        copy(
            back_in.at[source], back_in.at[source], bk_ss.at[step], bk_rs.at[source], sp, tp
        ).wait_recv()

    phase("gate")
    for g in range(groups):
        queries = keyquery[:, state_width + g * STATE : state_width + (g + 1) * STATE]
        at = slice(g * group_width, (g + 1) * group_width)
        per = group_width // slice_width
        incoming = jnp.concatenate([back_in[g * per + part] for part in range(per)], axis=1)
        arriving = contract(queries, incoming, ((1,), (0,))) * scale_in[:, at]
        gate = multiplier_ref[:, at].astype(f32)
        gated = (scan[:, at] + arriving) * (gate * (1.0 / (1.0 + jnp.exp(-gate))))
        gated = gated * lax.rsqrt(jnp.mean(gated * gated, axis=1, keepdims=True) + epsilon)
        heads[:, at] = (gated * cluster_gain[:, at]).astype(bf16)

    phase("project")
    local_blend.wait()
    column_chunk = 512

    def project(index, carry):
        at = pl.ds(pl.multiple_of(index * column_chunk, column_chunk), column_chunk)
        product = contract(heads[...], blend[:, at], ((1,), (0,))).astype(bf16)
        part_out[0, :, at] = product[0:rows_own, :]
        part_out[1, :, at] = product[rows_own:, :]
        return carry

    lax.fori_loop(0, model // column_chunk, project, 0)
    swap = copy(part_out.at[1 - tp], part_in, pt_ss, pt_rs, sp, 1 - tp)
    swap.start()
    phase("swap_wait")
    swap.wait_recv()
    phase("norm")
    mixed = (part_out[tp].astype(f32) + part_in[...].astype(f32)).astype(bf16)
    state = (skip_ref[...].astype(f32) + mixed.astype(f32)).astype(bf16)
    state_rows[...] = state
    state = state.astype(f32)
    state = state * lax.rsqrt(jnp.mean(state * state, axis=1, keepdims=True) + epsilon)
    acts[tp, level] = (state * feature_gain[...]).astype(bf16)

    phase("gather")
    def rows_to(place, ss, rs, target, core):
        return copy(acts.at[tp, place], acts.at[tp, place], ss, rs, target, core)

    top = levels - 1

    def along(place, hop, up_way):
        to = level_at(1 if up_way else -1) * 4 + spot
        return rows_to(place, ap_ss.at[hop + (0 if up_way else levels)], ap_rs.at[place], to, tp)

    def share(place):
        return rows_to(place, ad_ss.at[place], ad_rs.at[place], sp, 1 - tp)

    def send_along(hop):
        @pl.when((level >= hop) & (level < top))
        def _():
            along(level_at(-hop), hop, True).start()

        @pl.when((level + hop <= top) & (level > 0))
        def _():
            along(level_at(hop), hop, False).start()

    send_along(0)
    share(level).start()
    issue(4)
    phase("line_wait")
    for hop in range(1, levels):
        for up_way in (True, False):
            place = level_at(-hop if up_way else hop)

            @pl.when(level >= hop if up_way else level + hop <= top)
            def _():
                along(place, hop, up_way).wait_recv()
                share(place).start()

                if hop < top:

                    @pl.when(level < top if up_way else level > 0)
                    def _():
                        along(place, hop, up_way).start()

        issue(3 + 10 * hop)
    issue(5)
    phase("side_wait")
    for place in range(levels):
        copy(
            acts.at[1 - tp, place], acts.at[1 - tp, place], ad_ss.at[place], ad_rs.at[place], sp, 1 - tp
        ).wait_recv()
    issue(6)

    phase("up_wait")
    local_up.wait()
    for step in range(levels):
        for near in range(2):
            source = level_at(-step) * 4 + (beside[1] if near == 0 else 3 - spot)
            weight_copy(0, None, source, 0, sp).wait_recv()
    phase("lift")
    up_whole = (shards * up.shape[1], unit)

    def lift(index, carry):
        core, block = index // 2, lax.rem(index, 2)
        count = levels // 2
        rows = acts[core, pl.ds(block * count, count)].reshape(count * rows_own, model)
        lifted = jnp.maximum(contract(rows, up[...].reshape(up_whole), ((1,), (0,))), 0.0)
        at = pl.ds(pl.multiple_of(block * count * rows_own, count * rows_own), count * rows_own)
        hidden[core, at, :] = (lifted * lifted).astype(bf16)
        return carry

    lax.fori_loop(0, 4, lift, 0)
    issue(7)

    phase("lower")
    local_down.wait()
    lanes = down.shape[2]

    def pair_sources(t):
        row = lax.rem(t // levels + spot // 2, 2)
        first = lax.rem(t, levels) * 4 + row * 2
        return first, first + 1

    def pair_copy(t):
        return copy(pair_out.at[t], pair_in.at[t], pr_ss.at[t], pr_rs.at[t], sp, 1 - tp)

    def depth_copy(t, k):
        to = level_at(k)
        return copy(
            plane_out.at[t, to],
            depth_in.at[t, k],
            dp_ss.at[t, k],
            dp_rs.at[t, k],
            to * 4 + spot,
            tp,
        )

    def lower_step(t):
        sources = pair_sources(t)
        for source in sources:
            there = lax.rem(source, 4)

            @pl.when((there == beside[0]) | (there == 3 - spot))
            def _():
                weight_copy(1, None, source, 0, sp).wait_recv()

        both = jnp.concatenate([down[sources[0]], down[sources[1]]], axis=1)
        pair_out[t] = contract(hidden[1 - tp], both, ((1,), (0,))).astype(bf16)
        pair_copy(t).start()
        plane_sum = contract(hidden[tp], both, ((1,), (0,)))
        plane_out[t] = plane_sum.astype(bf16).reshape(levels, rows_own, 2 * lanes)

    def pair_step(t):
        pair_copy(t).wait_recv()
        summed = plane_out[t].astype(f32) + pair_in[t].reshape(
            levels, rows_own, 2 * lanes
        ).astype(f32)
        plane_out[t] = summed.astype(bf16)
        for k in range(1, levels):
            depth_copy(t, k).start()

    def depth_step(t):
        summed = plane_out[t, level].astype(f32)
        for k in range(1, levels):
            depth_copy(t, k).wait_recv()
            summed = summed + depth_in[t, k].astype(f32)
        summed = summed.astype(bf16).astype(f32)
        for place, source in enumerate(pair_sources(t)):
            at = pl.ds(pl.multiple_of(source * lanes, lanes), lanes)
            total = state_rows[:, at].astype(f32) + summed[:, place * lanes : (place + 1) * lanes]
            out_ref[:, at] = total.astype(bf16)

    count = shards // 2

    def stage(t, carry):
        for turn in range(levels + 1):
            if batches.get(50 + turn):

                @pl.when(t == turn)
                def _():
                    issue(50 + turn)

        @pl.when(t < count)
        def _():
            with jax.named_scope("lower_step"):
                lower_step(t)

        @pl.when((t >= 1) & (t < count + 1))
        def _():
            with jax.named_scope("pair_step"):
                pair_step(t - 1)

        @pl.when(t >= LAG)
        def _():
            with jax.named_scope("depth_step"):
                depth_step(t - LAG)

        return carry

    lax.fori_loop(0, count + LAG, stage, 0)

    phase("drain")
    @pl.when(sp < shards - 1)
    def _():
        for one in halo_copies:
            one.wait_send()

    for one in state_copies + back_copies:
        one.wait_send()
    @pl.when(own_team == 0)
    def _():
        cross.wait_send()

    swap.wait_send()
    for place in range(levels):
        share(place).wait_send()
    for hop in range(top):

        @pl.when((level >= hop) & (level < top))
        def _():
            along(level_at(-hop), hop, True).wait_send()

        @pl.when((level + hop <= top) & (level > 0))
        def _():
            along(level_at(hop), hop, False).wait_send()

    for kind in range(2):
        for step in range(levels):
            first_pass(kind, step).wait_send()
            second_pass(kind, step, False).wait_send()
            second_pass(kind, step, True).wait_send()
            if step:
                rise(kind, step).wait_send()

    def drain(t, carry):
        pair_copy(t).wait_send()
        for k in range(1, levels):
            depth_copy(t, k).wait_send()
        return carry

    lax.fori_loop(0, count, drain, 0)
    phase("")


LAG = 3


def plan(levels):
    ur, dr = ([("rise", kind, step) for step in range(1, levels)] for kind in range(2))
    uf, df = ([("first", kind, step) for step in range(levels)] for kind in range(2))
    uw, dw = ([("own", kind, step) for step in range(levels)] for kind in range(2))
    ux, dx = ([("other", kind, step) for step in range(levels)] for kind in range(2))
    return {
        0: ur + uf[:1] + df[:1],
        1: uw[:1] + ux[:1] + dw[:1] + dx[:1],
        3: dr + uf[1:] + uw[1:],
        4: ux[1:],
        13: df[1:] + dw[1:],
        51: dx[1:2],
        52: dx[2:3],
        53: dx[3:],
    }


def per_device_fused(team, *operands):
    (
        skip_stream_entering,
        content_signal_matrix,
        writer_signal_matrix,
        reader_signal_matrix,
        multiplier_signal,
        interval_before_softplus,
        extra_log_shrink,
        log_forget_speed,
        content_filter_coefs,
        writer_filter_coefs,
        reader_filter_coefs,
        skip_path_factor,
        cluster_scaling_vector,
        blend_result_matrix,
        feature_blend_scaling,
        widening_matrix,
        narrowing_matrix,
    ) = operands
    f32, bf16 = jnp.float32, jnp.bfloat16
    shards = lax.axis_size("sp")
    length, inner = content_signal_matrix.shape
    state_width = writer_signal_matrix.shape[1]
    local_heads = interval_before_softplus.shape[0]
    rows_own, model = skip_stream_entering.shape
    levels = shards // 4
    unit = widening_matrix.shape[1] // levels
    depth = widening_matrix.shape[0]
    lanes = narrowing_matrix.shape[1]
    slice_width = inner // team
    pairs = shards // 2
    dma = pltpu.SemaphoreType.DMA
    vmem, anywhere = pl.BlockSpec(memory_space=pltpu.VMEM), pl.BlockSpec(memory_space=pl.ANY)
    specs = [vmem] * 13 + [anywhere, vmem, anywhere, anywhere]
    scratch = [
        pltpu.VMEM((16, inner + 2 * state_width), bf16),
        pltpu.VMEM((8 + length, inner + 2 * state_width), f32),
        pltpu.VMEM((length, inner), f32),
        pltpu.VMEM((length, 2 * state_width), bf16),
        pltpu.VMEM(blend_result_matrix.shape, bf16),
        pltpu.VMEM((shards, depth, unit), bf16),
        pltpu.VMEM((shards, unit, lanes), bf16),
        pltpu.VMEM((length, local_heads * length), f32),
        pltpu.VMEM((local_heads, length), f32),
        pltpu.VMEM((length, inner), f32),
        pltpu.VMEM((length, inner), f32),
        pltpu.VMEM((team, STATE + 16, slice_width), bf16),
        pltpu.VMEM((team, STATE + 16, slice_width), bf16),
        pltpu.VMEM((team, STATE, slice_width), f32),
        pltpu.VMEM((team, 8, slice_width), f32),
        pltpu.VMEM((STATE, slice_width), bf16),
        pltpu.VMEM((STATE, slice_width), bf16),
        pltpu.VMEM((team, STATE, slice_width), bf16),
        pltpu.VMEM((team, STATE, slice_width), bf16),
        pltpu.VMEM((length, inner), bf16),
        pltpu.VMEM((2, rows_own, model), bf16),
        pltpu.VMEM((rows_own, model), bf16),
        pltpu.VMEM((rows_own, model), bf16),
        pltpu.VMEM((2, levels, rows_own, model), bf16),
        pltpu.VMEM((2, levels * rows_own, unit), bf16),
        pltpu.VMEM((pairs, levels * rows_own, 2 * lanes), bf16),
        pltpu.VMEM((pairs, levels * rows_own, 2 * lanes), bf16),
        pltpu.VMEM((pairs, levels, rows_own, 2 * lanes), bf16),
        pltpu.VMEM((pairs, levels, rows_own, 2 * lanes), bf16),
        dma((3,)),
        dma((3,)),
        dma((3,)),
        dma((8 + 2 * levels,)),
        dma((shards,)),
        dma((8 + 2 * levels,)),
        dma((shards,)),
        dma((team,)),
        dma((team,)),
        dma,
        dma,
        dma((team,)),
        dma((team,)),
        dma,
        dma,
        dma((2 * levels,)),
        dma((levels,)),
        dma((levels,)),
        dma((levels,)),
        dma((pairs,)),
        dma((pairs,)),
        dma((pairs, levels)),
        dma((pairs, levels)),
    ]
    return pl.pallas_call(
        functools.partial(layer_kernel, team),
        out_shape=jax.ShapeDtypeStruct((rows_own, model), bf16),
        in_specs=specs,
        out_specs=vmem,
        scratch_shapes=scratch,
        compiler_params=pltpu.CompilerParams(
            collective_id=0, has_side_effects=True, vmem_limit_bytes=63 * 1024 * 1024
        ),
    )(
        skip_stream_entering,
        content_signal_matrix,
        writer_signal_matrix,
        reader_signal_matrix,
        multiplier_signal,
        interval_before_softplus,
        extra_log_shrink,
        log_forget_speed.reshape(1, -1),
        content_filter_coefs,
        writer_filter_coefs,
        reader_filter_coefs,
        skip_path_factor.reshape(1, -1),
        cluster_scaling_vector.reshape(1, -1),
        blend_result_matrix,
        feature_blend_scaling.reshape(1, -1),
        widening_matrix,
        narrowing_matrix,
    )


def general_solution(mesh):
    shards, halves = mesh.shape["sp"], mesh.shape["tp"]
    team = math.gcd(shards, TEAM)
    teams = jax.sharding.Mesh(
        mesh.devices.reshape(shards // team, team, halves), ("sa", "sb", "tp")
    )
    placed = (
        P(("sa", "sb", "tp"), None),
        P(SP, "tp"),
        P(SP, "tp"),
        P(SP, "tp"),
        P(SP, "tp"),
        P("tp", SP),
        P("tp", SP),
        P("tp"),
        P(None, "tp"),
        P(None, "tp"),
        P(None, "tp"),
        P("tp"),
        P("tp"),
        P("tp", None),
        P(),
        P(SP, "tp"),
        P("tp", SP),
    )
    return jax.shard_map(
        per_device, mesh=teams, in_specs=placed, out_specs=P(("sa", "sb", "tp"), None), check_vma=False
    )


def fits(shards, halves, team, rows, tokens, inner, hidden, model, state_width):
    length = tokens // shards
    local = inner // halves
    return (
        halves == 2
        and shards == 2 * team
        and team % 4 == 0
        and length == BLOCK
        and length % 32 == 0
        and local % (team * 128) == 0
        and shards % 4 == 0
        and (hidden // halves) % (shards // 4 * 128) == 0
        and (shards // 4) == 4
        and model % (shards * 128) == 0
        and (state_width // halves) % STATE == 0
        and (local // (state_width // halves // STATE)) % (local // team) == 0
    )


def solution(mesh):
    shards, halves = mesh.shape["sp"], mesh.shape["tp"]
    team = math.gcd(shards, TEAM)
    general = general_solution(mesh)
    row, both = P("sp", "tp"), P(("sp", "tp"), None)
    tp_first, tp_last, tp_only = P("tp", "sp"), P(None, "tp"), P("tp")
    placed = (
        (both, row, row, row, row, tp_first, tp_first, tp_only, tp_last, tp_last, tp_last)
        + (tp_only, tp_only, P("tp", None), P(), row, tp_first)
    )
    fused = jax.shard_map(
        functools.partial(per_device_fused, team),
        mesh=mesh,
        in_specs=placed,
        out_specs=both,
        check_vma=False,
    )

    def layer(*operands):
        tokens, inner = operands[1].shape
        model, hidden = operands[15].shape
        state_width = operands[2].shape[1]
        if fits(shards, halves, team, tokens, tokens, inner, hidden, model, state_width):
            return fused(*operands)
        return general(*operands)

    return layer
```

```python
import functools
import math
import jax
import jax.numpy as jnp
from jax import lax
from jax.experimental import pallas as pl
from jax.experimental.pallas import tpu as pltpu
from jax.sharding import PartitionSpec as P

HEAD_DIM = 64
STATE = 128
BLOCK = 128


epsilon = 1e-05
precise = lax.Precision.HIGHEST
SP = ("sa", "sb")
TEAM = 8


def shifted(value, axis, steps):
    count = lax.axis_size(axis)
    initial, last = (max(0, -steps), min(count, count - steps))
    return lax.ppermute(value, axis, [(source, source + steps) for source in range(initial, last)])


def scan_rows(parts, factors, entering):
    def one(place, carried):
        entering[place] = carried.astype(jnp.bfloat16)
        return carried * factors[place] + parts[place].astype(jnp.float32)

    lax.fori_loop(0, parts.shape[0], one, jnp.zeros(parts.shape[1:], jnp.float32))


def prefix(log_total, end_state, rider):
    shards = lax.axis_size(SP)
    heads = end_state.shape[0] * end_state.shape[1]
    state_width = end_state.shape[-1]
    rows = end_state.reshape(-1, state_width).astype(jnp.bfloat16)
    count = rows.shape[0] // shards
    decays = jnp.repeat(jnp.exp(log_total).reshape(heads), rows.shape[0] // heads)
    extra = -(-count // state_width) * 16
    decays = decays.astype(jnp.bfloat16).reshape(shards, count)
    decays = jnp.pad(decays, ((0, 0), (0, extra * state_width - count)))
    packed = jnp.concatenate(
        [rows.reshape(shards, count, state_width), decays.reshape(shards, extra, state_width)],
        axis=1,
    )
    packed = lax.all_to_all(packed, SP, split_axis=0, concat_axis=0)
    parts = packed[:, :count]
    factors = packed[:, count:].reshape(shards, -1)[:, :count].astype(jnp.float32)
    entering = pl.pallas_call(
        scan_rows,
        out_shape=jax.ShapeDtypeStruct(parts.shape, jnp.bfloat16),
    )(parts, jnp.broadcast_to(factors[..., None], parts.shape))
    entering, rider = lax.optimization_barrier((entering, rider))
    back = lax.all_to_all(
        entering.reshape(rows.shape), SP, split_axis=0, concat_axis=0, tiled=True
    )
    return back.reshape(end_state.shape).astype(jnp.float32), rider


def summed_share(partial, axis):
    count = lax.axis_size(axis)
    if count != 2:
        return lax.psum_scatter(partial, axis, scatter_dimension=0, tiled=True)
    me = lax.axis_index(axis)
    length = partial.shape[0] // 2
    away = lax.dynamic_slice_in_dim(partial, (1 - me) * length, length, 0)
    kept = lax.dynamic_slice_in_dim(partial, me * length, length, 0)
    arrived = lax.ppermute(away, axis, [(0, 1), (1, 0)])
    return (kept.astype(jnp.float32) + arrived.astype(jnp.float32)).astype(jnp.bfloat16)


def convolve(inputs, rim_rows, conv_taps):
    width = conv_taps.shape[0]
    length = inputs.shape[0]
    extended = jnp.concatenate([rim_rows, inputs], axis=0)
    summed = extended[0:length].astype(jnp.float32) * conv_taps[0].astype(jnp.float32)
    for offset in range(1, width):
        summed = summed + extended[offset : offset + length].astype(jnp.float32) * conv_taps[
            offset
        ].astype(jnp.float32)
    return jax.nn.silu(summed)


def advance(carried, pair):
    block_state, block_factor = pair
    return (carried * block_factor[..., None, None] + block_state, carried)


def blockwise(values, interval_lengths, log_forgetting, key_rows, query_rows):
    length, groups, per_group, width = values.shape
    blocks = length // BLOCK
    value_blocks = values.reshape(blocks, BLOCK, groups, per_group, width)
    step_blocks = jnp.transpose(
        interval_lengths.reshape(groups, per_group, blocks, BLOCK), (2, 3, 0, 1)
    )
    weighted = value_blocks * step_blocks[..., None]
    cumulative = jnp.cumsum(
        jnp.transpose(log_forgetting.reshape(groups, per_group, blocks, BLOCK), (2, 0, 1, 3)),
        axis=-1,
    )
    key_blocks = key_rows.reshape(blocks, BLOCK, groups, -1)
    query_blocks = query_rows.reshape(blocks, BLOCK, groups, -1)
    causal = jnp.tril(jnp.ones((BLOCK, BLOCK), dtype=bool))
    decay_mask = jnp.exp(
        jnp.where(causal, cumulative[..., :, None] - cumulative[..., None, :], -jnp.inf)
    )
    scores = jnp.einsum("clgn,csgn->cgls", query_blocks, key_blocks, precision=precise)
    within = jnp.einsum("cgls,cgrls,csgrp->clgrp", scores, decay_mask, weighted, precision=precise)
    to_end = jnp.exp(cumulative[..., -1:] - cumulative)
    states = jnp.einsum("clgn,cgrl,clgrp->cgrpn", key_blocks, to_end, weighted, precision=precise)
    block_totals = cumulative[..., -1]
    initial = jnp.zeros(states.shape[1:], jnp.float32)
    final, entering = lax.scan(advance, initial, (states, jnp.exp(block_totals)))
    carried = jnp.einsum(
        "clgn,cgrpn,cgrl->clgrp", query_blocks, entering, jnp.exp(cumulative), precision=precise
    )
    from_start = (jnp.cumsum(block_totals, axis=0) - block_totals)[..., None] + cumulative
    return (within + carried, final, from_start, jnp.sum(block_totals, axis=0))


def normalize(rows, gain):
    widened = rows.astype(jnp.float32)
    scaled = widened * lax.rsqrt(jnp.mean(widened * widened, axis=-1, keepdims=True) + epsilon)
    return (scaled * gain).astype(jnp.bfloat16)


def per_device(
    skip_stream_entering,
    content_signal_matrix,
    writer_signal_matrix,
    reader_signal_matrix,
    multiplier_signal,
    interval_before_softplus,
    extra_log_shrink,
    log_forget_speed,
    content_filter_coefs,
    writer_filter_coefs,
    reader_filter_coefs,
    skip_path_factor,
    cluster_scaling_vector,
    blend_result_matrix,
    feature_blend_scaling,
    widening_matrix,
    narrowing_matrix,
):
    up_part = lax.all_to_all(widening_matrix, "sb", split_axis=1, concat_axis=0, tiled=True)
    narrowing_matrix, up_part = lax.optimization_barrier((narrowing_matrix, up_part))
    up_use = lax.all_gather(up_part, "sa", axis=0, tiled=True)
    down_part = lax.all_to_all(narrowing_matrix, "sb", split_axis=0, concat_axis=1, tiled=True)
    (
        content_signal_matrix,
        writer_signal_matrix,
        reader_signal_matrix,
        interval_before_softplus,
        down_part,
    ) = lax.optimization_barrier(
        (
            content_signal_matrix,
            writer_signal_matrix,
            reader_signal_matrix,
            interval_before_softplus,
            down_part,
        )
    )
    down_use = lax.all_gather(down_part, "sa")
    rim_width = content_filter_coefs.shape[0] - 1
    length = content_signal_matrix.shape[0]
    signals = (content_signal_matrix, writer_signal_matrix, reader_signal_matrix)
    tails = jnp.concatenate([signal[length - rim_width :] for signal in signals], axis=1)
    rims = shifted(tails, SP, 1)
    first, second = signals[0].shape[1], signals[0].shape[1] + signals[1].shape[1]
    values = convolve(signals[0], rims[:, :first], content_filter_coefs)
    key_rows = convolve(signals[1], rims[:, first:second], writer_filter_coefs)
    query_rows = convolve(signals[2], rims[:, second:], reader_filter_coefs)
    local_heads = interval_before_softplus.shape[0]
    local_groups = writer_signal_matrix.shape[1] // STATE
    per_group = local_heads // local_groups
    interval_lengths = jax.nn.softplus(interval_before_softplus)
    log_forgetting = extra_log_shrink - jnp.exp(log_forget_speed)[:, None] * interval_lengths
    shaped = values.reshape(length, local_groups, per_group, HEAD_DIM)
    local_out, end_state, from_start, device_total = blockwise(
        shaped,
        interval_lengths.reshape(local_groups, per_group, length),
        log_forgetting.reshape(local_groups, per_group, length),
        key_rows,
        query_rows,
    )
    incoming, up_use = prefix(device_total, end_state, up_use)
    query_blocks = query_rows.reshape(length // BLOCK, BLOCK, local_groups, STATE)
    arriving = jnp.einsum(
        "clgn,grpn,cgrl->clgrp", query_blocks, incoming, jnp.exp(from_start), precision=precise
    )
    scan_out = (local_out + arriving).reshape(length, local_heads * HEAD_DIM)
    gated = (scan_out + jnp.repeat(skip_path_factor, HEAD_DIM) * values) * jax.nn.silu(
        multiplier_signal.astype(jnp.float32)
    )
    grouped = gated.reshape(length, local_groups, -1)
    grouped = grouped * lax.rsqrt(jnp.mean(grouped * grouped, axis=-1, keepdims=True) + epsilon)
    heads_out = (grouped.reshape(length, -1) * cluster_scaling_vector).astype(jnp.bfloat16)
    mixer_rows = summed_share(
        jnp.dot(heads_out, blend_result_matrix, preferred_element_type=jnp.float32).astype(
            jnp.bfloat16
        ),
        "tp",
    )
    own_rows = (skip_stream_entering.astype(jnp.float32) + mixer_rows.astype(jnp.float32)).astype(
        jnp.bfloat16
    )
    normed = normalize(own_rows, feature_blend_scaling)
    down_whole = jnp.concatenate([down_use[k] for k in range(down_use.shape[0])], axis=1)

    def mixed(rows):
        lifted = jax.nn.relu(jnp.dot(rows, up_use, preferred_element_type=jnp.float32))
        hidden = (lifted * lifted).astype(jnp.bfloat16)
        partial = jnp.dot(hidden, down_whole, preferred_element_type=jnp.float32)
        return partial.astype(jnp.bfloat16)

    if lax.axis_size("tp") == 2:
        members, width = lax.axis_size("sb"), normed.shape[1]
        swap = [(0, 1), (1, 0)]
        copies = jnp.broadcast_to(normed[None], (members,) + normed.shape)
        own_half = lax.all_to_all(copies, "sb", split_axis=0, concat_axis=0)
        own_half = own_half.reshape(-1, width)
        other_half = lax.ppermute(own_half, "tp", swap)
        arrived = lax.ppermute(mixed(other_half), "tp", swap)
        joined = mixed(own_half).astype(jnp.float32) + arrived.astype(jnp.float32)
        joined = joined.astype(jnp.bfloat16).reshape(members, -1, width)
        shares = lax.all_to_all(joined, "sb", split_axis=0, concat_axis=0)
        mlp_rows = jnp.sum(shares.astype(jnp.float32), axis=0)
    else:
        team_rows = lax.all_gather(normed, ("sb", "tp"), axis=0, tiled=True)
        mlp_rows = lax.psum_scatter(
            mixed(team_rows), ("sb", "tp"), scatter_dimension=0, tiled=True
        )
    mlp_rows = mlp_rows.astype(jnp.bfloat16)
    return (own_rows.astype(jnp.float32) + mlp_rows.astype(jnp.float32)).astype(jnp.bfloat16)


TEAM_LINKS = pl.DeviceIdType.MESH


def split3(wide):
    one = wide.astype(jnp.bfloat16)
    rest = wide - one.astype(jnp.float32)
    two = rest.astype(jnp.bfloat16)
    return one, two, (rest - two.astype(jnp.float32)).astype(jnp.bfloat16)


def contract(left, right, dims):
    return lax.dot_general(left, right, (dims, ((), ())), preferred_element_type=jnp.float32)


def exact(left, right, dims, left_split):
    if left_split:
        terms = [contract(part, right, dims) for part in split3(left)]
    else:
        terms = [contract(left, part, dims) for part in split3(right)]
    return terms[0] + terms[1] + terms[2]


def selector(rows, columns, per_row):
    row = lax.broadcasted_iota(jnp.int32, (rows, columns), 0)
    column = lax.broadcasted_iota(jnp.int32, (rows, columns), 1)
    return jnp.where(column // per_row == row, 1.0, 0.0).astype(jnp.bfloat16)


def layer_kernel(
    team,
    skip_hbm,
    content_hbm,
    writer_hbm,
    reader_hbm,
    multiplier_hbm,
    interval_ref,
    shrink_ref,
    speed_ref,
    content_taps,
    writer_taps,
    reader_taps,
    skip_factor,
    cluster_gain,
    blend_hbm,
    feature_gain,
    up_hbm,
    down_hbm,
    out_ref,
    skip_ref,
    content_ref,
    writer_ref,
    reader_ref,
    multiplier_ref,
    halo,
    wide,
    values,
    keyquery,
    blend,
    up,
    down,
    column_decay,
    row_decay,
    scan,
    scale_in,
    state_out,
    state_in,
    entering,
    kept_decay,
    cross_out,
    cross_in,
    back_out,
    back_in,
    heads,
    part_out,
    part_in,
    state_rows,
    acts,
    hidden,
    pair_out,
    pair_in,
    plane_out,
    depth_in,
    local_sem,
    halo_ss,
    halo_rs,
    up_ss,
    up_rs,
    down_ss,
    down_rs,
    half_ss,
    half_rs,
    st_ss,
    st_rs,
    cr_ss,
    cr_rs,
    bk_ss,
    bk_rs,
    pt_ss,
    pt_rs,
    ap_ss,
    ap_rs,
    ad_ss,
    ad_rs,
    pr_ss,
    pr_rs,
    dp_ss,
    dp_rs,
):
    f32, bf16 = jnp.float32, jnp.bfloat16
    batches = plan(lax.axis_size("sp") // 4)
    shards = lax.axis_size("sp")
    sp, tp = lax.axis_index("sp"), lax.axis_index("tp")
    own_team, me = sp // team, lax.rem(sp, team)
    length, inner = content_ref.shape
    state_width = writer_ref.shape[1]
    local_heads = interval_ref.shape[0]
    groups = state_width // STATE
    group_width = inner // groups
    model = skip_ref.shape[1]
    unit = up.shape[2]
    slice_width = inner // team
    half = team // 2
    rows_own = skip_ref.shape[0]

    open_scope = []

    def phase(name):
        if open_scope:
            open_scope.pop().__exit__(None, None, None)
        if name:
            open_scope.append(jax.named_scope(name))
            open_scope[-1].__enter__()

    def copy(src, dst, ss, rs, sp_to, tp_to):
        return pltpu.make_async_remote_copy(
            src_ref=src,
            dst_ref=dst,
            send_sem=ss,
            recv_sem=rs,
            device_id=(sp_to, tp_to),
            device_id_type=TEAM_LINKS,
        )

    def mate(step):
        return own_team * team + lax.rem(me + step, team)

    level, spot = sp // 4, lax.rem(sp, 4)
    beside = (spot + 1 - 2 * lax.rem(spot, 2), lax.rem(spot + 2, 4))
    levels = shards // 4

    def level_at(step):
        return lax.rem(level + levels + step, levels)

    def weight_piece(kind, index):
        offset = pl.ds(pl.multiple_of(index * unit, unit), unit)
        return up_hbm.at[:, offset] if kind == 0 else down_hbm.at[offset, :]

    def weight_copy(kind, src, source, place, target):
        into, ss, rs = ((up, up_ss, up_rs), (down, down_ss, down_rs))[kind]
        if src is None:
            src = into.at[source]
        return copy(src, into.at[source], ss.at[place], rs.at[source], target, tp)

    def source_level(step, kind):
        if kind == 0 or step == 0:
            return level_at(-step)
        return step - 1 + jnp.where(level <= step - 1, 1, 0)

    def rise(kind, step):
        to = level_at(step)
        return weight_copy(kind, weight_piece(kind, to), sp, step, to * 4 + spot)

    def spread(kind, step, way):
        source = source_level(step, kind) * 4 + spot
        piece = weight_piece(kind, level) if step == 0 else None
        place = levels * (1 + way) + step
        return weight_copy(kind, piece, source, place, level * 4 + beside[way])

    def relay(kind, step, way):
        at_level = source_level(step, kind)
        return diagonal(kind, at_level, at_level * 4 + beside[way], way, step)

    def diagonal(kind, at_level, source, way, step):
        part = pl.ds(way * (unit // 2), unit // 2)
        held = up.at[source, :, part] if kind == 0 else down.at[source, part, :]
        place = kind * 2 * levels + way * levels
        target = level * 4 + beside[1 - way]
        return copy(held, held, half_ss.at[place + step], half_rs.at[place + at_level], target, tp)

    def neighbour(kind, step, way):
        return weight_copy(kind, None, source_level(step, kind) * 4 + beside[way], 0, sp)

    def issue(batch):
        for what, kind, step in batches.get(batch, ()):
            if what == "rise":
                rise(kind, step).start()
            if what == "spread":
                if step:
                    spread(kind, step, 0).wait_recv()
                for way in range(2):
                    spread(kind, step, way).start()
            if what == "relay":
                for way in range(2):
                    neighbour(kind, step, way).wait_recv()
                    relay(kind, step, way).start()

    local_up = pltpu.make_async_copy(weight_piece(0, level), up.at[sp], local_sem.at[0])
    local_down = pltpu.make_async_copy(weight_piece(1, level), down.at[sp], local_sem.at[1])
    local_blend = pltpu.make_async_copy(blend_hbm, blend, local_sem.at[2])
    brought = []
    for place, (source, into) in enumerate(
        (
            (content_hbm, content_ref),
            (writer_hbm, writer_ref),
            (reader_hbm, reader_ref),
            (multiplier_hbm, multiplier_ref),
            (skip_hbm, skip_ref),
        )
    ):
        brought.append(pltpu.make_async_copy(source, into, local_sem.at[3 + place]))
        brought[-1].start()
    local_up.start()
    local_down.start()
    local_blend.start()

    barrier = pltpu.get_barrier_semaphore()
    for step in range(1, shards):
        pl.semaphore_signal(
            barrier,
            inc=1,
            device_id=(lax.rem(sp + step, shards), tp),
            device_id_type=TEAM_LINKS,
        )
    pl.semaphore_signal(barrier, inc=1, device_id=(sp, 1 - tp), device_id_type=TEAM_LINKS)

    phase("decays")
    steps = interval_ref[...]
    steps = jnp.maximum(steps, 0.0) + jnp.log1p(jnp.exp(-jnp.abs(steps)))
    head_row = lax.broadcasted_iota(jnp.int32, (local_heads, local_heads), 0)
    head_column = lax.broadcasted_iota(jnp.int32, (local_heads, local_heads), 1)
    speed = jnp.where(head_row == head_column, speed_ref[...], 0.0)
    forget = shrink_ref[...] - jnp.exp(jnp.sum(speed, axis=1, keepdims=True)) * steps
    row_index = lax.broadcasted_iota(jnp.int32, (length, length), 0)
    column_index = lax.broadcasted_iota(jnp.int32, (length, length), 1)
    lower = jnp.where(row_index >= column_index, 1.0, 0.0).astype(bf16)
    upper = jnp.where(row_index <= column_index, 1.0, 0.0).astype(bf16)
    unity = jnp.where(row_index == column_index, 1.0, 0.0).astype(bf16)
    log_steps = jnp.log(steps)
    total_rows = exact(forget, upper, ((1,), (0,)), True)
    total_columns = exact(lower, forget, ((1,), (1,)), False)
    log_columns = exact(unity, log_steps, ((1,), (1,)), False)
    row_decay[...] = total_rows - log_steps
    by_head = selector(local_heads, local_heads * length, length)
    column_decay[...] = exact(total_columns, by_head, ((1,), (0,)), True)
    by_channel = selector(local_heads, inner, HEAD_DIM)
    scale_in[...] = exact(jnp.exp(total_columns), by_channel, ((1,), (0,)), True)
    last = total_columns[length - 1 : length, :]
    to_end = jnp.exp(last - total_columns + log_columns)
    end_scale = exact(to_end, by_channel, ((1,), (0,)), True)
    whole_decay = exact(
        jnp.broadcast_to(jnp.exp(last), (16, local_heads)), by_channel, ((1,), (0,)), True
    )
    skip_scale = exact(
        jnp.broadcast_to(skip_factor[...], (16, local_heads)), by_channel, ((1,), (0,)), True
    )

    for one in brought[:3]:
        one.wait()
    phase("barrier_wait")
    pl.semaphore_wait(barrier, shards)
    phase("first_sends")
    following = lax.rem(sp + 1, shards)
    spans = ((content_ref, 0, inner), (writer_ref, inner, state_width))
    spans = spans + ((reader_ref, inner + state_width, state_width),)
    halo_copies = []
    for place, (ref, first, size) in enumerate(spans):
        halo_copies.append(
            copy(
                ref.at[pl.ds(length - 16, 16), :],
                halo.at[:, pl.ds(first, size)],
                halo_ss.at[place],
                halo_rs.at[place],
                following,
                tp,
            )
        )

    @pl.when(sp < shards - 1)
    def _():
        for one in halo_copies:
            one.start()

    issue(0)

    phase("rim_wait")
    @pl.when(sp > 0)
    def _():
        for one in halo_copies:
            one.wait_recv()

    @pl.when(sp == 0)
    def _():
        halo[...] = jnp.zeros_like(halo)

    phase("convolve")
    chunk = state_width
    for ref, taps, first, size in (
        (content_ref, content_taps, 0, inner),
        (writer_ref, writer_taps, inner, state_width),
        (reader_ref, reader_taps, inner + state_width, state_width),
    ):
        for start in range(0, size, chunk):
            at = slice(start, start + chunk)
            placed = slice(first + start, first + start + chunk)
            wide[8:, placed] = ref[:, at].astype(f32)
            wide[0:8, placed] = halo[:, placed].astype(f32)[8:, :]
            weights = taps[:, at].astype(f32)
            count = taps.shape[0]
            base = 8 - (count - 1)
            total = wide[base : base + length, placed] * weights[0:1, :]
            for k in range(1, count):
                total = total + wide[base + k : base + k + length, placed] * weights[k : k + 1, :]
            total = total * (1.0 / (1.0 + jnp.exp(-total)))
            if first == 0:
                values[:, at] = total
            else:
                keyquery[:, first - inner + start : first - inner + start + chunk] = total.astype(bf16)

    phase("states")
    weighted = (values[...] * end_scale).astype(bf16)
    for g in range(groups):
        keys = keyquery[:, g * STATE : (g + 1) * STATE]
        made = contract(keys, weighted[:, g * group_width : (g + 1) * group_width], ((0,), (0,)))
        for part in range(group_width // slice_width):
            place = g * (group_width // slice_width) + part
            state_out[place, 0:STATE, :] = made[
                :, part * slice_width : (part + 1) * slice_width
            ].astype(bf16)
    high = whole_decay.astype(bf16)
    low = (whole_decay - high.astype(f32)).astype(bf16)
    first_row = lax.broadcasted_iota(jnp.int32, whole_decay.shape, 0) == 0
    packed = jnp.where(first_row, high.astype(f32), low.astype(f32)).astype(bf16)
    for place in range(team):
        state_out[place, STATE : STATE + 16, :] = packed[
            :, place * slice_width : (place + 1) * slice_width
        ]
    state_in[me] = state_out[me]
    state_copies = []
    for step in range(1, team):
        target = mate(step)
        state_copies.append(
            copy(
                state_out.at[lax.rem(target, team)],
                state_in.at[me],
                st_ss.at[step],
                st_rs.at[me],
                target,
                tp,
            )
        )
        state_copies[-1].start()
    issue(1)

    phase("within")
    causal = row_index >= column_index
    causal_pair = jnp.concatenate([causal, causal], axis=1)
    lane = lax.broadcasted_iota(jnp.int32, (length, 2 * HEAD_DIM), 1)
    pairs_per_group = group_width // (2 * HEAD_DIM)
    for g in range(groups):
        keys = keyquery[:, g * STATE : (g + 1) * STATE]
        queries = keyquery[:, state_width + g * STATE : state_width + (g + 1) * STATE]
        scores = contract(queries, keys, ((1,), (1,)))
        scores = jnp.concatenate([scores, scores], axis=1)
        for j in range(pairs_per_group):
            i = g * pairs_per_group + j
            rows = jnp.concatenate(
                [row_decay[2 * i : 2 * i + 1, :], row_decay[2 * i + 1 : 2 * i + 2, :]], axis=1
            )
            gap = column_decay[:, 2 * i * length : (2 * i + 2) * length] - rows
            decay = jnp.exp(jnp.where(causal_pair, gap, -jnp.inf))
            mixing = (scores * decay).astype(bf16)
            both = values[:, i * 2 * HEAD_DIM : (i + 1) * 2 * HEAD_DIM]
            blocks = jnp.concatenate(
                [jnp.where(lane < HEAD_DIM, both, 0.0), jnp.where(lane < HEAD_DIM, 0.0, both)],
                axis=0,
            ).astype(bf16)
            scan[:, i * 2 * HEAD_DIM : (i + 1) * 2 * HEAD_DIM] = contract(
                mixing, blocks, ((1,), (0,))
            )
    scan[...] = scan[...] + skip_scale[0:1, :] * values[...]

    phase("state_wait")
    carried = jnp.zeros((STATE, slice_width), f32)
    kept = jnp.ones((1, slice_width), f32)
    for step in range(1, team):
        source = lax.rem(me + step, team)
        copy(
            state_in.at[source], state_in.at[source], st_ss.at[step], st_rs.at[source], sp, tp
        ).wait_recv()
    phase("prefix")
    for place in range(team):
        entering[place] = carried
        kept_decay[place] = jnp.broadcast_to(kept, (8, slice_width))
        tail = state_in[place, STATE : STATE + 16, :].astype(f32)
        factor = tail[0:1, :] + tail[1:2, :]
        carried = carried * factor + state_in[place, 0:STATE, :].astype(f32)
        kept = kept * factor
    cross_out[...] = carried.astype(bf16)
    cross = copy(cross_out, cross_in, cr_ss, cr_rs, team + me, tp)

    @pl.when(own_team == 0)
    def _():
        cross.start()

    issue(2)
    phase("cross_wait")
    @pl.when(own_team > 0)
    def _():
        cross.wait_recv()

    phase("back")

    @pl.when(own_team == 0)
    def _():
        back_out[...] = entering[...].astype(bf16)

    @pl.when(own_team > 0)
    def _():
        earlier = cross_in[...].astype(f32)
        for place in range(team):
            back_out[place] = (entering[place] + kept_decay[place, 0:1, :] * earlier).astype(bf16)

    back_in[me] = back_out[me]
    back_copies = []
    for step in range(1, team):
        target = mate(step)
        back_copies.append(
            copy(
                back_out.at[lax.rem(target, team)],
                back_in.at[me],
                bk_ss.at[step],
                bk_rs.at[me],
                target,
                tp,
            )
        )
        back_copies[-1].start()
    issue(3)
    phase("back_wait")
    for step in range(1, team):
        source = lax.rem(me + step, team)
        copy(
            back_in.at[source], back_in.at[source], bk_ss.at[step], bk_rs.at[source], sp, tp
        ).wait_recv()

    phase("gate")
    brought[3].wait()
    for g in range(groups):
        queries = keyquery[:, state_width + g * STATE : state_width + (g + 1) * STATE]
        at = slice(g * group_width, (g + 1) * group_width)
        per = group_width // slice_width
        incoming = jnp.concatenate([back_in[g * per + part] for part in range(per)], axis=1)
        arriving = contract(queries, incoming, ((1,), (0,))) * scale_in[:, at]
        gate = multiplier_ref[:, at].astype(f32)
        gated = (scan[:, at] + arriving) * (gate * (1.0 / (1.0 + jnp.exp(-gate))))
        gated = gated * lax.rsqrt(jnp.mean(gated * gated, axis=1, keepdims=True) + epsilon)
        heads[:, at] = (gated * cluster_gain[:, at]).astype(bf16)

    phase("project")
    local_blend.wait()
    column_chunk = 512

    def project(index, carry):
        at = pl.ds(pl.multiple_of(index * column_chunk, column_chunk), column_chunk)
        product = contract(heads[...], blend[:, at], ((1,), (0,))).astype(bf16)
        part_out[0, :, at] = product[0:rows_own, :]
        part_out[1, :, at] = product[rows_own:, :]
        return carry

    lax.fori_loop(0, model // column_chunk, project, 0)
    swap = copy(part_out.at[1 - tp], part_in, pt_ss, pt_rs, sp, 1 - tp)
    swap.start()
    phase("swap_wait")
    swap.wait_recv()
    phase("norm")
    brought[4].wait()
    mixed = (part_out[tp].astype(f32) + part_in[...].astype(f32)).astype(bf16)
    state = (skip_ref[...].astype(f32) + mixed.astype(f32)).astype(bf16)
    state_rows[...] = state
    state = state.astype(f32)
    state = state * lax.rsqrt(jnp.mean(state * state, axis=1, keepdims=True) + epsilon)
    acts[tp, level] = (state * feature_gain[...]).astype(bf16)

    phase("gather")
    parts = 2

    def rows_to(place, part, ss, rs, target, core):
        rows = pl.ds(part * (rows_own // parts), rows_own // parts)
        held = acts.at[tp, place, rows]
        return copy(held, held, ss, rs.at[place * parts + part], target, core)

    top = levels - 1

    def along(place, part, hop, up_way):
        to = level_at(1 if up_way else -1) * 4 + spot
        order = (hop + (0 if up_way else levels)) * parts + part
        return rows_to(place, part, ap_ss.at[order], ap_rs, to, tp)

    def share(place, part):
        return rows_to(place, part, ad_ss.at[place * parts + part], ad_rs, sp, 1 - tp)

    def send_along(hop, part):
        @pl.when((level >= hop) & (level < top))
        def _():
            along(level_at(-hop), part, hop, True).start()

        @pl.when((level + hop <= top) & (level > 0))
        def _():
            along(level_at(hop), part, hop, False).start()

    for part in range(parts):
        send_along(0, part)
        share(level, part).start()
    issue(4)
    phase("line_wait")
    for hop in range(1, levels):
        for part in range(parts):
            for up_way in (True, False):
                place = level_at(-hop if up_way else hop)

                @pl.when(level >= hop if up_way else level + hop <= top)
                def _():
                    along(place, part, hop, up_way).wait_recv()
                    if hop < top:

                        @pl.when(level < top if up_way else level > 0)
                        def _():
                            along(place, part, hop, up_way).start()

                    share(place, part).start()

        issue(3 + 10 * hop)
    issue(5)
    phase("side_wait")
    for place in range(levels):
        for part in range(parts):
            share(place, part).wait_recv()
    issue(6)

    phase("up_wait")
    local_up.wait()
    for step in range(levels):
        for way in range(2):
            diagonal(0, step, step * 4 + 3 - spot, way, 0).wait_recv()
    phase("lift")
    up_whole = (shards * up.shape[1], unit)

    def lift(index, carry):
        core, block = index // 2, lax.rem(index, 2)
        count = levels // 2
        rows = acts[core, pl.ds(block * count, count)].reshape(count * rows_own, model)
        lifted = jnp.maximum(contract(rows, up[...].reshape(up_whole), ((1,), (0,))), 0.0)
        at = pl.ds(pl.multiple_of(block * count * rows_own, count * rows_own), count * rows_own)
        hidden[core, at, :] = (lifted * lifted).astype(bf16)
        return carry

    lax.fori_loop(0, 4, lift, 0)
    issue(7)

    phase("lower")
    local_down.wait()
    lanes = down.shape[2]

    def pair_sources(t):
        row = lax.rem(t // levels + spot // 2, 2)
        first = lax.rem(t, levels) * 4 + row * 2
        return first, first + 1

    def pair_copy(t):
        return copy(pair_out.at[t], pair_in.at[t], pr_ss.at[t], pr_rs.at[t], sp, 1 - tp)

    def depth_copy(t, k):
        to = level_at(k)
        return copy(
            plane_out.at[t, to],
            depth_in.at[t, k],
            dp_ss.at[t, k],
            dp_rs.at[t, k],
            to * 4 + spot,
            tp,
        )

    def lower_step(t):
        sources = pair_sources(t)

        @pl.when(t >= levels)
        def _():
            for way in range(2):
                at_level = lax.rem(t, levels)
                diagonal(1, at_level, at_level * 4 + 3 - spot, way, 0).wait_recv()

        both = jnp.concatenate([down[sources[0]], down[sources[1]]], axis=1)
        pair_out[t] = contract(hidden[1 - tp], both, ((1,), (0,))).astype(bf16)
        pair_copy(t).start()
        plane_sum = contract(hidden[tp], both, ((1,), (0,)))
        plane_out[t] = plane_sum.astype(bf16).reshape(levels, rows_own, 2 * lanes)

    def pair_step(t):
        pair_copy(t).wait_recv()
        summed = plane_out[t].astype(f32) + pair_in[t].reshape(
            levels, rows_own, 2 * lanes
        ).astype(f32)
        plane_out[t] = summed.astype(bf16)
        for k in range(1, levels):
            depth_copy(t, jnp.where(level < levels // 2, levels - k, k)).start()

    def depth_step(t):
        summed = plane_out[t, level].astype(f32)
        for k in range(1, levels):
            depth_copy(t, k).wait_recv()
            summed = summed + depth_in[t, k].astype(f32)
        summed = summed.astype(bf16).astype(f32)
        for place, source in enumerate(pair_sources(t)):
            at = pl.ds(pl.multiple_of(source * lanes, lanes), lanes)
            total = state_rows[:, at].astype(f32) + summed[:, place * lanes : (place + 1) * lanes]
            out_ref[:, at] = total.astype(bf16)

    count = shards // 2

    def stage(t, carry):
        for turn in range(levels + 1):
            if batches.get(50 + turn):

                @pl.when(t == turn)
                def _():
                    issue(50 + turn)

        @pl.when(t < count)
        def _():
            with jax.named_scope("lower_step"):
                lower_step(t)

        @pl.when((t >= 1) & (t < count + 1))
        def _():
            with jax.named_scope("pair_step"):
                pair_step(t - 1)

        @pl.when(t >= LAG)
        def _():
            with jax.named_scope("depth_step"):
                depth_step(t - LAG)

        return carry

    lax.fori_loop(0, count + LAG, stage, 0)

    phase("drain")
    @pl.when(sp < shards - 1)
    def _():
        for one in halo_copies:
            one.wait_send()

    for one in state_copies + back_copies:
        one.wait_send()
    @pl.when(own_team == 0)
    def _():
        cross.wait_send()

    swap.wait_send()
    for part in range(parts):
        for place in range(levels):
            share(place, part).wait_send()
        for hop in range(top):

            @pl.when((level >= hop) & (level < top))
            def _():
                along(level_at(-hop), part, hop, True).wait_send()

            @pl.when((level + hop <= top) & (level > 0))
            def _():
                along(level_at(hop), part, hop, False).wait_send()

    for kind in range(2):
        for step in range(levels):
            for way in range(2):
                spread(kind, step, way).wait_send()
                relay(kind, step, way).wait_send()
            if step:
                rise(kind, step).wait_send()

    def drain(t, carry):
        pair_copy(t).wait_send()
        for k in range(1, levels):
            depth_copy(t, k).wait_send()
        return carry

    lax.fori_loop(0, count, drain, 0)
    phase("")


LAG = 3


def plan(levels):
    ur, dr = ([("rise", kind, step) for step in range(1, levels)] for kind in range(2))
    us, ds = ([("spread", kind, step) for step in range(levels)] for kind in range(2))
    ut, dt = ([("relay", kind, step) for step in range(levels)] for kind in range(2))
    return {0: [('rise', 0, 1), ('rise', 0, 2), ('spread', 0, 0)], 1: [('rise', 0, 3), ('relay', 0, 0), ('spread', 1, 0), ('spread', 0, 1)], 3: [('relay', 1, 0), ('rise', 1, 1), ('rise', 1, 2), ('rise', 1, 3), ('spread', 0, 2), ('spread', 0, 3)], 4: [('relay', 0, 1), ('relay', 0, 2), ('relay', 0, 3)], 13: [('spread', 1, 1), ('spread', 1, 2), ('spread', 1, 3)], 50: [('relay', 1, 1)], 51: [('relay', 1, 2)], 52: [('relay', 1, 3)]}


def per_device_fused(team, *operands):
    (
        skip_stream_entering,
        content_signal_matrix,
        writer_signal_matrix,
        reader_signal_matrix,
        multiplier_signal,
        interval_before_softplus,
        extra_log_shrink,
        log_forget_speed,
        content_filter_coefs,
        writer_filter_coefs,
        reader_filter_coefs,
        skip_path_factor,
        cluster_scaling_vector,
        blend_result_matrix,
        feature_blend_scaling,
        widening_matrix,
        narrowing_matrix,
    ) = operands
    f32, bf16 = jnp.float32, jnp.bfloat16
    shards = lax.axis_size("sp")
    length, inner = content_signal_matrix.shape
    state_width = writer_signal_matrix.shape[1]
    local_heads = interval_before_softplus.shape[0]
    rows_own, model = skip_stream_entering.shape
    levels = shards // 4
    unit = widening_matrix.shape[1] // levels
    depth = widening_matrix.shape[0]
    lanes = narrowing_matrix.shape[1]
    slice_width = inner // team
    pairs = shards // 2
    dma = pltpu.SemaphoreType.DMA
    vmem, anywhere = pl.BlockSpec(memory_space=pltpu.VMEM), pl.BlockSpec(memory_space=pl.ANY)
    specs = [anywhere] * 5 + [vmem] * 8 + [anywhere, vmem, anywhere, anywhere]
    scratch = [
        pltpu.VMEM((rows_own, model), bf16),
        pltpu.VMEM((length, inner), bf16),
        pltpu.VMEM((length, state_width), bf16),
        pltpu.VMEM((length, state_width), bf16),
        pltpu.VMEM((length, inner), bf16),
        pltpu.VMEM((16, inner + 2 * state_width), bf16),
        pltpu.VMEM((8 + length, inner + 2 * state_width), f32),
        pltpu.VMEM((length, inner), f32),
        pltpu.VMEM((length, 2 * state_width), bf16),
        pltpu.VMEM(blend_result_matrix.shape, bf16),
        pltpu.VMEM((shards, depth, unit), bf16),
        pltpu.VMEM((shards, unit, lanes), bf16),
        pltpu.VMEM((length, local_heads * length), f32),
        pltpu.VMEM((local_heads, length), f32),
        pltpu.VMEM((length, inner), f32),
        pltpu.VMEM((length, inner), f32),
        pltpu.VMEM((team, STATE + 16, slice_width), bf16),
        pltpu.VMEM((team, STATE + 16, slice_width), bf16),
        pltpu.VMEM((team, STATE, slice_width), f32),
        pltpu.VMEM((team, 8, slice_width), f32),
        pltpu.VMEM((STATE, slice_width), bf16),
        pltpu.VMEM((STATE, slice_width), bf16),
        pltpu.VMEM((team, STATE, slice_width), bf16),
        pltpu.VMEM((team, STATE, slice_width), bf16),
        pltpu.VMEM((length, inner), bf16),
        pltpu.VMEM((2, rows_own, model), bf16),
        pltpu.VMEM((rows_own, model), bf16),
        pltpu.VMEM((rows_own, model), bf16),
        pltpu.VMEM((2, levels, rows_own, model), bf16),
        pltpu.VMEM((2, levels * rows_own, unit), bf16),
        pltpu.VMEM((pairs, levels * rows_own, 2 * lanes), bf16),
        pltpu.VMEM((pairs, levels * rows_own, 2 * lanes), bf16),
        pltpu.VMEM((pairs, levels, rows_own, 2 * lanes), bf16),
        pltpu.VMEM((pairs, levels, rows_own, 2 * lanes), bf16),
        dma((8,)),
        dma((3,)),
        dma((3,)),
        dma((3 * levels,)),
        dma((shards,)),
        dma((3 * levels,)),
        dma((shards,)),
        dma((4 * levels,)),
        dma((4 * levels,)),
        dma((team,)),
        dma((team,)),
        dma,
        dma,
        dma((team,)),
        dma((team,)),
        dma,
        dma,
        dma((4 * levels,)),
        dma((2 * levels,)),
        dma((2 * levels,)),
        dma((2 * levels,)),
        dma((pairs,)),
        dma((pairs,)),
        dma((pairs, levels)),
        dma((pairs, levels)),
    ]
    return pl.pallas_call(
        functools.partial(layer_kernel, team),
        out_shape=jax.ShapeDtypeStruct((rows_own, model), bf16),
        in_specs=specs,
        out_specs=vmem,
        scratch_shapes=scratch,
        compiler_params=pltpu.CompilerParams(
            collective_id=0, has_side_effects=True, vmem_limit_bytes=63 * 1024 * 1024
        ),
    )(
        skip_stream_entering,
        content_signal_matrix,
        writer_signal_matrix,
        reader_signal_matrix,
        multiplier_signal,
        interval_before_softplus,
        extra_log_shrink,
        log_forget_speed.reshape(1, -1),
        content_filter_coefs,
        writer_filter_coefs,
        reader_filter_coefs,
        skip_path_factor.reshape(1, -1),
        cluster_scaling_vector.reshape(1, -1),
        blend_result_matrix,
        feature_blend_scaling.reshape(1, -1),
        widening_matrix,
        narrowing_matrix,
    )


def general_solution(mesh):
    shards, halves = mesh.shape["sp"], mesh.shape["tp"]
    team = math.gcd(shards, TEAM)
    teams = jax.sharding.Mesh(
        mesh.devices.reshape(shards // team, team, halves), ("sa", "sb", "tp")
    )
    placed = (
        P(("sa", "sb", "tp"), None),
        P(SP, "tp"),
        P(SP, "tp"),
        P(SP, "tp"),
        P(SP, "tp"),
        P("tp", SP),
        P("tp", SP),
        P("tp"),
        P(None, "tp"),
        P(None, "tp"),
        P(None, "tp"),
        P("tp"),
        P("tp"),
        P("tp", None),
        P(),
        P(SP, "tp"),
        P("tp", SP),
    )
    return jax.shard_map(
        per_device, mesh=teams, in_specs=placed, out_specs=P(("sa", "sb", "tp"), None), check_vma=False
    )


def fits(shards, halves, team, rows, tokens, inner, hidden, model, state_width):
    length = tokens // shards
    local = inner // halves
    return (
        halves == 2
        and shards == 2 * team
        and team % 4 == 0
        and length == BLOCK
        and length % 32 == 0
        and local % (team * 128) == 0
        and shards % 4 == 0
        and (hidden // halves) % (shards // 4 * 128) == 0
        and (shards // 4) == 4
        and model % (shards * 128) == 0
        and (state_width // halves) % STATE == 0
        and (local // (state_width // halves // STATE)) % (local // team) == 0
    )


def solution(mesh):
    shards, halves = mesh.shape["sp"], mesh.shape["tp"]
    team = math.gcd(shards, TEAM)
    general = general_solution(mesh)
    row, both = P("sp", "tp"), P(("sp", "tp"), None)
    tp_first, tp_last, tp_only = P("tp", "sp"), P(None, "tp"), P("tp")
    placed = (
        (both, row, row, row, row, tp_first, tp_first, tp_only, tp_last, tp_last, tp_last)
        + (tp_only, tp_only, P("tp", None), P(), row, tp_first)
    )
    fused = jax.shard_map(
        functools.partial(per_device_fused, team),
        mesh=mesh,
        in_specs=placed,
        out_specs=both,
        check_vma=False,
    )

    def layer(*operands):
        tokens, inner = operands[1].shape
        model, hidden = operands[15].shape
        state_width = operands[2].shape[1]
        if fits(shards, halves, team, tokens, tokens, inner, hidden, model, state_width):
            return fused(*operands)
        return general(*operands)

    return layer
```

```python
import functools
import math
import jax
import jax.numpy as jnp
from jax import lax
from jax.experimental import pallas as pl
from jax.experimental.pallas import tpu as pltpu
from jax.sharding import PartitionSpec as P

HEAD_DIM = 64
STATE = 128
BLOCK = 128


epsilon = 1e-05
precise = lax.Precision.HIGHEST
SP = ("sa", "sb")
TEAM = 8


def shifted(value, axis, steps):
    count = lax.axis_size(axis)
    initial, last = (max(0, -steps), min(count, count - steps))
    return lax.ppermute(value, axis, [(source, source + steps) for source in range(initial, last)])


def scan_rows(parts, factors, entering):
    def one(place, carried):
        entering[place] = carried.astype(jnp.bfloat16)
        return carried * factors[place] + parts[place].astype(jnp.float32)

    lax.fori_loop(0, parts.shape[0], one, jnp.zeros(parts.shape[1:], jnp.float32))


def prefix(log_total, end_state, rider):
    shards = lax.axis_size(SP)
    heads = end_state.shape[0] * end_state.shape[1]
    state_width = end_state.shape[-1]
    rows = end_state.reshape(-1, state_width).astype(jnp.bfloat16)
    count = rows.shape[0] // shards
    decays = jnp.repeat(jnp.exp(log_total).reshape(heads), rows.shape[0] // heads)
    extra = -(-count // state_width) * 16
    decays = decays.astype(jnp.bfloat16).reshape(shards, count)
    decays = jnp.pad(decays, ((0, 0), (0, extra * state_width - count)))
    packed = jnp.concatenate(
        [rows.reshape(shards, count, state_width), decays.reshape(shards, extra, state_width)],
        axis=1,
    )
    packed = lax.all_to_all(packed, SP, split_axis=0, concat_axis=0)
    parts = packed[:, :count]
    factors = packed[:, count:].reshape(shards, -1)[:, :count].astype(jnp.float32)
    entering = pl.pallas_call(
        scan_rows,
        out_shape=jax.ShapeDtypeStruct(parts.shape, jnp.bfloat16),
    )(parts, jnp.broadcast_to(factors[..., None], parts.shape))
    entering, rider = lax.optimization_barrier((entering, rider))
    back = lax.all_to_all(
        entering.reshape(rows.shape), SP, split_axis=0, concat_axis=0, tiled=True
    )
    return back.reshape(end_state.shape).astype(jnp.float32), rider


def summed_share(partial, axis):
    count = lax.axis_size(axis)
    if count != 2:
        return lax.psum_scatter(partial, axis, scatter_dimension=0, tiled=True)
    me = lax.axis_index(axis)
    length = partial.shape[0] // 2
    away = lax.dynamic_slice_in_dim(partial, (1 - me) * length, length, 0)
    kept = lax.dynamic_slice_in_dim(partial, me * length, length, 0)
    arrived = lax.ppermute(away, axis, [(0, 1), (1, 0)])
    return (kept.astype(jnp.float32) + arrived.astype(jnp.float32)).astype(jnp.bfloat16)


def convolve(inputs, rim_rows, conv_taps):
    width = conv_taps.shape[0]
    length = inputs.shape[0]
    extended = jnp.concatenate([rim_rows, inputs], axis=0)
    summed = extended[0:length].astype(jnp.float32) * conv_taps[0].astype(jnp.float32)
    for offset in range(1, width):
        summed = summed + extended[offset : offset + length].astype(jnp.float32) * conv_taps[
            offset
        ].astype(jnp.float32)
    return jax.nn.silu(summed)


def advance(carried, pair):
    block_state, block_factor = pair
    return (carried * block_factor[..., None, None] + block_state, carried)


def blockwise(values, interval_lengths, log_forgetting, key_rows, query_rows):
    length, groups, per_group, width = values.shape
    blocks = length // BLOCK
    value_blocks = values.reshape(blocks, BLOCK, groups, per_group, width)
    step_blocks = jnp.transpose(
        interval_lengths.reshape(groups, per_group, blocks, BLOCK), (2, 3, 0, 1)
    )
    weighted = value_blocks * step_blocks[..., None]
    cumulative = jnp.cumsum(
        jnp.transpose(log_forgetting.reshape(groups, per_group, blocks, BLOCK), (2, 0, 1, 3)),
        axis=-1,
    )
    key_blocks = key_rows.reshape(blocks, BLOCK, groups, -1)
    query_blocks = query_rows.reshape(blocks, BLOCK, groups, -1)
    causal = jnp.tril(jnp.ones((BLOCK, BLOCK), dtype=bool))
    decay_mask = jnp.exp(
        jnp.where(causal, cumulative[..., :, None] - cumulative[..., None, :], -jnp.inf)
    )
    scores = jnp.einsum("clgn,csgn->cgls", query_blocks, key_blocks, precision=precise)
    within = jnp.einsum("cgls,cgrls,csgrp->clgrp", scores, decay_mask, weighted, precision=precise)
    to_end = jnp.exp(cumulative[..., -1:] - cumulative)
    states = jnp.einsum("clgn,cgrl,clgrp->cgrpn", key_blocks, to_end, weighted, precision=precise)
    block_totals = cumulative[..., -1]
    initial = jnp.zeros(states.shape[1:], jnp.float32)
    final, entering = lax.scan(advance, initial, (states, jnp.exp(block_totals)))
    carried = jnp.einsum(
        "clgn,cgrpn,cgrl->clgrp", query_blocks, entering, jnp.exp(cumulative), precision=precise
    )
    from_start = (jnp.cumsum(block_totals, axis=0) - block_totals)[..., None] + cumulative
    return (within + carried, final, from_start, jnp.sum(block_totals, axis=0))


def normalize(rows, gain):
    widened = rows.astype(jnp.float32)
    scaled = widened * lax.rsqrt(jnp.mean(widened * widened, axis=-1, keepdims=True) + epsilon)
    return (scaled * gain).astype(jnp.bfloat16)


def per_device(
    skip_stream_entering,
    content_signal_matrix,
    writer_signal_matrix,
    reader_signal_matrix,
    multiplier_signal,
    interval_before_softplus,
    extra_log_shrink,
    log_forget_speed,
    content_filter_coefs,
    writer_filter_coefs,
    reader_filter_coefs,
    skip_path_factor,
    cluster_scaling_vector,
    blend_result_matrix,
    feature_blend_scaling,
    widening_matrix,
    narrowing_matrix,
):
    up_part = lax.all_to_all(widening_matrix, "sb", split_axis=1, concat_axis=0, tiled=True)
    narrowing_matrix, up_part = lax.optimization_barrier((narrowing_matrix, up_part))
    up_use = lax.all_gather(up_part, "sa", axis=0, tiled=True)
    down_part = lax.all_to_all(narrowing_matrix, "sb", split_axis=0, concat_axis=1, tiled=True)
    (
        content_signal_matrix,
        writer_signal_matrix,
        reader_signal_matrix,
        interval_before_softplus,
        down_part,
    ) = lax.optimization_barrier(
        (
            content_signal_matrix,
            writer_signal_matrix,
            reader_signal_matrix,
            interval_before_softplus,
            down_part,
        )
    )
    down_use = lax.all_gather(down_part, "sa")
    rim_width = content_filter_coefs.shape[0] - 1
    length = content_signal_matrix.shape[0]
    signals = (content_signal_matrix, writer_signal_matrix, reader_signal_matrix)
    tails = jnp.concatenate([signal[length - rim_width :] for signal in signals], axis=1)
    rims = shifted(tails, SP, 1)
    first, second = signals[0].shape[1], signals[0].shape[1] + signals[1].shape[1]
    values = convolve(signals[0], rims[:, :first], content_filter_coefs)
    key_rows = convolve(signals[1], rims[:, first:second], writer_filter_coefs)
    query_rows = convolve(signals[2], rims[:, second:], reader_filter_coefs)
    local_heads = interval_before_softplus.shape[0]
    local_groups = writer_signal_matrix.shape[1] // STATE
    per_group = local_heads // local_groups
    interval_lengths = jax.nn.softplus(interval_before_softplus)
    log_forgetting = extra_log_shrink - jnp.exp(log_forget_speed)[:, None] * interval_lengths
    shaped = values.reshape(length, local_groups, per_group, HEAD_DIM)
    local_out, end_state, from_start, device_total = blockwise(
        shaped,
        interval_lengths.reshape(local_groups, per_group, length),
        log_forgetting.reshape(local_groups, per_group, length),
        key_rows,
        query_rows,
    )
    incoming, up_use = prefix(device_total, end_state, up_use)
    query_blocks = query_rows.reshape(length // BLOCK, BLOCK, local_groups, STATE)
    arriving = jnp.einsum(
        "clgn,grpn,cgrl->clgrp", query_blocks, incoming, jnp.exp(from_start), precision=precise
    )
    scan_out = (local_out + arriving).reshape(length, local_heads * HEAD_DIM)
    gated = (scan_out + jnp.repeat(skip_path_factor, HEAD_DIM) * values) * jax.nn.silu(
        multiplier_signal.astype(jnp.float32)
    )
    grouped = gated.reshape(length, local_groups, -1)
    grouped = grouped * lax.rsqrt(jnp.mean(grouped * grouped, axis=-1, keepdims=True) + epsilon)
    heads_out = (grouped.reshape(length, -1) * cluster_scaling_vector).astype(jnp.bfloat16)
    mixer_rows = summed_share(
        jnp.dot(heads_out, blend_result_matrix, preferred_element_type=jnp.float32).astype(
            jnp.bfloat16
        ),
        "tp",
    )
    own_rows = (skip_stream_entering.astype(jnp.float32) + mixer_rows.astype(jnp.float32)).astype(
        jnp.bfloat16
    )
    normed = normalize(own_rows, feature_blend_scaling)
    down_whole = jnp.concatenate([down_use[k] for k in range(down_use.shape[0])], axis=1)

    def mixed(rows):
        lifted = jax.nn.relu(jnp.dot(rows, up_use, preferred_element_type=jnp.float32))
        hidden = (lifted * lifted).astype(jnp.bfloat16)
        partial = jnp.dot(hidden, down_whole, preferred_element_type=jnp.float32)
        return partial.astype(jnp.bfloat16)

    if lax.axis_size("tp") == 2:
        members, width = lax.axis_size("sb"), normed.shape[1]
        swap = [(0, 1), (1, 0)]
        copies = jnp.broadcast_to(normed[None], (members,) + normed.shape)
        own_half = lax.all_to_all(copies, "sb", split_axis=0, concat_axis=0)
        own_half = own_half.reshape(-1, width)
        other_half = lax.ppermute(own_half, "tp", swap)
        arrived = lax.ppermute(mixed(other_half), "tp", swap)
        joined = mixed(own_half).astype(jnp.float32) + arrived.astype(jnp.float32)
        joined = joined.astype(jnp.bfloat16).reshape(members, -1, width)
        shares = lax.all_to_all(joined, "sb", split_axis=0, concat_axis=0)
        mlp_rows = jnp.sum(shares.astype(jnp.float32), axis=0)
    else:
        team_rows = lax.all_gather(normed, ("sb", "tp"), axis=0, tiled=True)
        mlp_rows = lax.psum_scatter(
            mixed(team_rows), ("sb", "tp"), scatter_dimension=0, tiled=True
        )
    mlp_rows = mlp_rows.astype(jnp.bfloat16)
    return (own_rows.astype(jnp.float32) + mlp_rows.astype(jnp.float32)).astype(jnp.bfloat16)


TEAM_LINKS = pl.DeviceIdType.MESH


def split3(wide):
    one = wide.astype(jnp.bfloat16)
    rest = wide - one.astype(jnp.float32)
    two = rest.astype(jnp.bfloat16)
    return one, two, (rest - two.astype(jnp.float32)).astype(jnp.bfloat16)


def contract(left, right, dims):
    return lax.dot_general(left, right, (dims, ((), ())), preferred_element_type=jnp.float32)


def exact(left, right, dims, left_split):
    if left_split:
        terms = [contract(part, right, dims) for part in split3(left)]
    else:
        terms = [contract(left, part, dims) for part in split3(right)]
    return terms[0] + terms[1] + terms[2]


def selector(rows, columns, per_row):
    row = lax.broadcasted_iota(jnp.int32, (rows, columns), 0)
    column = lax.broadcasted_iota(jnp.int32, (rows, columns), 1)
    return jnp.where(column // per_row == row, 1.0, 0.0).astype(jnp.bfloat16)


def layer_kernel(
    team,
    skip_hbm,
    content_hbm,
    writer_hbm,
    reader_hbm,
    multiplier_hbm,
    interval_ref,
    shrink_ref,
    speed_ref,
    content_taps,
    writer_taps,
    reader_taps,
    skip_factor,
    cluster_gain,
    blend_hbm,
    feature_gain,
    up_hbm,
    down_hbm,
    mixed_ref,
    out_ref,
    skip_ref,
    content_ref,
    writer_ref,
    reader_ref,
    multiplier_ref,
    halo,
    wide,
    values,
    keyquery,
    blend,
    up,
    down,
    column_decay,
    row_decay,
    scan,
    scale_in,
    state_out,
    state_in,
    entering,
    kept_decay,
    cross_out,
    cross_in,
    back_out,
    back_in,
    heads,
    part_out,
    part_in,
    acts,
    hidden,
    pair_out,
    pair_in,
    plane_out,
    depth_in,
    local_sem,
    halo_ss,
    halo_rs,
    up_ss,
    up_rs,
    down_ss,
    down_rs,
    half_ss,
    half_rs,
    st_ss,
    st_rs,
    cr_ss,
    cr_rs,
    bk_ss,
    bk_rs,
    pt_ss,
    pt_rs,
    ap_ss,
    ap_rs,
    ad_ss,
    ad_rs,
    pr_ss,
    pr_rs,
    dp_ss,
    dp_rs,
):
    f32, bf16 = jnp.float32, jnp.bfloat16
    batches = plan(lax.axis_size("sp") // 4)
    shards = lax.axis_size("sp")
    sp, tp = lax.axis_index("sp"), lax.axis_index("tp")
    own_team, me = sp // team, lax.rem(sp, team)
    length, inner = content_ref.shape
    state_width = writer_ref.shape[1]
    local_heads = interval_ref.shape[0]
    groups = state_width // STATE
    group_width = inner // groups
    model = skip_ref.shape[1]
    unit = up.shape[2]
    slice_width = inner // team
    half = team // 2
    rows_own = skip_ref.shape[0]

    open_scope = []

    def phase(name):
        if open_scope:
            open_scope.pop().__exit__(None, None, None)
        if name:
            open_scope.append(jax.named_scope(name))
            open_scope[-1].__enter__()

    def copy(src, dst, ss, rs, sp_to, tp_to):
        return pltpu.make_async_remote_copy(
            src_ref=src,
            dst_ref=dst,
            send_sem=ss,
            recv_sem=rs,
            device_id=(sp_to, tp_to),
            device_id_type=TEAM_LINKS,
        )

    def mate(step):
        return own_team * team + lax.rem(me + step, team)

    level, spot = sp // 4, lax.rem(sp, 4)
    beside = (spot + 1 - 2 * lax.rem(spot, 2), lax.rem(spot + 2, 4))
    levels = shards // 4

    def level_at(step):
        return lax.rem(level + levels + step, levels)

    def weight_piece(kind, index):
        offset = pl.ds(pl.multiple_of(index * unit, unit), unit)
        return up_hbm.at[:, offset] if kind == 0 else down_hbm.at[offset, :]

    def weight_copy(kind, src, source, place, target):
        into, ss, rs = ((up, up_ss, up_rs), (down, down_ss, down_rs))[kind]
        if src is None:
            src = into.at[source]
        return copy(src, into.at[source], ss.at[place], rs.at[source], target, tp)

    def source_level(step, kind):
        if kind == 0 or step == 0:
            return level_at(-step)
        return step - 1 + jnp.where(level <= step - 1, 1, 0)

    def rise(kind, step):
        to = level_at(step)
        return weight_copy(kind, weight_piece(kind, to), sp, step, to * 4 + spot)

    def spread(kind, step, way):
        source = source_level(step, kind) * 4 + spot
        piece = weight_piece(kind, level) if step == 0 else None
        place = levels * (1 + way) + step
        return weight_copy(kind, piece, source, place, level * 4 + beside[way])

    def relay(kind, step, way):
        at_level = source_level(step, kind)
        return diagonal(kind, at_level, at_level * 4 + beside[way], way, step)

    def diagonal(kind, at_level, source, way, step):
        part = pl.ds(way * (unit // 2), unit // 2)
        held = up.at[source, :, part] if kind == 0 else down.at[source, part, :]
        place = kind * 2 * levels + way * levels
        target = level * 4 + beside[1 - way]
        return copy(held, held, half_ss.at[place + step], half_rs.at[place + at_level], target, tp)

    def neighbour(kind, step, way):
        return weight_copy(kind, None, source_level(step, kind) * 4 + beside[way], 0, sp)

    def issue(batch):
        for what, kind, step in batches.get(batch, ()):
            if what == "rise":
                rise(kind, step).start()
            if what == "spread":
                if step:
                    spread(kind, step, 0).wait_recv()
                for way in range(2):
                    spread(kind, step, way).start()
            if what == "spread level":

                @pl.when(level != step)
                def _():
                    source = step * 4 + spot
                    slot = levels + step + jnp.where(level > step, 1, 0)
                    for way in range(2):
                        target = level * 4 + beside[way]
                        passing = weight_copy(kind, None, source, slot + way * levels, target)
                        if way == 0:
                            passing.wait_recv()
                        passing.start()

            if what == "relay level":

                @pl.when(level != step)
                def _():
                    slot = step + jnp.where(level > step, 1, 0)
                    for way in range(2):
                        source = step * 4 + beside[way]
                        weight_copy(kind, None, source, 0, sp).wait_recv()
                        diagonal(kind, step, source, way, slot).start()

            if what == "relay":
                for way in range(2):
                    neighbour(kind, step, way).wait_recv()
                    relay(kind, step, way).start()

    local_up = pltpu.make_async_copy(weight_piece(0, level), up.at[sp], local_sem.at[0])
    local_down = pltpu.make_async_copy(weight_piece(1, level), down.at[sp], local_sem.at[1])
    local_blend = pltpu.make_async_copy(blend_hbm, blend, local_sem.at[2])
    brought = []
    for place, (source, into) in enumerate(
        (
            (content_hbm, content_ref),
            (writer_hbm, writer_ref),
            (reader_hbm, reader_ref),
            (multiplier_hbm, multiplier_ref),
            (skip_hbm, skip_ref),
        )
    ):
        brought.append(pltpu.make_async_copy(source, into, local_sem.at[3 + place]))
        brought[-1].start()
    local_up.start()
    local_down.start()
    local_blend.start()

    barrier = pltpu.get_barrier_semaphore()
    for step in range(1, shards):
        pl.semaphore_signal(
            barrier,
            inc=1,
            device_id=(lax.rem(sp + step, shards), tp),
            device_id_type=TEAM_LINKS,
        )
    pl.semaphore_signal(barrier, inc=1, device_id=(sp, 1 - tp), device_id_type=TEAM_LINKS)

    phase("decays")
    steps = interval_ref[...]
    steps = jnp.maximum(steps, 0.0) + jnp.log1p(jnp.exp(-jnp.abs(steps)))
    head_row = lax.broadcasted_iota(jnp.int32, (local_heads, local_heads), 0)
    head_column = lax.broadcasted_iota(jnp.int32, (local_heads, local_heads), 1)
    speed = jnp.where(head_row == head_column, speed_ref[...], 0.0)
    forget = shrink_ref[...] - jnp.exp(jnp.sum(speed, axis=1, keepdims=True)) * steps
    row_index = lax.broadcasted_iota(jnp.int32, (length, length), 0)
    column_index = lax.broadcasted_iota(jnp.int32, (length, length), 1)
    lower = jnp.where(row_index >= column_index, 1.0, 0.0).astype(bf16)
    upper = jnp.where(row_index <= column_index, 1.0, 0.0).astype(bf16)
    unity = jnp.where(row_index == column_index, 1.0, 0.0).astype(bf16)
    log_steps = jnp.log(steps)
    total_rows = exact(forget, upper, ((1,), (0,)), True)
    total_columns = exact(lower, forget, ((1,), (1,)), False)
    log_columns = exact(unity, log_steps, ((1,), (1,)), False)
    row_decay[...] = total_rows - log_steps
    by_head = selector(local_heads, local_heads * length, length)
    column_decay[...] = exact(total_columns, by_head, ((1,), (0,)), True)
    by_channel = selector(local_heads, inner, HEAD_DIM)
    scale_in[...] = exact(jnp.exp(total_columns), by_channel, ((1,), (0,)), True)
    last = total_columns[length - 1 : length, :]
    to_end = jnp.exp(last - total_columns + log_columns)
    end_scale = exact(to_end, by_channel, ((1,), (0,)), True)
    whole_decay = exact(
        jnp.broadcast_to(jnp.exp(last), (16, local_heads)), by_channel, ((1,), (0,)), True
    )
    skip_scale = exact(
        jnp.broadcast_to(skip_factor[...], (16, local_heads)), by_channel, ((1,), (0,)), True
    )

    for one in brought[:3]:
        one.wait()
    phase("barrier_wait")
    pl.semaphore_wait(barrier, shards)
    phase("first_sends")
    following = lax.rem(sp + 1, shards)
    spans = ((content_ref, 0, inner), (writer_ref, inner, state_width))
    spans = spans + ((reader_ref, inner + state_width, state_width),)
    halo_copies = []
    for place, (ref, first, size) in enumerate(spans):
        halo_copies.append(
            copy(
                ref.at[pl.ds(length - 16, 16), :],
                halo.at[:, pl.ds(first, size)],
                halo_ss.at[place],
                halo_rs.at[place],
                following,
                tp,
            )
        )

    @pl.when(sp < shards - 1)
    def _():
        for one in halo_copies:
            one.start()

    issue(0)

    phase("rim_wait")
    @pl.when(sp > 0)
    def _():
        for one in halo_copies:
            one.wait_recv()

    @pl.when(sp == 0)
    def _():
        halo[...] = jnp.zeros_like(halo)

    phase("convolve")
    chunk = state_width
    for ref, taps, first, size in (
        (content_ref, content_taps, 0, inner),
        (writer_ref, writer_taps, inner, state_width),
        (reader_ref, reader_taps, inner + state_width, state_width),
    ):
        for start in range(0, size, chunk):
            at = slice(start, start + chunk)
            placed = slice(first + start, first + start + chunk)
            wide[8:, placed] = ref[:, at].astype(f32)
            wide[0:8, placed] = halo[:, placed].astype(f32)[8:, :]
            weights = taps[:, at].astype(f32)
            count = taps.shape[0]
            base = 8 - (count - 1)
            total = wide[base : base + length, placed] * weights[0:1, :]
            for k in range(1, count):
                total = total + wide[base + k : base + k + length, placed] * weights[k : k + 1, :]
            total = total * (1.0 / (1.0 + jnp.exp(-total)))
            if first == 0:
                values[:, at] = total
            else:
                keyquery[:, first - inner + start : first - inner + start + chunk] = total.astype(bf16)

    phase("states")
    weighted = (values[...] * end_scale).astype(bf16)
    for g in range(groups):
        keys = keyquery[:, g * STATE : (g + 1) * STATE]
        made = contract(keys, weighted[:, g * group_width : (g + 1) * group_width], ((0,), (0,)))
        for part in range(group_width // slice_width):
            place = g * (group_width // slice_width) + part
            state_out[place, 0:STATE, :] = made[
                :, part * slice_width : (part + 1) * slice_width
            ].astype(bf16)
    high = whole_decay.astype(bf16)
    low = (whole_decay - high.astype(f32)).astype(bf16)
    first_row = lax.broadcasted_iota(jnp.int32, whole_decay.shape, 0) == 0
    packed = jnp.where(first_row, high.astype(f32), low.astype(f32)).astype(bf16)
    for place in range(team):
        state_out[place, STATE : STATE + 16, :] = packed[
            :, place * slice_width : (place + 1) * slice_width
        ]
    state_in[me] = state_out[me]
    state_copies = []
    for step in range(1, team):
        target = mate(step)
        state_copies.append(
            copy(
                state_out.at[lax.rem(target, team)],
                state_in.at[me],
                st_ss.at[step],
                st_rs.at[me],
                target,
                tp,
            )
        )
        state_copies[-1].start()
    issue(1)

    phase("within")
    causal = row_index >= column_index
    causal_pair = jnp.concatenate([causal, causal], axis=1)
    lane = lax.broadcasted_iota(jnp.int32, (length, 2 * HEAD_DIM), 1)
    pairs_per_group = group_width // (2 * HEAD_DIM)
    for g in range(groups):
        keys = keyquery[:, g * STATE : (g + 1) * STATE]
        queries = keyquery[:, state_width + g * STATE : state_width + (g + 1) * STATE]
        scores = contract(queries, keys, ((1,), (1,)))
        scores = jnp.concatenate([scores, scores], axis=1)
        for j in range(pairs_per_group):
            i = g * pairs_per_group + j
            rows = jnp.concatenate(
                [row_decay[2 * i : 2 * i + 1, :], row_decay[2 * i + 1 : 2 * i + 2, :]], axis=1
            )
            gap = column_decay[:, 2 * i * length : (2 * i + 2) * length] - rows
            decay = jnp.exp(jnp.where(causal_pair, gap, -jnp.inf))
            mixing = (scores * decay).astype(bf16)
            both = values[:, i * 2 * HEAD_DIM : (i + 1) * 2 * HEAD_DIM]
            blocks = jnp.concatenate(
                [jnp.where(lane < HEAD_DIM, both, 0.0), jnp.where(lane < HEAD_DIM, 0.0, both)],
                axis=0,
            ).astype(bf16)
            scan[:, i * 2 * HEAD_DIM : (i + 1) * 2 * HEAD_DIM] = contract(
                mixing, blocks, ((1,), (0,))
            )
    scan[...] = scan[...] + skip_scale[0:1, :] * values[...]

    phase("state_wait")
    carried = jnp.zeros((STATE, slice_width), f32)
    kept = jnp.ones((1, slice_width), f32)
    for step in range(1, team):
        source = lax.rem(me + step, team)
        copy(
            state_in.at[source], state_in.at[source], st_ss.at[step], st_rs.at[source], sp, tp
        ).wait_recv()
    phase("prefix")
    for place in range(team):
        entering[place] = carried
        kept_decay[place] = jnp.broadcast_to(kept, (8, slice_width))
        tail = state_in[place, STATE : STATE + 16, :].astype(f32)
        factor = tail[0:1, :] + tail[1:2, :]
        carried = carried * factor + state_in[place, 0:STATE, :].astype(f32)
        kept = kept * factor
    cross_out[...] = carried.astype(bf16)
    cross = copy(cross_out, cross_in, cr_ss, cr_rs, team + me, tp)

    @pl.when(own_team == 0)
    def _():
        cross.start()

    issue(2)
    phase("cross_wait")
    @pl.when(own_team > 0)
    def _():
        cross.wait_recv()

    phase("back")

    @pl.when(own_team == 0)
    def _():
        back_out[...] = entering[...].astype(bf16)

    @pl.when(own_team > 0)
    def _():
        earlier = cross_in[...].astype(f32)
        for place in range(team):
            back_out[place] = (entering[place] + kept_decay[place, 0:1, :] * earlier).astype(bf16)

    back_in[me] = back_out[me]
    back_copies = []
    for step in range(1, team):
        target = mate(step)
        back_copies.append(
            copy(
                back_out.at[lax.rem(target, team)],
                back_in.at[me],
                bk_ss.at[step],
                bk_rs.at[me],
                target,
                tp,
            )
        )
        back_copies[-1].start()
    issue(3)
    phase("back_wait")
    for step in range(1, team):
        source = lax.rem(me + step, team)
        copy(
            back_in.at[source], back_in.at[source], bk_ss.at[step], bk_rs.at[source], sp, tp
        ).wait_recv()

    phase("gate")
    brought[3].wait()
    for g in range(groups):
        queries = keyquery[:, state_width + g * STATE : state_width + (g + 1) * STATE]
        at = slice(g * group_width, (g + 1) * group_width)
        per = group_width // slice_width
        incoming = jnp.concatenate([back_in[g * per + part] for part in range(per)], axis=1)
        arriving = contract(queries, incoming, ((1,), (0,))) * scale_in[:, at]
        gate = multiplier_ref[:, at].astype(f32)
        gated = (scan[:, at] + arriving) * (gate * (1.0 / (1.0 + jnp.exp(-gate))))
        gated = gated * lax.rsqrt(jnp.mean(gated * gated, axis=1, keepdims=True) + epsilon)
        heads[:, at] = (gated * cluster_gain[:, at]).astype(bf16)

    phase("project")
    local_blend.wait()
    column_chunk = 512

    def project(index, carry):
        at = pl.ds(pl.multiple_of(index * column_chunk, column_chunk), column_chunk)
        product = contract(heads[...], blend[:, at], ((1,), (0,))).astype(bf16)
        part_out[0, :, at] = product[0:rows_own, :]
        part_out[1, :, at] = product[rows_own:, :]
        return carry

    lax.fori_loop(0, model // column_chunk, project, 0)
    swap = copy(part_out.at[1 - tp], part_in, pt_ss, pt_rs, sp, 1 - tp)
    swap.start()
    phase("swap_wait")
    swap.wait_recv()
    phase("norm")
    brought[4].wait()
    mixed = (part_out[tp].astype(f32) + part_in[...].astype(f32)).astype(bf16)
    state = (skip_ref[...].astype(f32) + mixed.astype(f32)).astype(bf16)
    mixed_ref[...] = state
    state = state.astype(f32)
    state = state * lax.rsqrt(jnp.mean(state * state, axis=1, keepdims=True) + epsilon)
    acts[tp, level] = (state * feature_gain[...]).astype(bf16)

    phase("gather")
    parts = 2

    def rows_to(place, part, ss, rs, target, core):
        rows = pl.ds(part * (rows_own // parts), rows_own // parts)
        held = acts.at[tp, place, rows]
        return copy(held, held, ss, rs.at[place * parts + part], target, core)

    top = levels - 1

    def along(place, part, hop, up_way):
        to = level_at(1 if up_way else -1) * 4 + spot
        order = (hop + (0 if up_way else levels)) * parts + part
        return rows_to(place, part, ap_ss.at[order], ap_rs, to, tp)

    def share(place, part):
        return rows_to(place, part, ad_ss.at[place * parts + part], ad_rs, sp, 1 - tp)

    def up_ready():
        local_up.wait()
        for step in range(levels):
            for way in range(2):
                diagonal(0, step, step * 4 + 3 - spot, way, 0).wait_recv()

    def lift(block):
        count = levels // 2
        for place in range(count):
            for part in range(parts):
                share(block * count + place, part).wait_recv()
        up_whole = (shards * up.shape[1], unit)
        at = pl.ds(pl.multiple_of(block * count * rows_own, count * rows_own), count * rows_own)

        def one(core, carry):
            rows = acts[core, pl.ds(block * count, count)].reshape(count * rows_own, model)
            lifted = jnp.maximum(contract(rows, up[...].reshape(up_whole), ((1,), (0,))), 0.0)
            hidden[core, at, :] = (lifted * lifted).astype(bf16)
            return carry

        lax.fori_loop(0, 2, one, 0)

    def send_along(hop, part):
        @pl.when((level >= hop) & (level < top))
        def _():
            along(level_at(-hop), part, hop, True).start()

        @pl.when((level + hop <= top) & (level > 0))
        def _():
            along(level_at(hop), part, hop, False).start()

    for part in range(parts):
        send_along(0, part)
        share(level, part).start()
    issue(4)
    phase("line_wait")
    for hop in range(1, levels):
        for part in range(parts):
            for up_way in (True, False):
                place = level_at(-hop if up_way else hop)

                @pl.when(level >= hop if up_way else level + hop <= top)
                def _():
                    along(place, part, hop, up_way).wait_recv()
                    if hop < top:

                        @pl.when(level < top if up_way else level > 0)
                        def _():
                            along(place, part, hop, up_way).start()

                    share(place, part).start()

        issue(3 + 10 * hop)
        if hop == levels - 2:
            up_ready()
            lift(level // 2)
    issue(5)
    phase("lift")
    lift(1 - level // 2)
    issue(7)

    phase("lower")
    local_down.wait()
    lanes = down.shape[2]

    def pair_sources(t):
        row = lax.rem(t // levels + spot // 2, 2)
        first = lax.rem(t, levels) * 4 + row * 2
        return first, first + 1

    def pair_copy(t):
        return copy(pair_out.at[t], pair_in.at[t], pr_ss.at[t], pr_rs.at[t], sp, 1 - tp)

    def depth_copy(t, k):
        to = level_at(k)
        return copy(
            plane_out.at[t, to],
            depth_in.at[t, k],
            dp_ss.at[t, k],
            dp_rs.at[t, k],
            to * 4 + spot,
            tp,
        )

    def lower_step(t):
        sources = pair_sources(t)

        @pl.when(t >= levels)
        def _():
            for way in range(2):
                at_level = lax.rem(t, levels)
                diagonal(1, at_level, at_level * 4 + 3 - spot, way, 0).wait_recv()

        both = jnp.concatenate([down[sources[0]], down[sources[1]]], axis=1)
        pair_out[t] = contract(hidden[1 - tp], both, ((1,), (0,))).astype(bf16)
        pair_copy(t).start()
        plane_sum = contract(hidden[tp], both, ((1,), (0,)))
        plane_out[t] = plane_sum.astype(bf16).reshape(levels, rows_own, 2 * lanes)

    def pair_step(t):
        pair_copy(t).wait_recv()
        summed = plane_out[t].astype(f32) + pair_in[t].reshape(
            levels, rows_own, 2 * lanes
        ).astype(f32)
        plane_out[t] = summed.astype(bf16)
        for k in range(1, levels):
            depth_copy(t, jnp.where(level < levels // 2, levels - k, k)).start()

    def depth_step(t):
        summed = plane_out[t, level].astype(f32)
        for k in range(1, levels):
            depth_copy(t, k).wait_recv()
            summed = summed + depth_in[t, k].astype(f32)
        summed = summed.astype(bf16)
        for place, source in enumerate(pair_sources(t)):
            at = pl.ds(pl.multiple_of(source * lanes, lanes), lanes)
            out_ref[:, at] = summed[:, place * lanes : (place + 1) * lanes]

    count = shards // 2

    def stage(t, carry):
        for turn in range(levels + 1):
            if batches.get(50 + turn):

                @pl.when(t == turn)
                def _():
                    issue(50 + turn)

        @pl.when(t < count)
        def _():
            with jax.named_scope("lower_step"):
                lower_step(t)

        @pl.when((t >= 1) & (t < count + 1))
        def _():
            with jax.named_scope("pair_step"):
                pair_step(t - 1)

        @pl.when(t >= LAG)
        def _():
            with jax.named_scope("depth_step"):
                depth_step(t - LAG)

        return carry

    lax.fori_loop(0, count + LAG, stage, 0)

    phase("drain")
    @pl.when(sp < shards - 1)
    def _():
        for one in halo_copies:
            one.wait_send()

    for one in state_copies + back_copies:
        one.wait_send()
    @pl.when(own_team == 0)
    def _():
        cross.wait_send()

    swap.wait_send()
    for part in range(parts):
        for place in range(levels):
            share(place, part).wait_send()
        for hop in range(top):

            @pl.when((level >= hop) & (level < top))
            def _():
                along(level_at(-hop), part, hop, True).wait_send()

            @pl.when((level + hop <= top) & (level > 0))
            def _():
                along(level_at(hop), part, hop, False).wait_send()

    for kind in range(2):
        for step in range(levels):
            for way in range(2):
                spread(kind, step, way).wait_send()
                relay(kind, step, way).wait_send()
            if step:
                rise(kind, step).wait_send()

    def drain(t, carry):
        pair_copy(t).wait_send()
        for k in range(1, levels):
            depth_copy(t, k).wait_send()
        return carry

    lax.fori_loop(0, count, drain, 0)
    phase("")


LAG = 3


def plan(levels):
    ur, dr = ([("rise", kind, step) for step in range(1, levels)] for kind in range(2))
    us, ds = ([("spread", kind, step) for step in range(levels)] for kind in range(2))
    ut, dt = ([("relay", kind, step) for step in range(levels)] for kind in range(2))
    return {0: [('rise', 0, 1), ('rise', 0, 2), ('spread', 0, 0)], 1: [('rise', 0, 3), ('relay', 0, 0), ('spread', 1, 0), ('spread', 0, 1)], 3: [('relay', 1, 0), ('rise', 1, 1), ('rise', 1, 2), ('rise', 1, 3), ('spread', 0, 2), ('spread', 0, 3)], 4: [('relay', 0, 1), ('relay', 0, 2), ('relay', 0, 3)], 13: [('spread level', 1, 0), ('spread level', 1, 1), ('spread level', 1, 2), ('spread level', 1, 3)], 50: [('relay level', 1, 0)], 51: [('relay level', 1, 1)], 52: [('relay level', 1, 2)], 53: [('relay level', 1, 3)]}


def per_device_fused(team, *operands):
    (
        skip_stream_entering,
        content_signal_matrix,
        writer_signal_matrix,
        reader_signal_matrix,
        multiplier_signal,
        interval_before_softplus,
        extra_log_shrink,
        log_forget_speed,
        content_filter_coefs,
        writer_filter_coefs,
        reader_filter_coefs,
        skip_path_factor,
        cluster_scaling_vector,
        blend_result_matrix,
        feature_blend_scaling,
        widening_matrix,
        narrowing_matrix,
    ) = operands
    f32, bf16 = jnp.float32, jnp.bfloat16
    shards = lax.axis_size("sp")
    length, inner = content_signal_matrix.shape
    state_width = writer_signal_matrix.shape[1]
    local_heads = interval_before_softplus.shape[0]
    rows_own, model = skip_stream_entering.shape
    levels = shards // 4
    unit = widening_matrix.shape[1] // levels
    depth = widening_matrix.shape[0]
    lanes = narrowing_matrix.shape[1]
    slice_width = inner // team
    pairs = shards // 2
    dma = pltpu.SemaphoreType.DMA
    vmem, anywhere = pl.BlockSpec(memory_space=pltpu.VMEM), pl.BlockSpec(memory_space=pl.ANY)
    specs = [anywhere] * 5 + [vmem] * 8 + [anywhere, vmem, anywhere, anywhere]
    scratch = [
        pltpu.VMEM((rows_own, model), bf16),
        pltpu.VMEM((length, inner), bf16),
        pltpu.VMEM((length, state_width), bf16),
        pltpu.VMEM((length, state_width), bf16),
        pltpu.VMEM((length, inner), bf16),
        pltpu.VMEM((16, inner + 2 * state_width), bf16),
        pltpu.VMEM((8 + length, inner + 2 * state_width), f32),
        pltpu.VMEM((length, inner), f32),
        pltpu.VMEM((length, 2 * state_width), bf16),
        pltpu.VMEM(blend_result_matrix.shape, bf16),
        pltpu.VMEM((shards, depth, unit), bf16),
        pltpu.VMEM((shards, unit, lanes), bf16),
        pltpu.VMEM((length, local_heads * length), f32),
        pltpu.VMEM((local_heads, length), f32),
        pltpu.VMEM((length, inner), f32),
        pltpu.VMEM((length, inner), f32),
        pltpu.VMEM((team, STATE + 16, slice_width), bf16),
        pltpu.VMEM((team, STATE + 16, slice_width), bf16),
        pltpu.VMEM((team, STATE, slice_width), f32),
        pltpu.VMEM((team, 8, slice_width), f32),
        pltpu.VMEM((STATE, slice_width), bf16),
        pltpu.VMEM((STATE, slice_width), bf16),
        pltpu.VMEM((team, STATE, slice_width), bf16),
        pltpu.VMEM((team, STATE, slice_width), bf16),
        pltpu.VMEM((length, inner), bf16),
        pltpu.VMEM((2, rows_own, model), bf16),
        pltpu.VMEM((rows_own, model), bf16),
        pltpu.VMEM((2, levels, rows_own, model), bf16),
        pltpu.VMEM((2, levels * rows_own, unit), bf16),
        pltpu.VMEM((pairs, levels * rows_own, 2 * lanes), bf16),
        pltpu.VMEM((pairs, levels * rows_own, 2 * lanes), bf16),
        pltpu.VMEM((pairs, levels, rows_own, 2 * lanes), bf16),
        pltpu.VMEM((pairs, levels, rows_own, 2 * lanes), bf16),
        dma((8,)),
        dma((3,)),
        dma((3,)),
        dma((3 * levels,)),
        dma((shards,)),
        dma((3 * levels,)),
        dma((shards,)),
        dma((4 * levels,)),
        dma((4 * levels,)),
        dma((team,)),
        dma((team,)),
        dma,
        dma,
        dma((team,)),
        dma((team,)),
        dma,
        dma,
        dma((4 * levels,)),
        dma((2 * levels,)),
        dma((2 * levels,)),
        dma((2 * levels,)),
        dma((pairs,)),
        dma((pairs,)),
        dma((pairs, levels)),
        dma((pairs, levels)),
    ]
    state, mixed = pl.pallas_call(
        functools.partial(layer_kernel, team),
        out_shape=[jax.ShapeDtypeStruct((rows_own, model), bf16)] * 2,
        in_specs=specs,
        out_specs=[vmem, vmem],
        scratch_shapes=scratch,
        compiler_params=pltpu.CompilerParams(
            collective_id=0, has_side_effects=True, vmem_limit_bytes=63 * 1024 * 1024
        ),
    )(
        skip_stream_entering,
        content_signal_matrix,
        writer_signal_matrix,
        reader_signal_matrix,
        multiplier_signal,
        interval_before_softplus,
        extra_log_shrink,
        log_forget_speed.reshape(1, -1),
        content_filter_coefs,
        writer_filter_coefs,
        reader_filter_coefs,
        skip_path_factor.reshape(1, -1),
        cluster_scaling_vector.reshape(1, -1),
        blend_result_matrix,
        feature_blend_scaling.reshape(1, -1),
        widening_matrix,
        narrowing_matrix,
    )
    return (state.astype(f32) + mixed.astype(f32)).astype(bf16)


def general_solution(mesh):
    shards, halves = mesh.shape["sp"], mesh.shape["tp"]
    team = math.gcd(shards, TEAM)
    teams = jax.sharding.Mesh(
        mesh.devices.reshape(shards // team, team, halves), ("sa", "sb", "tp")
    )
    placed = (
        P(("sa", "sb", "tp"), None),
        P(SP, "tp"),
        P(SP, "tp"),
        P(SP, "tp"),
        P(SP, "tp"),
        P("tp", SP),
        P("tp", SP),
        P("tp"),
        P(None, "tp"),
        P(None, "tp"),
        P(None, "tp"),
        P("tp"),
        P("tp"),
        P("tp", None),
        P(),
        P(SP, "tp"),
        P("tp", SP),
    )
    return jax.shard_map(
        per_device, mesh=teams, in_specs=placed, out_specs=P(("sa", "sb", "tp"), None), check_vma=False
    )


def fits(shards, halves, team, rows, tokens, inner, hidden, model, state_width):
    length = tokens // shards
    local = inner // halves
    return (
        halves == 2
        and shards == 2 * team
        and team % 4 == 0
        and length == BLOCK
        and length % 32 == 0
        and local % (team * 128) == 0
        and shards % 4 == 0
        and (hidden // halves) % (shards // 4 * 128) == 0
        and (shards // 4) == 4
        and model % (shards * 128) == 0
        and (state_width // halves) % STATE == 0
        and (local // (state_width // halves // STATE)) % (local // team) == 0
    )


def solution(mesh):
    shards, halves = mesh.shape["sp"], mesh.shape["tp"]
    team = math.gcd(shards, TEAM)
    general = general_solution(mesh)
    row, both = P("sp", "tp"), P(("sp", "tp"), None)
    tp_first, tp_last, tp_only = P("tp", "sp"), P(None, "tp"), P("tp")
    placed = (
        (both, row, row, row, row, tp_first, tp_first, tp_only, tp_last, tp_last, tp_last)
        + (tp_only, tp_only, P("tp", None), P(), row, tp_first)
    )
    fused = jax.shard_map(
        functools.partial(per_device_fused, team),
        mesh=mesh,
        in_specs=placed,
        out_specs=both,
        check_vma=False,
    )

    def layer(*operands):
        tokens, inner = operands[1].shape
        model, hidden = operands[15].shape
        state_width = operands[2].shape[1]
        if fits(shards, halves, team, tokens, tokens, inner, hidden, model, state_width):
            return fused(*operands)
        return general(*operands)

    return layer
```

```python
import functools
import math
import jax
import jax.numpy as jnp
from jax import lax
from jax.experimental import pallas as pl
from jax.experimental.pallas import tpu as pltpu
from jax.sharding import PartitionSpec as P

HEAD_DIM = 64
STATE = 128
BLOCK = 128


epsilon = 1e-05
precise = lax.Precision.HIGHEST
SP = ("sa", "sb")
TEAM = 8


def shifted(value, axis, steps):
    count = lax.axis_size(axis)
    initial, last = (max(0, -steps), min(count, count - steps))
    return lax.ppermute(value, axis, [(source, source + steps) for source in range(initial, last)])


def scan_rows(parts, factors, entering):
    def one(place, carried):
        entering[place] = carried.astype(jnp.bfloat16)
        return carried * factors[place] + parts[place].astype(jnp.float32)

    lax.fori_loop(0, parts.shape[0], one, jnp.zeros(parts.shape[1:], jnp.float32))


def prefix(log_total, end_state, rider):
    shards = lax.axis_size(SP)
    heads = end_state.shape[0] * end_state.shape[1]
    state_width = end_state.shape[-1]
    rows = end_state.reshape(-1, state_width).astype(jnp.bfloat16)
    count = rows.shape[0] // shards
    decays = jnp.repeat(jnp.exp(log_total).reshape(heads), rows.shape[0] // heads)
    extra = -(-count // state_width) * 16
    decays = decays.astype(jnp.bfloat16).reshape(shards, count)
    decays = jnp.pad(decays, ((0, 0), (0, extra * state_width - count)))
    packed = jnp.concatenate(
        [rows.reshape(shards, count, state_width), decays.reshape(shards, extra, state_width)],
        axis=1,
    )
    packed = lax.all_to_all(packed, SP, split_axis=0, concat_axis=0)
    parts = packed[:, :count]
    factors = packed[:, count:].reshape(shards, -1)[:, :count].astype(jnp.float32)
    entering = pl.pallas_call(
        scan_rows,
        out_shape=jax.ShapeDtypeStruct(parts.shape, jnp.bfloat16),
    )(parts, jnp.broadcast_to(factors[..., None], parts.shape))
    entering, rider = lax.optimization_barrier((entering, rider))
    back = lax.all_to_all(
        entering.reshape(rows.shape), SP, split_axis=0, concat_axis=0, tiled=True
    )
    return back.reshape(end_state.shape).astype(jnp.float32), rider


def summed_share(partial, axis):
    count = lax.axis_size(axis)
    if count != 2:
        return lax.psum_scatter(partial, axis, scatter_dimension=0, tiled=True)
    me = lax.axis_index(axis)
    length = partial.shape[0] // 2
    away = lax.dynamic_slice_in_dim(partial, (1 - me) * length, length, 0)
    kept = lax.dynamic_slice_in_dim(partial, me * length, length, 0)
    arrived = lax.ppermute(away, axis, [(0, 1), (1, 0)])
    return (kept.astype(jnp.float32) + arrived.astype(jnp.float32)).astype(jnp.bfloat16)


def convolve(inputs, rim_rows, conv_taps):
    width = conv_taps.shape[0]
    length = inputs.shape[0]
    extended = jnp.concatenate([rim_rows, inputs], axis=0)
    summed = extended[0:length].astype(jnp.float32) * conv_taps[0].astype(jnp.float32)
    for offset in range(1, width):
        summed = summed + extended[offset : offset + length].astype(jnp.float32) * conv_taps[
            offset
        ].astype(jnp.float32)
    return jax.nn.silu(summed)


def advance(carried, pair):
    block_state, block_factor = pair
    return (carried * block_factor[..., None, None] + block_state, carried)


def blockwise(values, interval_lengths, log_forgetting, key_rows, query_rows):
    length, groups, per_group, width = values.shape
    blocks = length // BLOCK
    value_blocks = values.reshape(blocks, BLOCK, groups, per_group, width)
    step_blocks = jnp.transpose(
        interval_lengths.reshape(groups, per_group, blocks, BLOCK), (2, 3, 0, 1)
    )
    weighted = value_blocks * step_blocks[..., None]
    cumulative = jnp.cumsum(
        jnp.transpose(log_forgetting.reshape(groups, per_group, blocks, BLOCK), (2, 0, 1, 3)),
        axis=-1,
    )
    key_blocks = key_rows.reshape(blocks, BLOCK, groups, -1)
    query_blocks = query_rows.reshape(blocks, BLOCK, groups, -1)
    causal = jnp.tril(jnp.ones((BLOCK, BLOCK), dtype=bool))
    decay_mask = jnp.exp(
        jnp.where(causal, cumulative[..., :, None] - cumulative[..., None, :], -jnp.inf)
    )
    scores = jnp.einsum("clgn,csgn->cgls", query_blocks, key_blocks, precision=precise)
    within = jnp.einsum("cgls,cgrls,csgrp->clgrp", scores, decay_mask, weighted, precision=precise)
    to_end = jnp.exp(cumulative[..., -1:] - cumulative)
    states = jnp.einsum("clgn,cgrl,clgrp->cgrpn", key_blocks, to_end, weighted, precision=precise)
    block_totals = cumulative[..., -1]
    initial = jnp.zeros(states.shape[1:], jnp.float32)
    final, entering = lax.scan(advance, initial, (states, jnp.exp(block_totals)))
    carried = jnp.einsum(
        "clgn,cgrpn,cgrl->clgrp", query_blocks, entering, jnp.exp(cumulative), precision=precise
    )
    from_start = (jnp.cumsum(block_totals, axis=0) - block_totals)[..., None] + cumulative
    return (within + carried, final, from_start, jnp.sum(block_totals, axis=0))


def normalize(rows, gain):
    widened = rows.astype(jnp.float32)
    scaled = widened * lax.rsqrt(jnp.mean(widened * widened, axis=-1, keepdims=True) + epsilon)
    return (scaled * gain).astype(jnp.bfloat16)


def per_device(
    skip_stream_entering,
    content_signal_matrix,
    writer_signal_matrix,
    reader_signal_matrix,
    multiplier_signal,
    interval_before_softplus,
    extra_log_shrink,
    log_forget_speed,
    content_filter_coefs,
    writer_filter_coefs,
    reader_filter_coefs,
    skip_path_factor,
    cluster_scaling_vector,
    blend_result_matrix,
    feature_blend_scaling,
    widening_matrix,
    narrowing_matrix,
):
    up_part = lax.all_to_all(widening_matrix, "sb", split_axis=1, concat_axis=0, tiled=True)
    narrowing_matrix, up_part = lax.optimization_barrier((narrowing_matrix, up_part))
    up_use = lax.all_gather(up_part, "sa", axis=0, tiled=True)
    down_part = lax.all_to_all(narrowing_matrix, "sb", split_axis=0, concat_axis=1, tiled=True)
    (
        content_signal_matrix,
        writer_signal_matrix,
        reader_signal_matrix,
        interval_before_softplus,
        down_part,
    ) = lax.optimization_barrier(
        (
            content_signal_matrix,
            writer_signal_matrix,
            reader_signal_matrix,
            interval_before_softplus,
            down_part,
        )
    )
    down_use = lax.all_gather(down_part, "sa")
    rim_width = content_filter_coefs.shape[0] - 1
    length = content_signal_matrix.shape[0]
    signals = (content_signal_matrix, writer_signal_matrix, reader_signal_matrix)
    tails = jnp.concatenate([signal[length - rim_width :] for signal in signals], axis=1)
    rims = shifted(tails, SP, 1)
    first, second = signals[0].shape[1], signals[0].shape[1] + signals[1].shape[1]
    values = convolve(signals[0], rims[:, :first], content_filter_coefs)
    key_rows = convolve(signals[1], rims[:, first:second], writer_filter_coefs)
    query_rows = convolve(signals[2], rims[:, second:], reader_filter_coefs)
    local_heads = interval_before_softplus.shape[0]
    local_groups = writer_signal_matrix.shape[1] // STATE
    per_group = local_heads // local_groups
    interval_lengths = jax.nn.softplus(interval_before_softplus)
    log_forgetting = extra_log_shrink - jnp.exp(log_forget_speed)[:, None] * interval_lengths
    shaped = values.reshape(length, local_groups, per_group, HEAD_DIM)
    local_out, end_state, from_start, device_total = blockwise(
        shaped,
        interval_lengths.reshape(local_groups, per_group, length),
        log_forgetting.reshape(local_groups, per_group, length),
        key_rows,
        query_rows,
    )
    incoming, up_use = prefix(device_total, end_state, up_use)
    query_blocks = query_rows.reshape(length // BLOCK, BLOCK, local_groups, STATE)
    arriving = jnp.einsum(
        "clgn,grpn,cgrl->clgrp", query_blocks, incoming, jnp.exp(from_start), precision=precise
    )
    scan_out = (local_out + arriving).reshape(length, local_heads * HEAD_DIM)
    gated = (scan_out + jnp.repeat(skip_path_factor, HEAD_DIM) * values) * jax.nn.silu(
        multiplier_signal.astype(jnp.float32)
    )
    grouped = gated.reshape(length, local_groups, -1)
    grouped = grouped * lax.rsqrt(jnp.mean(grouped * grouped, axis=-1, keepdims=True) + epsilon)
    heads_out = (grouped.reshape(length, -1) * cluster_scaling_vector).astype(jnp.bfloat16)
    mixer_rows = summed_share(
        jnp.dot(heads_out, blend_result_matrix, preferred_element_type=jnp.float32).astype(
            jnp.bfloat16
        ),
        "tp",
    )
    own_rows = (skip_stream_entering.astype(jnp.float32) + mixer_rows.astype(jnp.float32)).astype(
        jnp.bfloat16
    )
    normed = normalize(own_rows, feature_blend_scaling)
    down_whole = jnp.concatenate([down_use[k] for k in range(down_use.shape[0])], axis=1)

    def mixed(rows):
        lifted = jax.nn.relu(jnp.dot(rows, up_use, preferred_element_type=jnp.float32))
        hidden = (lifted * lifted).astype(jnp.bfloat16)
        partial = jnp.dot(hidden, down_whole, preferred_element_type=jnp.float32)
        return partial.astype(jnp.bfloat16)

    if lax.axis_size("tp") == 2:
        members, width = lax.axis_size("sb"), normed.shape[1]
        swap = [(0, 1), (1, 0)]
        copies = jnp.broadcast_to(normed[None], (members,) + normed.shape)
        own_half = lax.all_to_all(copies, "sb", split_axis=0, concat_axis=0)
        own_half = own_half.reshape(-1, width)
        other_half = lax.ppermute(own_half, "tp", swap)
        arrived = lax.ppermute(mixed(other_half), "tp", swap)
        joined = mixed(own_half).astype(jnp.float32) + arrived.astype(jnp.float32)
        joined = joined.astype(jnp.bfloat16).reshape(members, -1, width)
        shares = lax.all_to_all(joined, "sb", split_axis=0, concat_axis=0)
        mlp_rows = jnp.sum(shares.astype(jnp.float32), axis=0)
    else:
        team_rows = lax.all_gather(normed, ("sb", "tp"), axis=0, tiled=True)
        mlp_rows = lax.psum_scatter(
            mixed(team_rows), ("sb", "tp"), scatter_dimension=0, tiled=True
        )
    mlp_rows = mlp_rows.astype(jnp.bfloat16)
    return (own_rows.astype(jnp.float32) + mlp_rows.astype(jnp.float32)).astype(jnp.bfloat16)


TEAM_LINKS = pl.DeviceIdType.MESH


def split3(wide):
    one = wide.astype(jnp.bfloat16)
    rest = wide - one.astype(jnp.float32)
    two = rest.astype(jnp.bfloat16)
    return one, two, (rest - two.astype(jnp.float32)).astype(jnp.bfloat16)


def contract(left, right, dims):
    return lax.dot_general(left, right, (dims, ((), ())), preferred_element_type=jnp.float32)


def exact(left, right, dims, left_split):
    if left_split:
        terms = [contract(part, right, dims) for part in split3(left)]
    else:
        terms = [contract(left, part, dims) for part in split3(right)]
    return terms[0] + terms[1] + terms[2]


def selector(rows, columns, per_row):
    row = lax.broadcasted_iota(jnp.int32, (rows, columns), 0)
    column = lax.broadcasted_iota(jnp.int32, (rows, columns), 1)
    return jnp.where(column // per_row == row, 1.0, 0.0).astype(jnp.bfloat16)


def layer_kernel(
    team,
    skip_hbm,
    content_hbm,
    writer_hbm,
    reader_hbm,
    multiplier_hbm,
    interval_ref,
    shrink_ref,
    speed_ref,
    content_taps,
    writer_taps,
    reader_taps,
    skip_factor,
    cluster_gain,
    blend_hbm,
    feature_gain,
    up_hbm,
    down_hbm,
    mixed_ref,
    out_ref,
    skip_ref,
    content_ref,
    writer_ref,
    reader_ref,
    multiplier_ref,
    halo,
    wide,
    values,
    keyquery,
    blend,
    up,
    down,
    column_decay,
    row_decay,
    scan,
    scale_in,
    state_out,
    state_in,
    entering,
    kept_decay,
    cross_out,
    cross_in,
    back_out,
    back_in,
    heads,
    part_out,
    part_in,
    acts,
    hidden,
    pair_out,
    pair_in,
    plane_out,
    depth_in,
    local_sem,
    halo_ss,
    halo_rs,
    up_ss,
    up_rs,
    down_ss,
    down_rs,
    half_ss,
    half_rs,
    st_ss,
    st_rs,
    cr_ss,
    cr_rs,
    bk_ss,
    bk_rs,
    pt_ss,
    pt_rs,
    ap_ss,
    ap_rs,
    ad_ss,
    ad_rs,
    pr_ss,
    pr_rs,
    dp_ss,
    dp_rs,
):
    f32, bf16 = jnp.float32, jnp.bfloat16
    batches = plan(lax.axis_size("sp") // 4)
    shards = lax.axis_size("sp")
    sp, tp = lax.axis_index("sp"), lax.axis_index("tp")
    own_team, me = sp // team, lax.rem(sp, team)
    length, inner = content_ref.shape
    state_width = writer_ref.shape[1]
    local_heads = interval_ref.shape[0]
    groups = state_width // STATE
    group_width = inner // groups
    model = skip_ref.shape[1]
    unit = up.shape[2]
    slice_width = inner // team
    half = team // 2
    rows_own = skip_ref.shape[0]

    open_scope = []

    def phase(name):
        if open_scope:
            open_scope.pop().__exit__(None, None, None)
        if name:
            open_scope.append(jax.named_scope(name))
            open_scope[-1].__enter__()

    def copy(src, dst, ss, rs, sp_to, tp_to):
        return pltpu.make_async_remote_copy(
            src_ref=src,
            dst_ref=dst,
            send_sem=ss,
            recv_sem=rs,
            device_id=(sp_to, tp_to),
            device_id_type=TEAM_LINKS,
        )

    def mate(step):
        return own_team * team + lax.rem(me + step, team)

    level, spot = sp // 4, lax.rem(sp, 4)
    beside = (spot + 1 - 2 * lax.rem(spot, 2), lax.rem(spot + 2, 4))
    levels = shards // 4

    def level_at(step):
        return lax.rem(level + levels + step, levels)

    def weight_piece(kind, index):
        offset = pl.ds(pl.multiple_of(index * unit, unit), unit)
        return up_hbm.at[:, offset] if kind == 0 else down_hbm.at[offset, :]

    def weight_copy(kind, src, source, place, target):
        into, ss, rs = ((up, up_ss, up_rs), (down, down_ss, down_rs))[kind]
        if src is None:
            src = into.at[source]
        return copy(src, into.at[source], ss.at[place], rs.at[source], target, tp)

    def source_level(step, kind):
        if kind == 0 or step == 0:
            return level_at(-step)
        return step - 1 + jnp.where(level <= step - 1, 1, 0)

    def rise(kind, step):
        to = level_at(step)
        return weight_copy(kind, weight_piece(kind, to), sp, step, to * 4 + spot)

    def spread(kind, step, way):
        source = source_level(step, kind) * 4 + spot
        piece = weight_piece(kind, level) if step == 0 else None
        place = levels * (1 + way) + step
        return weight_copy(kind, piece, source, place, level * 4 + beside[way])

    def relay(kind, step, way):
        at_level = source_level(step, kind)
        return diagonal(kind, at_level, at_level * 4 + beside[way], way, step)

    def diagonal(kind, at_level, source, way, step):
        part = pl.ds(way * (unit // 2), unit // 2)
        held = up.at[source, :, part] if kind == 0 else down.at[source, part, :]
        place = kind * 2 * levels + way * levels
        target = level * 4 + beside[1 - way]
        return copy(held, held, half_ss.at[place + step], half_rs.at[place + at_level], target, tp)

    def neighbour(kind, step, way):
        return weight_copy(kind, None, source_level(step, kind) * 4 + beside[way], 0, sp)

    def issue(batch):
        for what, kind, step in batches.get(batch, ()):
            if what == "rise":
                rise(kind, step).start()
            if what == "spread":
                if step:
                    spread(kind, step, 0).wait_recv()
                for way in range(2):
                    spread(kind, step, way).start()
            if what == "spread level":

                @pl.when(level != step)
                def _():
                    source = step * 4 + spot
                    slot = levels + step + jnp.where(level > step, 1, 0)
                    for way in range(2):
                        target = level * 4 + beside[way]
                        passing = weight_copy(kind, None, source, slot + way * levels, target)
                        if way == 0:
                            passing.wait_recv()
                        passing.start()

            if what == "relay level":

                @pl.when(level != step)
                def _():
                    slot = step + jnp.where(level > step, 1, 0)
                    for way in range(2):
                        source = step * 4 + beside[way]
                        weight_copy(kind, None, source, 0, sp).wait_recv()
                        diagonal(kind, step, source, way, slot).start()

            if what == "relay":
                for way in range(2):
                    neighbour(kind, step, way).wait_recv()
                    relay(kind, step, way).start()

    local_up = pltpu.make_async_copy(weight_piece(0, level), up.at[sp], local_sem.at[0])
    local_down = pltpu.make_async_copy(weight_piece(1, level), down.at[sp], local_sem.at[1])
    local_blend = pltpu.make_async_copy(blend_hbm, blend, local_sem.at[2])
    brought = []
    for place, (source, into) in enumerate(
        (
            (content_hbm, content_ref),
            (writer_hbm, writer_ref),
            (reader_hbm, reader_ref),
            (multiplier_hbm, multiplier_ref),
            (skip_hbm, skip_ref),
        )
    ):
        brought.append(pltpu.make_async_copy(source, into, local_sem.at[3 + place]))
        brought[-1].start()
    local_up.start()
    local_down.start()
    local_blend.start()

    barrier = pltpu.get_barrier_semaphore()
    for step in range(1, shards):
        pl.semaphore_signal(
            barrier,
            inc=1,
            device_id=(lax.rem(sp + step, shards), tp),
            device_id_type=TEAM_LINKS,
        )
    pl.semaphore_signal(barrier, inc=1, device_id=(sp, 1 - tp), device_id_type=TEAM_LINKS)

    phase("decays")
    steps = interval_ref[...]
    steps = jnp.maximum(steps, 0.0) + jnp.log1p(jnp.exp(-jnp.abs(steps)))
    head_row = lax.broadcasted_iota(jnp.int32, (local_heads, local_heads), 0)
    head_column = lax.broadcasted_iota(jnp.int32, (local_heads, local_heads), 1)
    speed = jnp.where(head_row == head_column, speed_ref[...], 0.0)
    forget = shrink_ref[...] - jnp.exp(jnp.sum(speed, axis=1, keepdims=True)) * steps
    row_index = lax.broadcasted_iota(jnp.int32, (length, length), 0)
    column_index = lax.broadcasted_iota(jnp.int32, (length, length), 1)
    lower = jnp.where(row_index >= column_index, 1.0, 0.0).astype(bf16)
    upper = jnp.where(row_index <= column_index, 1.0, 0.0).astype(bf16)
    unity = jnp.where(row_index == column_index, 1.0, 0.0).astype(bf16)
    log_steps = jnp.log(steps)
    total_rows = exact(forget, upper, ((1,), (0,)), True)
    total_columns = exact(lower, forget, ((1,), (1,)), False)
    log_columns = exact(unity, log_steps, ((1,), (1,)), False)
    row_decay[...] = total_rows - log_steps
    by_head = selector(local_heads, local_heads * length, length)
    column_decay[...] = exact(total_columns, by_head, ((1,), (0,)), True)
    by_channel = selector(local_heads, inner, HEAD_DIM)
    scale_in[...] = exact(jnp.exp(total_columns), by_channel, ((1,), (0,)), True)
    last = total_columns[length - 1 : length, :]
    to_end = jnp.exp(last - total_columns + log_columns)
    end_scale = exact(to_end, by_channel, ((1,), (0,)), True)
    whole_decay = exact(
        jnp.broadcast_to(jnp.exp(last), (16, local_heads)), by_channel, ((1,), (0,)), True
    )
    skip_scale = exact(
        jnp.broadcast_to(skip_factor[...], (16, local_heads)), by_channel, ((1,), (0,)), True
    )

    for one in brought[:3]:
        one.wait()
    phase("barrier_wait")
    pl.semaphore_wait(barrier, shards)
    phase("first_sends")
    following = lax.rem(sp + 1, shards)
    spans = ((content_ref, 0, inner), (writer_ref, inner, state_width))
    spans = spans + ((reader_ref, inner + state_width, state_width),)
    halo_copies = []
    for place, (ref, first, size) in enumerate(spans):
        halo_copies.append(
            copy(
                ref.at[pl.ds(length - 16, 16), :],
                halo.at[:, pl.ds(first, size)],
                halo_ss.at[place],
                halo_rs.at[place],
                following,
                tp,
            )
        )

    @pl.when(sp < shards - 1)
    def _():
        for one in halo_copies:
            one.start()

    issue(0)

    phase("rim_wait")
    @pl.when(sp > 0)
    def _():
        for one in halo_copies:
            one.wait_recv()

    @pl.when(sp == 0)
    def _():
        halo[...] = jnp.zeros_like(halo)

    phase("convolve")
    chunk = state_width
    for ref, taps, first, size in (
        (content_ref, content_taps, 0, inner),
        (writer_ref, writer_taps, inner, state_width),
        (reader_ref, reader_taps, inner + state_width, state_width),
    ):
        for start in range(0, size, chunk):
            at = slice(start, start + chunk)
            placed = slice(first + start, first + start + chunk)
            wide[8:, placed] = ref[:, at].astype(f32)
            wide[0:8, placed] = halo[:, placed].astype(f32)[8:, :]
            weights = taps[:, at].astype(f32)
            count = taps.shape[0]
            base = 8 - (count - 1)
            total = wide[base : base + length, placed] * weights[0:1, :]
            for k in range(1, count):
                total = total + wide[base + k : base + k + length, placed] * weights[k : k + 1, :]
            total = total * (1.0 / (1.0 + jnp.exp(-total)))
            if first == 0:
                values[:, at] = total
            else:
                keyquery[:, first - inner + start : first - inner + start + chunk] = total.astype(bf16)

    phase("states")
    weighted = (values[...] * end_scale).astype(bf16)
    for g in range(groups):
        keys = keyquery[:, g * STATE : (g + 1) * STATE]
        made = contract(keys, weighted[:, g * group_width : (g + 1) * group_width], ((0,), (0,)))
        for part in range(group_width // slice_width):
            place = g * (group_width // slice_width) + part
            state_out[place, 0:STATE, :] = made[
                :, part * slice_width : (part + 1) * slice_width
            ].astype(bf16)
    high = whole_decay.astype(bf16)
    low = (whole_decay - high.astype(f32)).astype(bf16)
    first_row = lax.broadcasted_iota(jnp.int32, whole_decay.shape, 0) == 0
    packed = jnp.where(first_row, high.astype(f32), low.astype(f32)).astype(bf16)
    for place in range(team):
        state_out[place, STATE : STATE + 16, :] = packed[
            :, place * slice_width : (place + 1) * slice_width
        ]
    state_in[me] = state_out[me]
    state_copies = []
    for step in range(1, team):
        target = mate(step)
        state_copies.append(
            copy(
                state_out.at[lax.rem(target, team)],
                state_in.at[me],
                st_ss.at[step],
                st_rs.at[me],
                target,
                tp,
            )
        )
        state_copies[-1].start()
    issue(1)

    phase("within")
    causal = row_index >= column_index
    causal_pair = jnp.concatenate([causal, causal], axis=1)
    lane = lax.broadcasted_iota(jnp.int32, (length, 2 * HEAD_DIM), 1)
    pairs_per_group = group_width // (2 * HEAD_DIM)
    for g in range(groups):
        keys = keyquery[:, g * STATE : (g + 1) * STATE]
        queries = keyquery[:, state_width + g * STATE : state_width + (g + 1) * STATE]
        scores = contract(queries, keys, ((1,), (1,)))
        scores = jnp.concatenate([scores, scores], axis=1)
        for j in range(pairs_per_group):
            i = g * pairs_per_group + j
            rows = jnp.concatenate(
                [row_decay[2 * i : 2 * i + 1, :], row_decay[2 * i + 1 : 2 * i + 2, :]], axis=1
            )
            gap = column_decay[:, 2 * i * length : (2 * i + 2) * length] - rows
            decay = jnp.exp(jnp.where(causal_pair, gap, -jnp.inf))
            mixing = (scores * decay).astype(bf16)
            both = values[:, i * 2 * HEAD_DIM : (i + 1) * 2 * HEAD_DIM]
            blocks = jnp.concatenate(
                [jnp.where(lane < HEAD_DIM, both, 0.0), jnp.where(lane < HEAD_DIM, 0.0, both)],
                axis=0,
            ).astype(bf16)
            scan[:, i * 2 * HEAD_DIM : (i + 1) * 2 * HEAD_DIM] = contract(
                mixing, blocks, ((1,), (0,))
            )
    scan[...] = scan[...] + skip_scale[0:1, :] * values[...]

    phase("state_wait")
    carried = jnp.zeros((STATE, slice_width), f32)
    kept = jnp.ones((1, slice_width), f32)
    for step in range(1, team):
        source = lax.rem(me + step, team)
        copy(
            state_in.at[source], state_in.at[source], st_ss.at[step], st_rs.at[source], sp, tp
        ).wait_recv()
    phase("prefix")
    for place in range(team):
        entering[place] = carried
        kept_decay[place] = jnp.broadcast_to(kept, (8, slice_width))
        tail = state_in[place, STATE : STATE + 16, :].astype(f32)
        factor = tail[0:1, :] + tail[1:2, :]
        carried = carried * factor + state_in[place, 0:STATE, :].astype(f32)
        kept = kept * factor
    cross_out[...] = carried.astype(bf16)
    cross = copy(cross_out, cross_in, cr_ss, cr_rs, team + me, tp)

    @pl.when(own_team == 0)
    def _():
        cross.start()

    issue(2)
    phase("cross_wait")
    @pl.when(own_team > 0)
    def _():
        cross.wait_recv()

    phase("back")

    @pl.when(own_team == 0)
    def _():
        back_out[...] = entering[...].astype(bf16)

    @pl.when(own_team > 0)
    def _():
        earlier = cross_in[...].astype(f32)
        for place in range(team):
            back_out[place] = (entering[place] + kept_decay[place, 0:1, :] * earlier).astype(bf16)

    back_in[me] = back_out[me]
    back_copies = []
    for step in range(1, team):
        target = mate(step)
        back_copies.append(
            copy(
                back_out.at[lax.rem(target, team)],
                back_in.at[me],
                bk_ss.at[step],
                bk_rs.at[me],
                target,
                tp,
            )
        )
        back_copies[-1].start()
    issue(3)
    phase("back_wait")
    for step in range(1, team):
        source = lax.rem(me + step, team)
        copy(
            back_in.at[source], back_in.at[source], bk_ss.at[step], bk_rs.at[source], sp, tp
        ).wait_recv()

    phase("gate")
    brought[3].wait()
    for g in range(groups):
        queries = keyquery[:, state_width + g * STATE : state_width + (g + 1) * STATE]
        at = slice(g * group_width, (g + 1) * group_width)
        per = group_width // slice_width
        incoming = jnp.concatenate([back_in[g * per + part] for part in range(per)], axis=1)
        arriving = contract(queries, incoming, ((1,), (0,))) * scale_in[:, at]
        gate = multiplier_ref[:, at].astype(f32)
        gated = (scan[:, at] + arriving) * (gate * (1.0 / (1.0 + jnp.exp(-gate))))
        gated = gated * lax.rsqrt(jnp.mean(gated * gated, axis=1, keepdims=True) + epsilon)
        heads[:, at] = (gated * cluster_gain[:, at]).astype(bf16)

    phase("project")
    local_blend.wait()
    column_chunk = 512

    def project(index, carry):
        at = pl.ds(pl.multiple_of(index * column_chunk, column_chunk), column_chunk)
        product = contract(heads[...], blend[:, at], ((1,), (0,))).astype(bf16)
        part_out[0, :, at] = product[0:rows_own, :]
        part_out[1, :, at] = product[rows_own:, :]
        return carry

    lax.fori_loop(0, model // column_chunk, project, 0)
    swap = copy(part_out.at[1 - tp], part_in, pt_ss, pt_rs, sp, 1 - tp)
    swap.start()
    phase("swap_wait")
    swap.wait_recv()
    phase("norm")
    brought[4].wait()
    mixed = (part_out[tp].astype(f32) + part_in[...].astype(f32)).astype(bf16)
    state = (skip_ref[...].astype(f32) + mixed.astype(f32)).astype(bf16)
    mixed_ref[...] = state
    state = state.astype(f32)
    state = state * lax.rsqrt(jnp.mean(state * state, axis=1, keepdims=True) + epsilon)
    acts[tp, level] = (state * feature_gain[...]).astype(bf16)

    phase("gather")
    parts = 2

    def rows_to(place, part, ss, rs, target, core):
        rows = pl.ds(part * (rows_own // parts), rows_own // parts)
        held = acts.at[tp, place, rows]
        return copy(held, held, ss, rs.at[place * parts + part], target, core)

    top = levels - 1

    def along(place, part, hop, up_way):
        to = level_at(1 if up_way else -1) * 4 + spot
        order = (hop + (0 if up_way else levels)) * parts + part
        return rows_to(place, part, ap_ss.at[order], ap_rs, to, tp)

    def share(place, part):
        return rows_to(place, part, ad_ss.at[place * parts + part], ad_rs, sp, 1 - tp)

    def up_ready():
        local_up.wait()
        for step in range(levels):
            for way in range(2):
                diagonal(0, step, step * 4 + 3 - spot, way, 0).wait_recv()

    def lift(block):
        count = levels // 2
        for place in range(count):
            for part in range(parts):
                share(block * count + place, part).wait_recv()
        up_whole = (shards * up.shape[1], unit)
        at = pl.ds(pl.multiple_of(block * count * rows_own, count * rows_own), count * rows_own)

        def one(core, carry):
            rows = acts[core, pl.ds(block * count, count)].reshape(count * rows_own, model)
            lifted = jnp.maximum(contract(rows, up[...].reshape(up_whole), ((1,), (0,))), 0.0)
            hidden[core, at, :] = (lifted * lifted).astype(bf16)
            return carry

        lax.fori_loop(0, 2, one, 0)

    def send_along(hop, part):
        @pl.when((level >= hop) & (level < top))
        def _():
            along(level_at(-hop), part, hop, True).start()

        @pl.when((level + hop <= top) & (level > 0))
        def _():
            along(level_at(hop), part, hop, False).start()

    for part in range(parts):
        send_along(0, part)
        share(level, part).start()
    issue(4)
    phase("line_wait")
    for hop in range(1, levels):
        for part in range(parts):
            for up_way in (True, False):
                place = level_at(-hop if up_way else hop)

                @pl.when(level >= hop if up_way else level + hop <= top)
                def _():
                    along(place, part, hop, up_way).wait_recv()
                    if hop < top:

                        @pl.when(level < top if up_way else level > 0)
                        def _():
                            along(place, part, hop, up_way).start()

                    share(place, part).start()

        issue(3 + 10 * hop)
        if hop == levels - 2:
            up_ready()
            lift(level // 2)
    issue(5)
    phase("lift")
    lift(1 - level // 2)
    issue(7)

    phase("lower")
    local_down.wait()
    lanes = down.shape[2]

    def pair_sources(t):
        row = lax.rem(t // levels + spot // 2, 2)
        first = lax.rem(t, levels) * 4 + row * 2
        return first, first + 1

    def pair_copy(t):
        return copy(pair_out.at[t], pair_in.at[t], pr_ss.at[t], pr_rs.at[t], sp, 1 - tp)

    def depth_copy(t, k):
        to = level_at(k)
        return copy(
            plane_out.at[t, to],
            depth_in.at[t, k],
            dp_ss.at[t, k],
            dp_rs.at[t, k],
            to * 4 + spot,
            tp,
        )

    def lower_step(t):
        sources = pair_sources(t)

        @pl.when(t >= levels)
        def _():
            for way in range(2):
                at_level = lax.rem(t, levels)
                diagonal(1, at_level, at_level * 4 + 3 - spot, way, 0).wait_recv()

        both = jnp.concatenate([down[sources[0]], down[sources[1]]], axis=1)
        pair_out[t] = contract(hidden[1 - tp], both, ((1,), (0,))).astype(bf16)
        pair_copy(t).start()
        plane_sum = contract(hidden[tp], both, ((1,), (0,)))
        plane_out[t] = plane_sum.astype(bf16).reshape(levels, rows_own, 2 * lanes)

    def pair_step(t):
        pair_copy(t).wait_recv()
        summed = plane_out[t].astype(f32) + pair_in[t].reshape(
            levels, rows_own, 2 * lanes
        ).astype(f32)
        plane_out[t] = summed.astype(bf16)
        for k in range(1, levels):
            depth_copy(t, jnp.where(level < levels // 2, levels - k, k)).start()

    def depth_step(t):
        summed = plane_out[t, level].astype(f32)
        for k in range(1, levels):
            depth_copy(t, k).wait_recv()
            summed = summed + depth_in[t, k].astype(f32)
        summed = summed.astype(bf16)
        for place, source in enumerate(pair_sources(t)):
            at = pl.ds(pl.multiple_of(source * lanes, lanes), lanes)
            out_ref[:, at] = summed[:, place * lanes : (place + 1) * lanes]

    count = shards // 2

    def stage(t, carry):
        @pl.when((t >= 1) & (t < count + 1))
        def _():
            with jax.named_scope("pair_step"):
                pair_step(t - 1)

        for turn in range(levels + 1):
            if batches.get(50 + turn):

                @pl.when(t == turn)
                def _():
                    issue(50 + turn)

        @pl.when(t < count)
        def _():
            with jax.named_scope("lower_step"):
                lower_step(t)

        @pl.when(t >= LAG)
        def _():
            with jax.named_scope("depth_step"):
                depth_step(t - LAG)

        return carry

    lax.fori_loop(0, count + LAG, stage, 0)

    phase("drain")
    @pl.when(sp < shards - 1)
    def _():
        for one in halo_copies:
            one.wait_send()

    for one in state_copies + back_copies:
        one.wait_send()
    @pl.when(own_team == 0)
    def _():
        cross.wait_send()

    swap.wait_send()
    for part in range(parts):
        for place in range(levels):
            share(place, part).wait_send()
        for hop in range(top):

            @pl.when((level >= hop) & (level < top))
            def _():
                along(level_at(-hop), part, hop, True).wait_send()

            @pl.when((level + hop <= top) & (level > 0))
            def _():
                along(level_at(hop), part, hop, False).wait_send()

    for kind in range(2):
        for step in range(levels):
            for way in range(2):
                spread(kind, step, way).wait_send()
                relay(kind, step, way).wait_send()
            if step:
                rise(kind, step).wait_send()

    def drain(t, carry):
        pair_copy(t).wait_send()
        for k in range(1, levels):
            depth_copy(t, k).wait_send()
        return carry

    lax.fori_loop(0, count, drain, 0)
    phase("")


LAG = 3


def plan(levels):
    ur, dr = ([("rise", kind, step) for step in range(1, levels)] for kind in range(2))
    us, ds = ([("spread", kind, step) for step in range(levels)] for kind in range(2))
    ut, dt = ([("relay", kind, step) for step in range(levels)] for kind in range(2))
    return {0: [('rise', 0, 1), ('rise', 0, 2), ('spread', 0, 0)], 1: [('rise', 0, 3), ('relay', 0, 0), ('spread', 1, 0), ('spread', 0, 1)], 3: [('relay', 1, 0), ('rise', 1, 1), ('rise', 1, 2), ('rise', 1, 3), ('spread', 0, 2), ('spread', 0, 3)], 4: [('relay', 0, 1), ('relay', 0, 2), ('relay', 0, 3)], 13: [('spread level', 1, 0), ('spread level', 1, 1), ('spread level', 1, 2), ('spread level', 1, 3)], 50: [('relay level', 1, 0)], 51: [('relay level', 1, 1)], 52: [('relay level', 1, 2)], 53: [('relay level', 1, 3)]}


def per_device_fused(team, *operands):
    (
        skip_stream_entering,
        content_signal_matrix,
        writer_signal_matrix,
        reader_signal_matrix,
        multiplier_signal,
        interval_before_softplus,
        extra_log_shrink,
        log_forget_speed,
        content_filter_coefs,
        writer_filter_coefs,
        reader_filter_coefs,
        skip_path_factor,
        cluster_scaling_vector,
        blend_result_matrix,
        feature_blend_scaling,
        widening_matrix,
        narrowing_matrix,
    ) = operands
    f32, bf16 = jnp.float32, jnp.bfloat16
    shards = lax.axis_size("sp")
    length, inner = content_signal_matrix.shape
    state_width = writer_signal_matrix.shape[1]
    local_heads = interval_before_softplus.shape[0]
    rows_own, model = skip_stream_entering.shape
    levels = shards // 4
    unit = widening_matrix.shape[1] // levels
    depth = widening_matrix.shape[0]
    lanes = narrowing_matrix.shape[1]
    slice_width = inner // team
    pairs = shards // 2
    dma = pltpu.SemaphoreType.DMA
    vmem, anywhere = pl.BlockSpec(memory_space=pltpu.VMEM), pl.BlockSpec(memory_space=pl.ANY)
    specs = [anywhere] * 5 + [vmem] * 8 + [anywhere, vmem, anywhere, anywhere]
    scratch = [
        pltpu.VMEM((rows_own, model), bf16),
        pltpu.VMEM((length, inner), bf16),
        pltpu.VMEM((length, state_width), bf16),
        pltpu.VMEM((length, state_width), bf16),
        pltpu.VMEM((length, inner), bf16),
        pltpu.VMEM((16, inner + 2 * state_width), bf16),
        pltpu.VMEM((8 + length, inner + 2 * state_width), f32),
        pltpu.VMEM((length, inner), f32),
        pltpu.VMEM((length, 2 * state_width), bf16),
        pltpu.VMEM(blend_result_matrix.shape, bf16),
        pltpu.VMEM((shards, depth, unit), bf16),
        pltpu.VMEM((shards, unit, lanes), bf16),
        pltpu.VMEM((length, local_heads * length), f32),
        pltpu.VMEM((local_heads, length), f32),
        pltpu.VMEM((length, inner), f32),
        pltpu.VMEM((length, inner), f32),
        pltpu.VMEM((team, STATE + 16, slice_width), bf16),
        pltpu.VMEM((team, STATE + 16, slice_width), bf16),
        pltpu.VMEM((team, STATE, slice_width), f32),
        pltpu.VMEM((team, 8, slice_width), f32),
        pltpu.VMEM((STATE, slice_width), bf16),
        pltpu.VMEM((STATE, slice_width), bf16),
        pltpu.VMEM((team, STATE, slice_width), bf16),
        pltpu.VMEM((team, STATE, slice_width), bf16),
        pltpu.VMEM((length, inner), bf16),
        pltpu.VMEM((2, rows_own, model), bf16),
        pltpu.VMEM((rows_own, model), bf16),
        pltpu.VMEM((2, levels, rows_own, model), bf16),
        pltpu.VMEM((2, levels * rows_own, unit), bf16),
        pltpu.VMEM((pairs, levels * rows_own, 2 * lanes), bf16),
        pltpu.VMEM((pairs, levels * rows_own, 2 * lanes), bf16),
        pltpu.VMEM((pairs, levels, rows_own, 2 * lanes), bf16),
        pltpu.VMEM((pairs, levels, rows_own, 2 * lanes), bf16),
        dma((8,)),
        dma((3,)),
        dma((3,)),
        dma((3 * levels,)),
        dma((shards,)),
        dma((3 * levels,)),
        dma((shards,)),
        dma((4 * levels,)),
        dma((4 * levels,)),
        dma((team,)),
        dma((team,)),
        dma,
        dma,
        dma((team,)),
        dma((team,)),
        dma,
        dma,
        dma((4 * levels,)),
        dma((2 * levels,)),
        dma((2 * levels,)),
        dma((2 * levels,)),
        dma((pairs,)),
        dma((pairs,)),
        dma((pairs, levels)),
        dma((pairs, levels)),
    ]
    state, mixed = pl.pallas_call(
        functools.partial(layer_kernel, team),
        out_shape=[jax.ShapeDtypeStruct((rows_own, model), bf16)] * 2,
        in_specs=specs,
        out_specs=[vmem, vmem],
        scratch_shapes=scratch,
        compiler_params=pltpu.CompilerParams(
            collective_id=0, has_side_effects=True, vmem_limit_bytes=63 * 1024 * 1024
        ),
    )(
        skip_stream_entering,
        content_signal_matrix,
        writer_signal_matrix,
        reader_signal_matrix,
        multiplier_signal,
        interval_before_softplus,
        extra_log_shrink,
        log_forget_speed.reshape(1, -1),
        content_filter_coefs,
        writer_filter_coefs,
        reader_filter_coefs,
        skip_path_factor.reshape(1, -1),
        cluster_scaling_vector.reshape(1, -1),
        blend_result_matrix,
        feature_blend_scaling.reshape(1, -1),
        widening_matrix,
        narrowing_matrix,
    )
    return (state.astype(f32) + mixed.astype(f32)).astype(bf16)


def general_solution(mesh):
    shards, halves = mesh.shape["sp"], mesh.shape["tp"]
    team = math.gcd(shards, TEAM)
    teams = jax.sharding.Mesh(
        mesh.devices.reshape(shards // team, team, halves), ("sa", "sb", "tp")
    )
    placed = (
        P(("sa", "sb", "tp"), None),
        P(SP, "tp"),
        P(SP, "tp"),
        P(SP, "tp"),
        P(SP, "tp"),
        P("tp", SP),
        P("tp", SP),
        P("tp"),
        P(None, "tp"),
        P(None, "tp"),
        P(None, "tp"),
        P("tp"),
        P("tp"),
        P("tp", None),
        P(),
        P(SP, "tp"),
        P("tp", SP),
    )
    return jax.shard_map(
        per_device, mesh=teams, in_specs=placed, out_specs=P(("sa", "sb", "tp"), None), check_vma=False
    )


def fits(shards, halves, team, rows, tokens, inner, hidden, model, state_width):
    length = tokens // shards
    local = inner // halves
    return (
        halves == 2
        and shards == 2 * team
        and team % 4 == 0
        and length == BLOCK
        and length % 32 == 0
        and local % (team * 128) == 0
        and shards % 4 == 0
        and (hidden // halves) % (shards // 4 * 128) == 0
        and (shards // 4) == 4
        and model % (shards * 128) == 0
        and (state_width // halves) % STATE == 0
        and (local // (state_width // halves // STATE)) % (local // team) == 0
    )


def solution(mesh):
    shards, halves = mesh.shape["sp"], mesh.shape["tp"]
    team = math.gcd(shards, TEAM)
    general = general_solution(mesh)
    row, both = P("sp", "tp"), P(("sp", "tp"), None)
    tp_first, tp_last, tp_only = P("tp", "sp"), P(None, "tp"), P("tp")
    placed = (
        (both, row, row, row, row, tp_first, tp_first, tp_only, tp_last, tp_last, tp_last)
        + (tp_only, tp_only, P("tp", None), P(), row, tp_first)
    )
    fused = jax.shard_map(
        functools.partial(per_device_fused, team),
        mesh=mesh,
        in_specs=placed,
        out_specs=both,
        check_vma=False,
    )

    def layer(*operands):
        tokens, inner = operands[1].shape
        model, hidden = operands[15].shape
        state_width = operands[2].shape[1]
        if fits(shards, halves, team, tokens, tokens, inner, hidden, model, state_width):
            return fused(*operands)
        return general(*operands)

    return layer
```
